32 devices in a mesh: ep: 16 (over z, y, x), tp: 2 (over core).
Axes of the slice: x: 2, y: 2, z: 4, core: 2. Of those that a mesh axis runs over, the one named last changes fastest.
Arguments:
- tokens: bfloat16 [512, 2048], P('ep'), may hold values from -6 to 6
- mix_gain: float32 [2048], replicated, may hold values from 0.1 to 1.9
- w_query: bfloat16 [2048, 512], P('ep', 'tp'), may hold values from -0.125 to 0.125
- w_key: bfloat16 [2048, 512], P('ep', 'tp'), may hold values from -0.125 to 0.125
- w_value: bfloat16 [2048, 512], P('ep', 'tp'), may hold values from -0.125 to 0.125
- w_outgate: bfloat16 [2048, 512], P('ep', 'tp'), may hold values from -0.125 to 0.125
- w_igate: bfloat16 [2048, 8], P('ep', 'tp'), may hold values from -0.125 to 0.125
- w_fgate: bfloat16 [2048, 8], P('ep', 'tp'), may hold values from -0.125 to 0.125
- igate_bias: float32 [8], P('tp'), may hold values from -2 to 1
- fgate_bias: float32 [8], P('tp'), may hold values from 0 to 4
- head_gain: float32 [512], P('tp'), may hold values from 0.1 to 1.9
- w_out: bfloat16 [512, 2048], P('tp', 'ep'), may hold values from -0.25 to 0.25
- state_matrix: float32 [512, 8, 64, 64], P('ep', 'tp'), may hold values from -2.4 to 2.4
- state_norm: float32 [512, 8, 64], P('ep', 'tp'), may hold values from -2.4 to 2.4
- state_max: float32 [512, 8], P('ep', 'tp'), may hold values from -4 to 4
- ffn_gain: float32 [2048], replicated, may hold values from 0.1 to 1.9
- w_expert_gate: bfloat16 [16, 2048, 1408], P('ep', None, 'tp'), may hold values from -0.125 to 0.125
- w_expert_up: bfloat16 [16, 2048, 1408], P('ep', None, 'tp'), may hold values from -0.125 to 0.125
- w_expert_down: bfloat16 [16, 1408, 2048], P('ep', 'tp'), may hold values from -0.15625 to 0.15625
- routes: int32 [512, 3], P('ep'), may hold values from 0 to 15, all different within a row; in each aligned block of 32 rows (0 to 31, 32 to 63, ...) at most 12 rows name the same one
- route_weights: float32 [512, 3], P('ep'), may hold values from 0.2 to 1
Outputs:
- mixed: bfloat16 [512, 2048], P('ep')
- new_matrix: float32 [512, 8, 64, 64], P('ep', 'tp')
- new_norm: float32 [512, 8, 64], P('ep', 'tp')
- new_max: float32 [512, 8], P('ep', 'tp')
The draws below stay inside these ranges and needn't reach their ends.
Inputs may be any that keep to these rules, and one draw needn't show every extreme that they name: `routes`: each row names 3 different experts. Among the rows of one device, no expert is named by more than 12 rows, a bound that some block reaches.
All inputs are finite; a program needn't handle non-finite values.
Results may differ from the reference program's by a relative error of at most 0.017.
Values may be sent and summed in bfloat16 or wider, within the bound.
A program may use at most 128 MiB of HBM per device.

```python
import math
import jax
import jax.numpy as jnp
import numpy as np
from jax import lax

D = 2048
HEADS = 8
HEAD_SIZE = 64
HW = 512
D_EXP = 1408
TOPK = 3
EXPERTS = 16
SEQ_DEV = 32
B = 512
CAP = 12
N_EP = 16
N_TP = 2


def steps_of(stream_key, shape, split, low, high):
    level = 1.0
    for position, shards_of in split:
        draws = jax.random.uniform(jax.random.fold_in(jax.random.fold_in(stream_key, 6), position), (shards_of,), jnp.float32, low / len(split), high / len(split))
        level = level * jnp.repeat(jnp.exp(draws), shape[position] // shards_of).reshape((-1,) + (1,) * (len(shape) - 1 - position))
    return level


def routed_block(stream_key, own, number, rows, amount, top, reach, lean):
    order = jax.random.permutation(stream_key, amount)
    packed, usual = load_shares(amount, rows * top, reach, lean, True), load_shares(amount, rows * top, reach, lean, False)
    places = jnp.arange(amount)

    def named(tallies, offset_by):
        used = int((tallies > 0).sum())
        fixed = max(1, used // 4)
        shifted = fixed + (places - fixed + offset_by * (used - fixed)) % max(1, amount - fixed)
        return jnp.zeros((amount,), jnp.int32).at[order[jnp.where(places < fixed, places, shifted)]].set(jnp.asarray(tallies, jnp.int32))

    tallies = jnp.where(number % 4 == 0, named(packed, number // 4), named(usual, number - number // 4 - 1))
    mixed = jax.random.permutation(jax.random.fold_in(own, 3), amount)
    source_of, sink = mixed[0:amount // 2 * 2:2], mixed[1:amount // 2 * 2:2]
    room = jnp.minimum(tallies[source_of] - 1, reach - tallies[sink]) // 2
    room = jnp.where((source_of == order[0]) | (sink == order[0]) | (tallies[sink] == 0), 0, jnp.maximum(room, 0))
    shifted = jax.random.randint(jax.random.fold_in(own, 4), (amount // 2,), 0, 1 << 20) % (room + 1)
    tallies = tallies.at[source_of].add(-shifted).at[sink].add(shifted)
    labels = jnp.searchsorted(jnp.cumsum(tallies), jnp.arange(rows * top), side="right").astype(jnp.int32)
    listing = labels.reshape(top, rows).T
    listing = listing[jax.random.permutation(jax.random.fold_in(own, 1), rows)]
    offset_by = jax.random.randint(jax.random.fold_in(own, 2), (rows, 1), 0, top)
    return jnp.take_along_axis(listing, (jnp.arange(top)[None, :] + offset_by) % top, axis=1)


def load_shares(number_of, total, reach, lean, full):
    loads = [(1 << 20) // math.isqrt(rank ** lean) + 1 for rank in range(1, number_of + 1)]
    largest = reach if full else min(reach, max(-(-total // number_of), total * loads[0] // sum(loads)))
    least = 1 if total - largest >= number_of - 1 else 0
    given, rest = [largest] + [least] * (number_of - 1), total - largest - least * (number_of - 1)
    while rest > 0:
        candidates = [i for i in range(1, number_of) if given[i] < largest] or [i for i in range(1, number_of) if given[i] < reach]
        pool, budget = sum([loads[i] for i in candidates]), rest
        for i in candidates:
            more = min(reach - given[i], max(1, budget * loads[i] // pool), rest)
            given[i] = given[i] + more
            rest = rest - more
    return np.array(given)


def normal_values(key, dims, spread, limit, pieces=(), kind=jnp.bfloat16):
    values = jax.random.normal(key, dims, jnp.float32) * spread
    if len(pieces) > 0:
        values = steps_of(key, dims, pieces, -0.22, 0.18) * values
    return jnp.clip(values, min=-limit, max=limit).astype(kind)


def setup_inputs(seed: int = 0) -> dict:
    arg_keys = jax.random.split(jax.random.key(seed), 22)
    tokens = normal_values(arg_keys[0], (B, D), 1.0, 6.0, ((0, 16),))
    mix_gain = jnp.clip(1.0 + 0.18 * jax.random.normal(arg_keys[1], (D,), jnp.float32), 0.1, 1.9)
    w_query = normal_values(arg_keys[2], (D, HW), D ** -0.5, 0.125, ((0, 16), (1, 2)))
    w_key = normal_values(arg_keys[3], (D, HW), D ** -0.5, 0.125, ((0, 16), (1, 2)))
    w_value = normal_values(arg_keys[4], (D, HW), D ** -0.5, 0.125, ((0, 16), (1, 2)))
    w_outgate = normal_values(arg_keys[5], (D, HW), D ** -0.5, 0.125, ((0, 16), (1, 2)))
    w_igate = normal_values(arg_keys[6], (D, HEADS), D ** -0.5, 0.125, ((0, 16), (1, 2)))
    w_fgate = normal_values(arg_keys[7], (D, HEADS), D ** -0.5, 0.125, ((0, 16), (1, 2)))
    igate_bias = jnp.clip(-2.0 + 3.0 * jax.random.uniform(arg_keys[8], (HEADS,), jnp.float32) ** steps_of(arg_keys[8], (HEADS,), ((0, 2),), -0.2, 0.2), -2.0, 1.0)
    fgate_bias = jnp.clip(4.0 * jax.random.uniform(arg_keys[9], (HEADS,), jnp.float32) ** steps_of(arg_keys[9], (HEADS,), ((0, 2),), -0.2, 0.2), 0.0, 4.0)
    head_gain = jnp.clip(1.0 + 0.18 * jax.random.normal(arg_keys[10], (HW,), jnp.float32), 0.1, 1.9)
    w_out = normal_values(arg_keys[11], (HW, D), HW ** -0.5, 0.25, ((0, 2), (1, 16)))
    state_matrix = normal_values(arg_keys[12], (B, HEADS, HEAD_SIZE, HEAD_SIZE), 0.3, 2.4, ((0, 16), (1, 2)), jnp.float32)
    state_norm = normal_values(arg_keys[13], (B, HEADS, HEAD_SIZE), 0.3, 2.4, ((0, 16), (1, 2)), jnp.float32)
    state_max = normal_values(arg_keys[14], (B, HEADS), 1.0, 4.0, ((0, 16), (1, 2)), jnp.float32)
    ffn_gain = jnp.clip(1.0 + 0.18 * jax.random.normal(arg_keys[15], (D,), jnp.float32), 0.1, 1.9)
    w_expert_gate = normal_values(arg_keys[16], (EXPERTS, D, D_EXP), D ** -0.5, 0.125, ((0, 16), (2, 2)))
    w_expert_up = normal_values(arg_keys[17], (EXPERTS, D, D_EXP), D ** -0.5, 0.125, ((0, 16), (2, 2)))
    w_expert_down = normal_values(arg_keys[18], (EXPERTS, D_EXP, D), D_EXP ** -0.5, 0.15625, ((0, 16), (1, 2)))
    routes_keys = jax.random.split(jax.random.fold_in(arg_keys[19], 1), B // SEQ_DEV)
    routes_turns = jax.random.permutation(jax.random.fold_in(arg_keys[19], 3), B // SEQ_DEV)
    routes = jax.vmap(lambda own, number: routed_block(jax.random.fold_in(arg_keys[19], 2), own, number, SEQ_DEV, EXPERTS, TOPK, CAP, 2))(routes_keys, routes_turns).reshape((B, TOPK))
    route_weights = jnp.clip(0.2 + 0.8 * jax.random.uniform(arg_keys[20], (B, TOPK), jnp.float32) ** steps_of(arg_keys[20], (B, TOPK), ((0, 16),), -0.2, 0.2), 0.2, 1.0)
    return {"tokens": tokens, "mix_gain": mix_gain, "w_query": w_query, "w_key": w_key, "w_value": w_value, "w_outgate": w_outgate, "w_igate": w_igate, "w_fgate": w_fgate, "igate_bias": igate_bias, "fgate_bias": fgate_bias, "head_gain": head_gain, "w_out": w_out, "state_matrix": state_matrix, "state_norm": state_norm, "state_max": state_max, "ffn_gain": ffn_gain, "w_expert_gate": w_expert_gate, "w_expert_up": w_expert_up, "w_expert_down": w_expert_down, "routes": routes, "route_weights": route_weights}


def rms_scale(values_in, gain_vec):
    widened = values_in.astype(jnp.float32)
    return widened * lax.rsqrt(lax.optimization_barrier(jnp.mean(widened * widened, axis=-1, keepdims=True)) + 1e-06) * gain_vec

def memory_cell(query, key_row, value_row, outgate, input_pre, forget_pre, head_gain, state_matrix, state_norm, state_max):
    seq_rows, head_count = input_pre.shape
    head_size = query.shape[1] // head_count
    query_heads = query.astype(jnp.float32).reshape(seq_rows, head_count, head_size)
    key_heads = key_row.astype(jnp.float32).reshape(seq_rows, head_count, head_size) * head_size ** (-0.5)
    value_heads = value_row.astype(jnp.float32).reshape(seq_rows, head_count, head_size)
    log_forget = jax.nn.log_sigmoid(forget_pre)
    new_max = jnp.maximum(log_forget + state_max, input_pre)
    keep_old = jnp.exp(log_forget + state_max - new_max)
    keep_new = jnp.exp(input_pre - new_max)
    new_matrix = keep_old[:, :, None, None] * state_matrix + keep_new[:, :, None, None] * value_heads[:, :, :, None] * key_heads[:, :, None, :]
    new_norm = keep_old[:, :, None] * state_norm + keep_new[:, :, None] * key_heads
    numerator = jnp.einsum('bhvd,bhd->bhv', new_matrix, query_heads, precision=lax.Precision.HIGHEST)
    denominator = lax.optimization_barrier(jnp.sum(new_norm * query_heads, axis=-1))
    cell_read = numerator / jnp.maximum(jnp.abs(denominator), jnp.exp(-new_max))[:, :, None]
    centered = cell_read - lax.optimization_barrier(jnp.mean(cell_read, axis=-1, keepdims=True))
    variance = lax.optimization_barrier(jnp.mean(centered * centered, axis=-1, keepdims=True))
    scaled_cell = (centered * lax.rsqrt(variance + 1e-06)).reshape(seq_rows, head_count * head_size)
    cell_out = (scaled_cell * head_gain * jax.nn.sigmoid(outgate.astype(jnp.float32))).astype(jnp.bfloat16)
    return (cell_out, new_matrix, new_norm, new_max)

def reference(tokens, mix_gain, w_query, w_key, w_value, w_outgate, w_igate, w_fgate, igate_bias, fgate_bias, head_gain, w_out, state_matrix, state_norm, state_max, ffn_gain, w_expert_gate, w_expert_up, w_expert_down, routes, route_weights):
    normed = rms_scale(tokens, mix_gain).astype(jnp.bfloat16)

    def project(weight):
        return jnp.dot(normed, weight, preferred_element_type=jnp.float32)
    query = project(w_query).astype(jnp.bfloat16)
    key_row = project(w_key).astype(jnp.bfloat16)
    value_row = project(w_value).astype(jnp.bfloat16)
    outgate = project(w_outgate).astype(jnp.bfloat16)
    input_pre = project(w_igate) + igate_bias
    forget_pre = project(w_fgate) + fgate_bias
    cell_out, new_matrix, new_norm, new_max = memory_cell(query, key_row, value_row, outgate, input_pre, forget_pre, head_gain, state_matrix, state_norm, state_max)
    seq_rows, width = tokens.shape
    cell_width = cell_out.shape[1]
    blocks = jnp.einsum('bth,thd->btd', cell_out.astype(jnp.float32).reshape(seq_rows, N_TP, cell_width // N_TP), w_out.astype(jnp.float32).reshape(N_TP, cell_width // N_TP, width))
    rounded = lax.optimization_barrier(blocks.astype(jnp.bfloat16))
    resid = (tokens.astype(jnp.float32) + lax.optimization_barrier(jnp.sum(rounded.astype(jnp.float32), axis=1))).astype(jnp.bfloat16)
    normed_two = rms_scale(resid, ffn_gain).astype(jnp.bfloat16)
    groups = N_EP
    per_group = seq_rows // groups
    expert_total = w_expert_gate.shape[0]
    top_count = routes.shape[1]
    flat_routes = routes.reshape(groups, per_group * top_count)
    onehot = (flat_routes[:, :, None] == jnp.arange(expert_total, dtype=jnp.int32)[None, None, :]).astype(jnp.int32)
    earlier = jnp.cumsum(onehot, axis=1, dtype=jnp.int32) - onehot
    slots = lax.optimization_barrier(jnp.sum(onehot * earlier, axis=-1, dtype=jnp.int32)).astype(jnp.int32)
    group_ids = jnp.broadcast_to(jnp.arange(groups, dtype=jnp.int32)[:, None], flat_routes.shape)
    token_ids = (jnp.arange(seq_rows * top_count, dtype=jnp.int32) // top_count).reshape(groups, per_group * top_count)
    table = jnp.zeros((expert_total, groups, CAP), jnp.int32).at[flat_routes, group_ids, slots].set(token_ids)

    def run_expert(operands):
        gate_weight, up_weight, down_weight, row_ids = operands
        rows = normed_two[row_ids.reshape(-1)]
        gate_pre = jnp.dot(rows, gate_weight, preferred_element_type=jnp.float32)
        up_pre = jnp.dot(rows, up_weight, preferred_element_type=jnp.float32)
        hidden = (jax.nn.silu(gate_pre) * up_pre).astype(jnp.bfloat16)
        expert_width = hidden.shape[1]
        parts = jnp.einsum('rtf,tfd->rtd', hidden.astype(jnp.float32).reshape(-1, N_TP, expert_width // N_TP), down_weight.astype(jnp.float32).reshape(N_TP, expert_width // N_TP, width))
        rounded_parts = lax.optimization_barrier(parts.astype(jnp.bfloat16))
        return lax.optimization_barrier(jnp.sum(rounded_parts.astype(jnp.float32), axis=1)).astype(jnp.bfloat16)
    outputs = lax.map(run_expert, (w_expert_gate, w_expert_up, w_expert_down, table))
    picked = outputs[flat_routes, group_ids * CAP + slots]
    picked = picked.reshape(seq_rows, top_count, width).astype(jnp.float32)
    mixed = (resid.astype(jnp.float32) + lax.optimization_barrier(jnp.sum(picked * route_weights[:, :, None], axis=1))).astype(jnp.bfloat16)
    return (mixed, new_matrix, new_norm, new_max)
```

```python
import functools

import jax
import jax.numpy as jnp
from jax import lax
from jax.experimental import pallas as pl
from jax.experimental.pallas import tpu as pltpu
from jax.sharding import PartitionSpec as P

MESH = pl.DeviceIdType.MESH
PLANE = 4
LANES = 128
SUB = 8
LAYER_BYTES = 40 * 1024 * 1024
UPDATE_BYTES = 12 * 1024 * 1024


def remote(src, dst, send_sem, recv_sem, target):
    return pltpu.make_async_remote_copy(
        src_ref=src,
        dst_ref=dst,
        send_sem=send_sem,
        recv_sem=recv_sem,
        device_id=target,
        device_id_type=MESH,
    )


def dot_t(left, right):
    return lax.dot_general(
        left, right, (((1,), (1,)), ((), ())), preferred_element_type=jnp.float32
    )


def fetch_all(pairs, sems):
    copies = []
    for index, (source, kept) in enumerate(pairs):
        copy = pltpu.make_async_copy(source, kept, sems.at[index])
        copy.start()
        copies.append(copy)
    return copies


def place(index, size):
    return pl.ds(pl.multiple_of(index * size, size), size)


def split_three(values):
    high = values.astype(jnp.bfloat16)
    rest = values - high.astype(jnp.float32)
    middle = rest.astype(jnp.bfloat16)
    return [high, middle, (rest - middle.astype(jnp.float32)).astype(jnp.bfloat16)]


def exact_dot(values, chosen):
    rows = values[0].shape[0]
    parts = [part for value in values for part in split_three(value)]
    product = jnp.dot(
        jnp.concatenate(parts, axis=0), chosen, preferred_element_type=jnp.float32
    )
    results = []
    for index in range(len(values)):
        start = 3 * index * rows
        pieces = [product[start + rows * part : start + rows * (part + 1)] for part in range(3)]
        results.append(pieces[0] + pieces[1] + pieces[2])
    return results


def ones_where(condition):
    return jnp.where(condition, 1.0, 0.0).astype(jnp.bfloat16)


def gather_rows(chosen, values):
    return jnp.dot(chosen, values, preferred_element_type=jnp.float32).astype(jnp.bfloat16)


def layer_kernel(
    count,
    tokens_hbm,
    mix_gain_hbm,
    wq_hbm,
    wk_hbm,
    wv_hbm,
    wg_hbm,
    igate_hbm,
    fgate_hbm,
    ibias_hbm,
    fbias_hbm,
    head_gain_hbm,
    w_out_hbm,
    matrix_hbm,
    norm_hbm,
    max_hbm,
    ffn_gain_hbm,
    w_gate_hbm,
    w_up_hbm,
    w_down_hbm,
    routes_hbm,
    route_weights_hbm,
    mixed_ref,
    left_ref,
    keys_ref,
    decay_ref,
    new_norm_ref,
    new_max_ref,
    tokens,
    mix_gain,
    igate,
    fgate,
    ibias,
    fbias,
    head_gain,
    matrix,
    state_norm,
    state_max,
    ffn_gain,
    w_gate,
    w_up,
    w_down,
    routes,
    route_weights,
    turned,
    gate_rows,
    gate_t,
    weights_a,
    weights_b,
    w_planes,
    normed,
    spread,
    partial_a,
    partial_b,
    outgoing_a,
    outgoing_b,
    arrived_a,
    arrived_b,
    packed,
    chosen_out,
    chosen_in,
    token_out,
    token_near,
    token_far,
    cell_mine,
    cell_theirs,
    cell_out,
    cell_near,
    cell_far,
    token_rows,
    reads,
    resid,
    row_values,
    down_send,
    down_recv,
    finished,
    returned,
    last_send,
    last_recv,
    local_sem,
    a_send,
    a_recv,
    b_send,
    b_recv,
    g_send,
    g_recv,
    x_send,
    x_recv,
    z_send,
    z_recv,
    pa_send,
    pa_recv,
    pb_send,
    pb_recv,
    o_send,
    o_recv,
    t_send,
    t_recv,
    k_send,
    k_recv,
    c_send,
    c_recv,
    f_send,
    f_recv,
    r_send,
    r_recv,
):
    bf, f32 = jnp.bfloat16, jnp.float32
    ep, tp = lax.axis_index("ep"), lax.axis_index("tp")
    lines = count // PLANE
    line, spot = ep // PLANE, ep % PLANE
    rows, width = tokens.shape
    half = width // 2
    depth = wq_hbm.shape[0]
    block = depth * PLANE
    heads = igate.shape[0]
    size = matrix.shape[3]
    wide = heads * size
    pair = 2 * wide
    area = count * SUB
    top = route_weights.shape[0]
    columns = w_out_hbm.shape[1]
    slab = lines * columns
    part_wide = slab // 2
    partner = (ep, 1 - tp)
    beside = spot + 1 - 2 * (spot % 2)
    across = lax.rem(spot + 2, PLANE)
    beside_peer = (line * PLANE + beside, tp)
    across_peer = (line * PLANE + across, tp)
    corner_peer = (line * PLANE + PLANE - 1 - spot, tp)
    my_half, other_half = place(tp, half), place(1 - tp, half)
    my_rows, other_rows = place(tp, wide), place(1 - tp, wide)
    own_rows = place(spot, depth)

    def line_peer(step):
        other = lax.rem(line + step, lines)
        return other, (other * PLANE + spot, tp)

    first_loads = fetch_all(
        (
            (wq_hbm, weights_a.at[own_rows, :wide]),
            (wk_hbm, weights_a.at[own_rows, wide:]),
            (igate_hbm, igate),
            (fgate_hbm, fgate),
            (wv_hbm, weights_b.at[own_rows, :wide]),
            (wg_hbm, weights_b.at[own_rows, wide:]),
            (tokens_hbm, tokens),
            (mix_gain_hbm, mix_gain),
            (w_out_hbm, w_planes.at[spot, my_rows, place(line, columns)]),
            (routes_hbm, routes),
            (route_weights_hbm, route_weights),
        ),
        local_sem,
    )
    barrier = pltpu.get_barrier_semaphore()
    for step in range(1, count):
        pl.semaphore_signal(
            barrier, inc=1, device_id=(lax.rem(ep + step, count), tp), device_id_type=MESH
        )
    pl.semaphore_signal(barrier, inc=1, device_id=partner, device_id_type=MESH)
    turned[...] = jnp.zeros_like(turned)
    gate_t[...] = jnp.zeros_like(gate_t)
    for copy in first_loads[:4]:
        copy.wait()
    turned[:heads, :] = igate[...].astype(f32)
    turned[heads : 2 * heads, :] = fgate[...].astype(f32)
    gate_rows[spot] = turned[: 2 * heads, :].astype(bf)
    pl.semaphore_wait(barrier, count)

    def plane_copies(buffer_view, send, recv):
        def make(owner, part, slot, target):
            view = buffer_view(owner, part)
            return remote(view, view, send.at[slot], recv.at[slot], target)

        return make

    def weight_view(buffer):
        def view(owner, part):
            tall = depth // 2
            return buffer.at[pl.ds(pl.multiple_of(owner * depth + part * tall, tall), tall)]

        return view

    def out_view(owner, part):
        return w_planes.at[owner, my_rows, part * part_wide : (part + 1) * part_wide]

    def open_plane(make):
        first = [
            make(spot, 0, 0, beside_peer),
            make(spot, 1, 2, across_peer),
            make(spot, 1, 1, beside_peer),
            make(spot, 0, 3, across_peer),
        ]
        for copy in first:
            copy.start()
        return first

    def relay_plane(make, first):
        first[0].wait_recv()
        ahead = make(beside, 0, 4, across_peer)
        ahead.start()
        first[1].wait_recv()
        aside = make(across, 1, 5, beside_peer)
        aside.start()
        return [ahead, aside]

    def close_plane(first, second):
        first[2].wait_recv()
        first[3].wait_recv()
        for copy in first:
            copy.wait_send()
        for copy in second:
            copy.wait()

    make_a = plane_copies(weight_view(weights_a), a_send, a_recv)
    make_b = plane_copies(weight_view(weights_b), b_send, b_recv)
    make_o = plane_copies(out_view, o_send, o_recv)
    a_first = open_plane(make_a)
    gate_copies = []
    for slot, target in enumerate((beside_peer, across_peer, corner_peer)):
        view = gate_rows.at[spot]
        copy = remote(view, view, g_send.at[slot], g_recv.at[slot], target)
        copy.start()
        gate_copies.append(copy)
    for copy in first_loads[4:9]:
        copy.wait()
    widened = tokens[...].astype(f32)
    scale = lax.rsqrt(jnp.mean(widened * widened, axis=-1, keepdims=True) + 1e-06)
    normed[...] = (widened * scale * mix_gain[...]).astype(bf)
    x_copies, z_copies = [], []
    for step in range(1, lines):
        other, target = line_peer(step)
        copy = remote(
            normed.at[:, place(other, block)],
            spread.at[line],
            x_send.at[step],
            x_recv.at[step],
            target,
        )
        copy.start()
        x_copies.append(copy)
    for step in range(1, lines):
        view = w_planes.at[spot, my_rows, place(line, columns)]
        copy = remote(view, view, z_send.at[step], z_recv.at[step], line_peer(step)[1])
        copy.start()
        z_copies.append(copy)
    spread[line] = normed[:, place(line, block)]
    for copy in first_loads[9:]:
        copy.wait()
    late_loads = fetch_all(
        (
            (matrix_hbm, matrix),
            (norm_hbm, state_norm),
            (max_hbm, state_max),
            (ibias_hbm, ibias),
            (fbias_hbm, fbias),
            (head_gain_hbm, head_gain),
            (ffn_gain_hbm, ffn_gain),
            (w_gate_hbm, w_gate),
            (w_up_hbm, w_up),
            (w_down_hbm, w_down),
        ),
        local_sem,
    )

    slot_row = lax.broadcasted_iota(jnp.int32, (area, rows), 0).astype(f32)
    expert = lax.broadcasted_iota(jnp.int32, (count, rows), 0).astype(f32)
    before = jnp.where(
        lax.broadcasted_iota(jnp.int32, (rows, rows), 0)
        < lax.broadcasted_iota(jnp.int32, (rows, rows), 1),
        1.0,
        0.0,
    )
    taken = jnp.zeros((count, 1), f32)
    sent = [jnp.zeros((area, rows), f32) for _ in range(3)]
    mixes = [jnp.zeros((area, rows), f32) for _ in range(3)]
    for k in range(top):
        named = routes[k : k + 1, :].astype(f32)
        match = jnp.where(expert == named, 1.0, 0.0)
        earlier = jnp.dot(match, before, preferred_element_type=f32) + taken
        taken = taken + jnp.sum(match, axis=1, keepdims=True)
        position = jnp.sum(match * earlier, axis=0, keepdims=True)
        low = jnp.where(position < SUB, named * SUB + position, -1000.0)
        high = jnp.where(position < SUB, -1000.0, named * SUB + position - SUB)
        for index, target in enumerate((low, high, high + SUB // 2)):
            hit = slot_row == target
            sent[index] += jnp.where(hit, 1.0, 0.0)
            mixes[index] += jnp.where(hit, route_weights[k : k + 1, :], 0.0)
    for index in range(3):
        chosen_out[index] = sent[index].astype(bf)
        coarse = mixes[index].astype(bf).astype(f32)
        joined = jnp.concatenate(
            [coarse, mixes[index] - coarse, jnp.zeros((area, area - 2 * rows), f32)], axis=1
        )
        chosen_in[index] = joined.T[: 2 * rows].astype(bf)

    def pack_rows(values, target):
        middle = values.shape[1] // 2
        target[:, :, : 2 * middle] = gather_rows(chosen_out[0], values).reshape(
            count, SUB, 2 * middle
        )
        extra = jnp.dot(chosen_out[1], values[:, :middle], preferred_element_type=f32)
        extra += jnp.dot(chosen_out[2], values[:, middle:], preferred_element_type=f32)
        target[:, :, 2 * middle :] = extra.astype(bf).reshape(count, SUB, middle)

    a_second = relay_plane(make_a, a_first)
    b_first = open_plane(make_b)
    pack_rows(tokens[:, my_half], token_out)
    late_loads[0].wait()

    def pack_matrix(start, stop):
        @pl.loop(start, stop)
        def _(index):
            item = 2 * index
            joined = jnp.concatenate(
                [matrix[item].reshape(wide, size), matrix[item + 1].reshape(wide, size)], axis=1
            )
            flipped = joined.T
            upper = flipped.astype(bf)
            packed[index, : 2 * size] = upper
            packed[index, 2 * size :] = (flipped - upper.astype(f32)).astype(bf)

    pack_matrix(0, rows // 4)
    for copy in gate_copies:
        copy.wait()
    for owner in range(PLANE):
        part = gate_rows[owner]
        gate_t[: 2 * heads, owner * depth : (owner + 1) * depth] = part
        gate_t[LANES // 2 : LANES // 2 + 2 * heads, owner * depth : (owner + 1) * depth] = part
    for copy in x_copies:
        copy.wait()
    close_plane(a_first, a_second)
    arranged = spread[...].reshape(lines * rows, block)
    product = jnp.dot(arranged, weights_a[...], preferred_element_type=f32)
    gates = dot_t(arranged, gate_t[...])
    coarse = gates.astype(bf).astype(f32)
    first = lax.broadcasted_iota(jnp.int32, gates.shape, 1) < LANES // 2
    picked = jnp.where(first, coarse, gates - coarse).astype(bf)
    outgoing_a[:, :, :pair] = product.astype(bf).reshape(lines, rows, pair)
    outgoing_a[:, :, pair:] = picked.reshape(lines, rows, LANES)
    partial_a[:, :, :pair] = product.reshape(lines, rows, pair)
    partial_a[:, :, pair:] = jnp.where(first, gates, 0.0).reshape(lines, rows, LANES)

    def send_partials(outgoing, arrived, send, recv):
        copies = []
        for step in range(1, lines):
            other, target = line_peer(step)
            copy = remote(
                outgoing.at[other], arrived.at[step], send.at[step], recv.at[step], target
            )
            copy.start()
            copies.append(copy)
        return copies

    pa_copies = send_partials(outgoing_a, arrived_a, pa_send, pa_recv)
    b_second = relay_plane(make_b, b_first)
    pack_matrix(rows // 4, rows // 2)
    for copy in late_loads[1:7]:
        copy.wait()

    chosen_head = ones_where(
        lax.broadcasted_iota(jnp.int32, (LANES, pair), 0) % (LANES // 2)
        == lax.broadcasted_iota(jnp.int32, (LANES, pair), 1) // size
    )
    same_head = ones_where(
        lax.broadcasted_iota(jnp.int32, (wide, wide), 0) // size
        == lax.broadcasted_iota(jnp.int32, (wide, wide), 1) // size
    )
    same_place = ones_where(
        lax.broadcasted_iota(jnp.int32, (wide, wide), 0) % size
        == lax.broadcasted_iota(jnp.int32, (wide, wide), 1) % size
    )
    turned[...] = jnp.zeros_like(turned)
    turned[:heads, :rows] = state_max[...]
    old_max_lane = turned[...].T[:rows]
    turned[...] = jnp.zeros_like(turned)
    turned[0:1, :heads] = ibias[...]
    turned[1:2, :heads] = fbias[...]
    ibias_lane, fbias_lane = turned[0:1, :], turned[1:2, :]
    biases = jnp.concatenate(
        [ibias_lane + pltpu.roll(fbias_lane, heads, 1), jnp.zeros((7, LANES), f32)], axis=0
    )
    old_max_wide, bias_wide = (
        exact_dot([old_max_lane], chosen_head)[0][:, :wide],
        exact_dot([biases], chosen_head)[0][:1],
    )
    old_norm = jnp.concatenate([state_norm[:, head, :] for head in range(heads)], axis=1)

    for copy in z_copies:
        copy.wait()
    close_plane(b_first, b_second)
    product = jnp.dot(arranged, weights_b[...], preferred_element_type=f32)
    outgoing_b[...] = product.astype(bf).reshape(lines, rows, pair)
    partial_b[...] = product.reshape(lines, rows, pair)
    pb_copies = send_partials(outgoing_b, arrived_b, pb_send, pb_recv)
    o_first = open_plane(make_o)

    def scatter(source, near, send, recv):
        copies = []
        for step in range(1, count):
            other = lax.rem(ep + step, count)
            copy = remote(
                source.at[other], near.at[ep], send.at[step], recv.at[step], (other, tp)
            )
            copy.start()
            copies.append(copy)
        near[ep] = source[ep]
        return copies

    token_copies = scatter(token_out, token_near, k_send, k_recv)

    total = partial_a[line]
    for step in range(1, lines):
        pa_copies[step - 1].wait()
        total = total + arrived_a[step].astype(f32)
    gates_lane = total[:, pair:]
    gates_wide = exact_dot([gates_lane], chosen_head)[0]

    def gate_math(input_pre, forget_pre, old_max):
        log_forget = jnp.minimum(forget_pre, 0.0) - jnp.log(1.0 + jnp.exp(-jnp.abs(forget_pre)))
        new_max = jnp.maximum(log_forget + old_max, input_pre)
        return new_max, jnp.exp(log_forget + old_max - new_max), jnp.exp(input_pre - new_max)

    new_max, keep_old, keep_new = gate_math(
        gates_wide[:, :wide] + bias_wide[:, :wide],
        gates_wide[:, wide:] + bias_wide[:, wide:],
        old_max_wide,
    )
    query = total[:, :wide].astype(bf).astype(f32)
    key = total[:, wide:pair].astype(bf).astype(f32) * size ** (-0.5)
    pack = 2 * heads
    row = lax.broadcasted_iota(jnp.int32, (rows, pack, wide), 1)
    head = lax.broadcasted_iota(jnp.int32, (rows, pack, wide), 2) // size
    only = row == head
    spread_query = jnp.where(only, jnp.broadcast_to(query[:, None, :], only.shape), 0.0)
    tiled = jnp.dot(
        spread_query.reshape(rows * pack, wide).astype(bf),
        same_place,
        preferred_element_type=f32,
    )
    asked_shape = (rows * pack, wide)
    parity = (lax.broadcasted_iota(jnp.int32, asked_shape, 0) // pack) % 2
    lane_parity = (lax.broadcasted_iota(jnp.int32, asked_shape, 1) // size) % 2
    asked = jnp.where(parity == lane_parity, tiled, 0.0).astype(bf)
    for index in range(rows // 2):
        span = slice(2 * pack * index, 2 * pack * (index + 1))
        reads[span, :] = jnp.dot(asked[span], packed[index], preferred_element_type=f32)
    read_old = jnp.sum(jnp.where(only, reads[...].reshape(rows, pack, wide), 0.0), axis=1)
    query_key, query_norm = exact_dot([query * key, query * old_norm], same_head)
    divisor = jnp.maximum(
        jnp.abs(keep_old * query_norm + keep_new * query_key), jnp.exp(-new_max)
    )
    o_second = relay_plane(make_o, o_first)
    late = partial_b[line]
    for step in range(1, lines):
        pb_copies[step - 1].wait()
        late = late + arrived_b[step].astype(f32)
    value = late[:, :wide].astype(bf).astype(f32)
    outgate = late[:, wide:].astype(bf).astype(f32)
    read = (keep_old * read_old + keep_new * query_key * value) / divisor
    centered = read - exact_dot([read], same_head)[0] * (1.0 / size)
    variance = exact_dot([centered * centered], same_head)[0] * (1.0 / size)
    cell = (
        centered * lax.rsqrt(variance + 1e-06) * head_gain[...] * jax.nn.sigmoid(outgate)
    ).astype(bf)
    cell_mine[...] = cell
    swap = remote(cell_mine, cell_theirs, t_send.at[0], t_recv.at[0], partner)
    swap.start()
    pack_rows(cell, cell_out)
    cell_copies = scatter(cell_out, cell_near, c_send, c_recv)

    for copy in token_copies:
        copy.wait()
    token_swap = remote(token_near, token_far, t_send.at[1], t_recv.at[1], partner)
    token_swap.start()
    close_plane(o_first, o_second)
    out_slab = w_planes.at[:, my_rows]
    out_swap = remote(out_slab, out_slab, t_send.at[2], t_recv.at[2], partner)
    out_swap.start()

    lane_gates = gates_lane + pltpu.roll(gates_lane, LANES // 2, 1)
    lane_max, lane_old, lane_new = gate_math(
        lane_gates + ibias_lane,
        pltpu.roll(lane_gates, LANES - heads, 1) + fbias_lane,
        old_max_lane,
    )
    turned[:rows, :] = lane_max
    new_max_ref[...] = turned[...].T[:heads, :rows]
    row_lane = lax.broadcasted_iota(jnp.int32, (rows, pack, LANES), 1)
    lane = lax.broadcasted_iota(jnp.int32, (rows, pack, LANES), 2)
    chosen = ((row_lane == lane) | (row_lane == lane + heads)) & (lane < heads)

    def per_head(values):
        wider = jnp.broadcast_to(values[:, None, :], (rows, pack, LANES))
        return jnp.sum(jnp.where(chosen, wider, 0.0), axis=-1, keepdims=True)

    old_scale, new_scale = per_head(lane_old), per_head(lane_new)
    decay_ref[...] = jnp.broadcast_to(old_scale, decay_ref.shape)
    same = only | (row == head + heads)
    spread_key = jnp.where(same, jnp.broadcast_to(key[:, None, :], same.shape), 0.0)
    key_rows = jnp.dot(
        spread_key.reshape(rows * pack, wide).astype(bf),
        same_place[:, :size],
        preferred_element_type=f32,
    ).reshape(rows, pack, size)
    keys_ref[...] = key_rows
    new_norm_ref[...] = (
        old_scale[:, :heads] * state_norm[...] + (new_scale * key_rows)[:, :heads]
    )
    scaled = jnp.where(same, jnp.broadcast_to(value[:, None, :], same.shape) * new_scale, 0.0)
    coarse = scaled.astype(bf).astype(f32)
    left_ref[...] = jnp.where(row < heads, coarse, scaled - coarse)

    swap.wait()
    token_swap.wait()
    out_swap.wait()
    home_columns = pl.ds(pl.multiple_of(tp * part_wide, part_wide), part_wide)
    for owner in range(PLANE):
        added = jnp.dot(
            cell_mine[...], w_planes[owner, my_rows, home_columns], preferred_element_type=f32
        ) + jnp.dot(
            cell_theirs[...], w_planes[owner, other_rows, home_columns], preferred_element_type=f32
        )
        for index in range(lines // 2):
            start = (index * PLANE + owner) * columns
            resid[:, start : start + columns] = added[:, index * columns : (index + 1) * columns]
    resid[...] = (tokens[:, my_half].astype(f32) + resid[...]).astype(bf).astype(f32)

    extra_rows = area // 2
    lift_row = lax.broadcasted_iota(jnp.int32, (extra_rows, area), 0)
    lift_column = lax.broadcasted_iota(jnp.int32, (extra_rows, area), 1)
    lift_place = (lift_row // (SUB // 2)) * SUB + lift_row % (SUB // 2)
    lift_low = ones_where(lift_column == lift_place)
    lift_high = ones_where(lift_column == lift_place + SUB // 2)

    def unpack_rows(source):
        middle = source.shape[2] // 3
        flat = source[:, :, : 2 * middle].reshape(area, 2 * middle)
        extra = source[:, :, 2 * middle :].reshape(area, middle)
        joined = jnp.concatenate(
            [gather_rows(lift_low, extra), gather_rows(lift_high, extra)], axis=1
        )
        return jnp.concatenate([flat, joined], axis=0)

    token_rows[:, my_half] = unpack_rows(token_near)
    token_rows[:, other_half] = unpack_rows(token_far)

    forwards = []
    for step in range(count):
        source = lax.rem(ep + count - step, count)
        if step > 0:
            cell_copies[step - 1].wait()
        copy = remote(
            cell_near.at[source],
            cell_far.at[source],
            f_send.at[step],
            f_recv.at[step],
            partner,
        )
        copy.start()
        forwards.append(copy)
    near_rows = unpack_rows(cell_near)
    for copy in forwards:
        copy.wait()
    far_rows = unpack_rows(cell_far)
    squares = jnp.zeros((near_rows.shape[0], columns), f32)
    for owner in range(PLANE):
        added = jnp.dot(
            near_rows, w_planes[owner, my_rows], preferred_element_type=f32
        ) + jnp.dot(far_rows, w_planes[owner, other_rows], preferred_element_type=f32)
        for index in range(lines):
            start = (index * PLANE + owner) * columns
            place_columns = slice(start, start + columns)
            summed = (
                token_rows[:, place_columns].astype(f32)
                + added[:, index * columns : (index + 1) * columns]
            ).astype(bf)
            row_values[:, place_columns] = summed
            widened = summed.astype(f32)
            squares += widened * widened
    scale = lax.rsqrt(jnp.sum(squares, axis=-1, keepdims=True) * (1.0 / width) + 1e-06)
    row_values[...] = (row_values[...].astype(f32) * scale * ffn_gain[...]).astype(bf)
    for copy in late_loads[7:]:
        copy.wait()
    gate_pre = dot_t(row_values[...], w_gate[...])
    up_pre = dot_t(row_values[...], w_up[...])
    hidden = (gate_pre * jax.nn.sigmoid(gate_pre) * up_pre).astype(bf)
    down_send[...] = jnp.dot(
        hidden, w_down[:, other_half], preferred_element_type=f32
    ).astype(bf)
    swap = remote(down_send, down_recv, t_send.at[3], t_recv.at[3], partner)
    swap.start()
    kept = jnp.dot(hidden, w_down[:, my_half], preferred_element_type=f32).astype(bf)
    swap.wait()
    done = (kept.astype(f32) + down_recv[...].astype(f32)).astype(bf)
    finished[:, :, :half] = done[:area].reshape(count, SUB, half)
    turn = (((0,), (0,)), ((), ()))
    folded = lax.dot_general(
        lift_low, done[area:, : half // 2], turn, preferred_element_type=f32
    ) + lax.dot_general(lift_high, done[area:, half // 2 :], turn, preferred_element_type=f32)
    finished[:, :, half:] = folded.astype(bf).reshape(count, SUB, half // 2)
    return_copies = scatter(finished, returned, r_send, r_recv)
    for copy in return_copies:
        copy.wait()
    back = returned[:, :, :half].reshape(area, half)
    back_extra = returned[:, :, half:].reshape(area, half // 2)

    def combine(index, values):
        both = jnp.dot(chosen_in[index], values, preferred_element_type=f32)
        return both[:rows] + both[rows:]

    weighted = combine(0, back) + jnp.concatenate(
        [combine(1, back_extra), combine(2, back_extra)], axis=1
    )
    last_send[...] = (resid[...] + weighted).astype(bf)
    swap = remote(last_send, last_recv, t_send.at[4], t_recv.at[4], partner)
    swap.start()
    mixed_ref[:, my_half] = last_send[...]
    swap.wait()
    mixed_ref[:, other_half] = last_recv[...]


def update_kernel(
    mixed_ref,
    left_ref,
    keys_ref,
    decay_ref,
    norm_ref,
    max_ref,
    matrix_hbm,
    mixed_out,
    new_matrix_ref,
    new_norm_out,
    new_max_out,
    matrix,
    in_sems,
    out_sems,
):
    rows, heads, size, _ = matrix.shape
    wide = heads * size
    chunk = 8
    chunks = rows // chunk
    loads = []
    for index in range(chunks):
        part = pl.ds(index * chunk, chunk)
        copy = pltpu.make_async_copy(matrix_hbm.at[part], matrix.at[part], in_sems.at[index])
        copy.start()
        loads.append(copy)
    mixed_out[...] = mixed_ref[...]
    new_norm_out[...] = norm_ref[...]
    new_max_out[...] = max_ref[...]
    stores = []
    for index in range(chunks):
        loads[index].wait()

        @pl.loop(0, chunk // 4)
        def _(group):
            for inner in range(4):
                item = index * chunk + group * 4 + inner
                outer = lax.dot_general(
                    left_ref[item].astype(jnp.bfloat16),
                    keys_ref[item].astype(jnp.bfloat16),
                    (((0,), (0,)), ((), ())),
                    preferred_element_type=jnp.float32,
                ).reshape(heads, size, size)
                scale = decay_ref[item][:heads][:, None, :]
                matrix[item] = scale * matrix[item] + outer

        part = pl.ds(index * chunk, chunk)
        copy = pltpu.make_async_copy(matrix.at[part], new_matrix_ref.at[part], out_sems.at[index])
        copy.start()
        stores.append(copy)
    for copy in stores:
        copy.wait()


def layer_call(
    tokens,
    mix_gain,
    weight_list,
    igate_bias,
    fgate_bias,
    head_gain,
    w_out,
    state_matrix,
    state_norm,
    state_max,
    ffn_gain,
    expert_weights,
    routes,
    route_weights,
):
    rows, width = tokens.shape
    w_query, w_key, w_value, w_outgate, w_igate, w_fgate = weight_list
    depth, wide = w_query.shape
    count = lax.axis_size("ep")
    lines = count // PLANE
    heads = w_igate.shape[1]
    size = state_matrix.shape[3]
    half, block, pair, area = width // 2, depth * PLANE, 2 * wide, count * SUB
    slots = area + area // 2
    gate_t = jnp.swapaxes(expert_weights[0][0], 0, 1)
    up_t = jnp.swapaxes(expert_weights[1][0], 0, 1)
    down = expert_weights[2][0]
    vmem = pl.BlockSpec(memory_space=pltpu.VMEM)
    far = pl.BlockSpec(memory_space=pltpu.HBM)
    anywhere = pl.BlockSpec(memory_space=pl.ANY)
    dma = pltpu.SemaphoreType.DMA
    bf, f32 = jnp.bfloat16, jnp.float32
    shape = jax.ShapeDtypeStruct
    tile = (count, SUB, half + half // 2)
    thin = (count, SUB, wide + wide // 2)
    made = (
        shape((rows, width), bf),
        shape((rows, 2 * heads, wide), f32),
        shape((rows, 2 * heads, size), f32),
        shape((rows, 2 * heads, size), f32),
        shape(state_norm.shape, f32),
        shape((heads, rows), f32),
    )
    results = pl.pallas_call(
        functools.partial(layer_kernel, count),
        out_shape=made,
        in_specs=[far] * 21,
        out_specs=(vmem,) * 6,
        scratch_shapes=[
            pltpu.VMEM((rows, width), bf),
            pltpu.VMEM((1, width), f32),
            pltpu.VMEM((heads, depth), bf),
            pltpu.VMEM((heads, depth), bf),
            pltpu.VMEM((1, heads), f32),
            pltpu.VMEM((1, heads), f32),
            pltpu.VMEM((1, wide), f32),
            pltpu.VMEM(state_matrix.shape, f32),
            pltpu.VMEM(state_norm.shape, f32),
            pltpu.VMEM((heads, rows), f32),
            pltpu.VMEM((1, width), f32),
            pltpu.VMEM(gate_t.shape, bf),
            pltpu.VMEM(up_t.shape, bf),
            pltpu.VMEM(down.shape, bf),
            pltpu.VMEM((routes.shape[1], rows), jnp.int32),
            pltpu.VMEM((routes.shape[1], rows), f32),
            pltpu.VMEM((LANES, LANES), f32),
            pltpu.VMEM((PLANE, 2 * heads, depth), bf),
            pltpu.VMEM((LANES, block), bf),
            pltpu.VMEM((block, pair), bf),
            pltpu.VMEM((block, pair), bf),
            pltpu.VMEM((PLANE, pair, lines * w_out.shape[1]), bf),
            pltpu.VMEM((rows, width), bf),
            pltpu.VMEM((lines, rows, block), bf),
            pltpu.VMEM((lines, rows, pair + LANES), f32),
            pltpu.VMEM((lines, rows, pair), f32),
            pltpu.VMEM((lines, rows, pair + LANES), bf),
            pltpu.VMEM((lines, rows, pair), bf),
            pltpu.VMEM((lines, rows, pair + LANES), bf),
            pltpu.VMEM((lines, rows, pair), bf),
            pltpu.VMEM((rows // 2, wide, wide), bf),
            pltpu.VMEM((3, area, rows), bf),
            pltpu.VMEM((3, 2 * rows, area), bf),
            pltpu.VMEM(tile, bf),
            pltpu.VMEM(tile, bf),
            pltpu.VMEM(tile, bf),
            pltpu.VMEM((rows, wide), bf),
            pltpu.VMEM((rows, wide), bf),
            pltpu.VMEM(thin, bf),
            pltpu.VMEM(thin, bf),
            pltpu.VMEM(thin, bf),
            pltpu.VMEM((slots, width), bf),
            pltpu.VMEM((rows * 2 * heads, wide), f32),
            pltpu.VMEM((rows, half), f32),
            pltpu.VMEM((slots, width), bf),
            pltpu.VMEM((slots, half), bf),
            pltpu.VMEM((slots, half), bf),
            pltpu.VMEM(tile, bf),
            pltpu.VMEM(tile, bf),
            pltpu.VMEM((rows, half), bf),
            pltpu.VMEM((rows, half), bf),
            dma((11,)),
            dma((6,)),
            dma((6,)),
            dma((6,)),
            dma((6,)),
            dma((3,)),
            dma((3,)),
            dma((lines,)),
            dma((lines,)),
            dma((lines,)),
            dma((lines,)),
            dma((lines,)),
            dma((lines,)),
            dma((lines,)),
            dma((lines,)),
            dma((6,)),
            dma((6,)),
            dma((5,)),
            dma((5,)),
            dma((count,)),
            dma((count,)),
            dma((count,)),
            dma((count,)),
            dma((count,)),
            dma((count,)),
            dma((count,)),
            dma((count,)),
        ],
        compiler_params=pltpu.CompilerParams(
            collective_id=0, has_side_effects=True, vmem_limit_bytes=LAYER_BYTES
        ),
    )(
        tokens,
        mix_gain[None, :],
        w_query,
        w_key,
        w_value,
        w_outgate,
        jnp.swapaxes(w_igate, 0, 1),
        jnp.swapaxes(w_fgate, 0, 1),
        igate_bias[None, :],
        fgate_bias[None, :],
        head_gain[None, :],
        w_out,
        state_matrix,
        state_norm,
        jnp.swapaxes(state_max, 0, 1),
        ffn_gain[None, :],
        gate_t,
        up_t,
        down,
        jnp.swapaxes(routes, 0, 1),
        jnp.swapaxes(route_weights, 0, 1),
    )
    mixed, new_matrix, new_norm, new_max = pl.pallas_call(
        update_kernel,
        out_shape=(made[0], shape(state_matrix.shape, f32), made[4], made[5]),
        in_specs=[vmem] * 6 + [anywhere],
        out_specs=(vmem, anywhere, vmem, vmem),
        scratch_shapes=[
            pltpu.VMEM(state_matrix.shape, f32),
            dma((rows // 8,)),
            dma((rows // 8,)),
        ],
        compiler_params=pltpu.CompilerParams(vmem_limit_bytes=UPDATE_BYTES),
    )(*results, state_matrix)
    return mixed, new_matrix, new_norm, jnp.swapaxes(new_max, 0, 1)


def rms_scale(values_in, gain_vec):
    widened = values_in.astype(jnp.float32)
    return (
        widened * lax.rsqrt(jnp.mean(widened * widened, axis=-1, keepdims=True) + 1e-06) * gain_vec
    )


def memory_cell(
    query,
    key_row,
    value_row,
    outgate,
    input_pre,
    forget_pre,
    head_gain,
    state_matrix,
    state_norm,
    state_max,
):
    seq_rows, head_count = input_pre.shape
    head_size = query.shape[1] // head_count
    query_heads = query.astype(jnp.float32).reshape(seq_rows, head_count, head_size)
    key_heads = key_row.astype(jnp.float32).reshape(
        seq_rows, head_count, head_size
    ) * head_size ** (-0.5)
    value_heads = value_row.astype(jnp.float32).reshape(seq_rows, head_count, head_size)
    log_forget = jax.nn.log_sigmoid(forget_pre)
    new_max = jnp.maximum(log_forget + state_max, input_pre)
    keep_old = jnp.exp(log_forget + state_max - new_max)
    keep_new = jnp.exp(input_pre - new_max)
    new_matrix = (
        keep_old[:, :, None, None] * state_matrix
        + keep_new[:, :, None, None] * value_heads[:, :, :, None] * key_heads[:, :, None, :]
    )
    new_norm = keep_old[:, :, None] * state_norm + keep_new[:, :, None] * key_heads
    numerator = jnp.einsum(
        "bhvd,bhd->bhv", new_matrix, query_heads, precision=lax.Precision.HIGHEST
    )
    denominator = jnp.sum(new_norm * query_heads, axis=-1)
    cell_read = numerator / jnp.maximum(jnp.abs(denominator), jnp.exp(-new_max))[:, :, None]
    centered = cell_read - jnp.mean(cell_read, axis=-1, keepdims=True)
    variance = jnp.mean(centered * centered, axis=-1, keepdims=True)
    scaled_cell = (centered * lax.rsqrt(variance + 1e-06)).reshape(seq_rows, head_count * head_size)
    cell_out = (scaled_cell * head_gain * jax.nn.sigmoid(outgate.astype(jnp.float32))).astype(
        jnp.bfloat16
    )
    return (cell_out, new_matrix, new_norm, new_max)


def kernels_fit(tokens, w_query, w_igate, w_out, w_expert_gate, routes):
    ep_count = lax.axis_size("ep")
    rows, width = tokens.shape
    capacity = max(2, 2 * rows * routes.shape[1] // (w_expert_gate.shape[0] * ep_count))
    return (
        lax.axis_size("tp") == 2
        and ep_count % (2 * PLANE) == 0
        and w_query.shape[0] == LANES
        and w_query.shape[1] % LANES == 0
        and w_out.shape[1] % LANES == 0
        and width % (2 * LANES) == 0
        and rows % 16 == 0
        and w_igate.shape[1] == 4
        and rows <= LANES
        and w_expert_gate.shape[0] == 1
        and capacity == SUB + SUB // 2
        and ep_count * SUB == LANES
        and w_query.shape[1] == 2 * LANES
    )


def body(
    tokens,
    mix_gain,
    w_query,
    w_key,
    w_value,
    w_outgate,
    w_igate,
    w_fgate,
    igate_bias,
    fgate_bias,
    head_gain,
    w_out,
    state_matrix,
    state_norm,
    state_max,
    ffn_gain,
    w_expert_gate,
    w_expert_up,
    w_expert_down,
    routes,
    route_weights,
):
    seq_rows, width = tokens.shape
    weight_list = (w_query, w_key, w_value, w_outgate, w_igate, w_fgate)
    if kernels_fit(tokens, w_query, w_igate, w_out, w_expert_gate, routes):
        mixed, new_matrix, new_norm, new_max = layer_call(
            tokens,
            mix_gain,
            weight_list,
            igate_bias,
            fgate_bias,
            head_gain,
            w_out,
            state_matrix,
            state_norm,
            state_max,
            ffn_gain,
            (w_expert_gate, w_expert_up, w_expert_down),
            routes,
            route_weights,
        )
        return (mixed, new_matrix, new_norm, new_max)
    normed = rms_scale(tokens, mix_gain).astype(jnp.bfloat16)
    spread = lax.all_to_all(normed, "ep", split_axis=1, concat_axis=0, tiled=True)
    joined = jnp.concatenate(weight_list, axis=1)
    summed = lax.psum_scatter(
        jnp.dot(spread, joined, preferred_element_type=jnp.float32),
        "ep",
        scatter_dimension=0,
        tiled=True,
    )
    bounds = [0]
    for weight in weight_list:
        bounds.append(bounds[-1] + weight.shape[1])
    projected = tuple(
        (summed[:, bounds[index] : bounds[index + 1]] for index in range(len(weight_list)))
    )
    query = projected[0].astype(jnp.bfloat16)
    key_row = projected[1].astype(jnp.bfloat16)
    value_row = projected[2].astype(jnp.bfloat16)
    outgate = projected[3].astype(jnp.bfloat16)
    input_pre = projected[4] + igate_bias
    forget_pre = projected[5] + fgate_bias
    cell_out, new_matrix, new_norm, new_max = memory_cell(
        query,
        key_row,
        value_row,
        outgate,
        input_pre,
        forget_pre,
        head_gain,
        state_matrix,
        state_norm,
        state_max,
    )
    partial_out = jnp.dot(
        cell_out,
        lax.all_gather(w_out, "ep", axis=1, tiled=True),
        preferred_element_type=jnp.float32,
    )
    attended = lax.psum(partial_out.astype(jnp.bfloat16), "tp").astype(jnp.float32)
    resid = (tokens.astype(jnp.float32) + attended).astype(jnp.bfloat16)
    normed_two = rms_scale(resid, ffn_gain).astype(jnp.bfloat16)
    ep_count = lax.axis_size("ep")
    local_experts = w_expert_gate.shape[0]
    expert_total = local_experts * ep_count
    top_count = routes.shape[1]
    capacity = max(2, 2 * seq_rows * top_count // expert_total)
    flat_routes = routes.reshape(-1)
    onehot = (flat_routes[:, None] == jnp.arange(expert_total, dtype=jnp.int32)[None, :]).astype(
        jnp.int32
    )
    earlier = jnp.cumsum(onehot, axis=0, dtype=jnp.int32) - onehot
    slots = jnp.sum(onehot * earlier, axis=1, dtype=jnp.int32)
    targets = flat_routes * capacity + slots
    dispatch = (
        targets[:, None] == jnp.arange(expert_total * capacity, dtype=jnp.int32)[None, :]
    ).astype(jnp.bfloat16)
    route_rows = jnp.repeat(normed_two, top_count, axis=0)
    outgoing = jnp.einsum(
        "rs,rd->sd", dispatch, route_rows, preferred_element_type=jnp.float32
    ).astype(jnp.bfloat16)
    outgoing = outgoing.reshape(expert_total, capacity, width)
    received = lax.all_to_all(outgoing, "ep", split_axis=0, concat_axis=0, tiled=True)
    slot_count = received.shape[1]
    regrouped = received.reshape(ep_count, local_experts, slot_count, width)
    gate_pre = jnp.einsum(
        "nxcd,xdf->nxcf", regrouped, w_expert_gate, preferred_element_type=jnp.float32
    )
    up_pre = jnp.einsum(
        "nxcd,xdf->nxcf", regrouped, w_expert_up, preferred_element_type=jnp.float32
    )
    hidden = (jax.nn.silu(gate_pre) * up_pre).astype(jnp.bfloat16)
    partial_down = jnp.einsum(
        "nxcf,xfd->nxcd", hidden, w_expert_down, preferred_element_type=jnp.float32
    )
    expert_sum = lax.psum(partial_down.astype(jnp.bfloat16), "tp")
    finished = expert_sum.reshape(ep_count * local_experts, slot_count, width)
    returned = lax.all_to_all(finished, "ep", split_axis=0, concat_axis=0, tiled=True)
    picked = jnp.dot(
        dispatch,
        returned.reshape(expert_total * capacity, width),
        preferred_element_type=jnp.float32,
    )
    weighted = jnp.sum(
        picked.reshape(seq_rows, top_count, width) * route_weights[:, :, None], axis=1
    )
    mixed = (resid.astype(jnp.float32) + weighted).astype(jnp.bfloat16)
    return (mixed, new_matrix, new_norm, new_max)


def solution(mesh):
    placed = (
        P("ep", None),
        P(),
        P("ep", "tp"),
        P("ep", "tp"),
        P("ep", "tp"),
        P("ep", "tp"),
        P("ep", "tp"),
        P("ep", "tp"),
        P("tp"),
        P("tp"),
        P("tp"),
        P("tp", "ep"),
        P("ep", "tp", None, None),
        P("ep", "tp", None),
        P("ep", "tp"),
        P(),
        P("ep", None, "tp"),
        P("ep", None, "tp"),
        P("ep", "tp", None),
        P("ep", None),
        P("ep", None),
    )
    return jax.shard_map(
        body,
        mesh=mesh,
        in_specs=placed,
        out_specs=(P("ep", None), P("ep", "tp", None, None), P("ep", "tp", None), P("ep", "tp")),
        check_vma=False,
    )
```

```python
import functools

import jax
import jax.numpy as jnp
from jax import lax
from jax.experimental import pallas as pl
from jax.experimental.pallas import tpu as pltpu
from jax.sharding import PartitionSpec as P

MESH = pl.DeviceIdType.MESH
PLANE = 4
LANES = 128
SUB = 8
LAYER_BYTES = 40 * 1024 * 1024
UPDATE_BYTES = 12 * 1024 * 1024


def remote(src, dst, send_sem, recv_sem, target):
    return pltpu.make_async_remote_copy(
        src_ref=src,
        dst_ref=dst,
        send_sem=send_sem,
        recv_sem=recv_sem,
        device_id=target,
        device_id_type=MESH,
    )


def dot_t(left, right):
    return lax.dot_general(
        left, right, (((1,), (1,)), ((), ())), preferred_element_type=jnp.float32
    )


def fetch_all(pairs, sems):
    copies = []
    for index, (source, kept) in enumerate(pairs):
        copy = pltpu.make_async_copy(source, kept, sems.at[index])
        copy.start()
        copies.append(copy)
    return copies


def place(index, size):
    return pl.ds(pl.multiple_of(index * size, size), size)


def split_three(values):
    high = values.astype(jnp.bfloat16)
    rest = values - high.astype(jnp.float32)
    middle = rest.astype(jnp.bfloat16)
    return [high, middle, (rest - middle.astype(jnp.float32)).astype(jnp.bfloat16)]


def exact_dot(values, chosen):
    rows = values[0].shape[0]
    parts = [part for value in values for part in split_three(value)]
    product = jnp.dot(
        jnp.concatenate(parts, axis=0), chosen, preferred_element_type=jnp.float32
    )
    results = []
    for index in range(len(values)):
        start = 3 * index * rows
        pieces = [product[start + rows * part : start + rows * (part + 1)] for part in range(3)]
        results.append(pieces[0] + pieces[1] + pieces[2])
    return results


def ones_where(condition):
    return jnp.where(condition, 1.0, 0.0).astype(jnp.bfloat16)


def gather_rows(chosen, values):
    return jnp.dot(chosen, values, preferred_element_type=jnp.float32).astype(jnp.bfloat16)


def layer_kernel(
    count,
    tokens_hbm,
    mix_gain_hbm,
    wq_hbm,
    wk_hbm,
    wv_hbm,
    wg_hbm,
    igate_hbm,
    fgate_hbm,
    ibias_hbm,
    fbias_hbm,
    head_gain_hbm,
    w_out_hbm,
    matrix_hbm,
    norm_hbm,
    max_hbm,
    ffn_gain_hbm,
    w_gate_hbm,
    w_up_hbm,
    w_down_hbm,
    routes_hbm,
    route_weights_hbm,
    mixed_ref,
    left_ref,
    keys_ref,
    decay_ref,
    new_norm_ref,
    new_max_ref,
    tokens,
    mix_gain,
    igate,
    fgate,
    ibias,
    fbias,
    head_gain,
    matrix,
    state_norm,
    state_max,
    ffn_gain,
    w_gate,
    w_up,
    w_down,
    routes,
    route_weights,
    turned,
    gate_rows,
    gate_t,
    weights_a,
    weights_b,
    w_planes,
    normed,
    spread,
    partial_a,
    partial_b,
    outgoing_a,
    outgoing_b,
    arrived_a,
    arrived_b,
    packed,
    chosen_out,
    chosen_in,
    token_out,
    token_near,
    token_far,
    cell_mine,
    cell_theirs,
    cell_out,
    cell_near,
    cell_far,
    token_rows,
    reads,
    resid,
    row_values,
    down_send,
    down_recv,
    finished,
    returned,
    last_send,
    last_recv,
    local_sem,
    a_send,
    a_recv,
    b_send,
    b_recv,
    g_send,
    g_recv,
    x_send,
    x_recv,
    z_send,
    z_recv,
    pa_send,
    pa_recv,
    pb_send,
    pb_recv,
    o_send,
    o_recv,
    t_send,
    t_recv,
    k_send,
    k_recv,
    c_send,
    c_recv,
    f_send,
    f_recv,
    r_send,
    r_recv,
):
    bf, f32 = jnp.bfloat16, jnp.float32
    ep, tp = lax.axis_index("ep"), lax.axis_index("tp")
    lines = count // PLANE
    line, spot = ep // PLANE, ep % PLANE
    rows, width = tokens.shape
    half = width // 2
    depth = wq_hbm.shape[0]
    block = depth * PLANE
    heads = igate.shape[0]
    size = matrix.shape[3]
    wide = heads * size
    pair = 2 * wide
    area = count * SUB
    top = route_weights.shape[0]
    columns = w_out_hbm.shape[1]
    slab = lines * columns
    part_wide = slab // 2
    partner = (ep, 1 - tp)
    beside = spot + 1 - 2 * (spot % 2)
    across = lax.rem(spot + 2, PLANE)
    beside_peer = (line * PLANE + beside, tp)
    across_peer = (line * PLANE + across, tp)
    corner_peer = (line * PLANE + PLANE - 1 - spot, tp)
    my_half, other_half = place(tp, half), place(1 - tp, half)
    my_rows, other_rows = place(tp, wide), place(1 - tp, wide)
    own_rows = place(spot, depth)

    def line_peer(step):
        other = lax.rem(line + step, lines)
        return other, (other * PLANE + spot, tp)

    first_loads = fetch_all(
        (
            (wq_hbm, weights_a.at[own_rows, :wide]),
            (wk_hbm, weights_a.at[own_rows, wide:]),
            (igate_hbm, igate),
            (fgate_hbm, fgate),
            (wv_hbm, weights_b.at[own_rows, :wide]),
            (wg_hbm, weights_b.at[own_rows, wide:]),
            (tokens_hbm, tokens),
            (mix_gain_hbm, mix_gain),
            (w_out_hbm, w_planes.at[spot, my_rows, place(line, columns)]),
            (routes_hbm, routes),
            (route_weights_hbm, route_weights),
        ),
        local_sem,
    )
    barrier = pltpu.get_barrier_semaphore()
    for step in range(1, count):
        pl.semaphore_signal(
            barrier, inc=1, device_id=(lax.rem(ep + step, count), tp), device_id_type=MESH
        )
    pl.semaphore_signal(barrier, inc=1, device_id=partner, device_id_type=MESH)
    turned[...] = jnp.zeros_like(turned)
    gate_t[...] = jnp.zeros_like(gate_t)
    for copy in first_loads[:4]:
        copy.wait()
    turned[:heads, :] = igate[...].astype(f32)
    turned[heads : 2 * heads, :] = fgate[...].astype(f32)
    gate_rows[spot] = turned[: 2 * heads, :].astype(bf)
    pl.semaphore_wait(barrier, count)

    def plane_copies(buffer_view, send, recv):
        def make(owner, part, slot, target):
            view = buffer_view(owner, part)
            return remote(view, view, send.at[slot], recv.at[slot], target)

        return make

    def weight_view(buffer):
        def view(owner, part):
            tall = depth // 2
            return buffer.at[pl.ds(pl.multiple_of(owner * depth + part * tall, tall), tall)]

        return view

    def out_view(owner, part):
        return w_planes.at[owner, my_rows, part * part_wide : (part + 1) * part_wide]

    def open_plane(make):
        first = [
            make(spot, 0, 0, beside_peer),
            make(spot, 1, 2, across_peer),
            make(spot, 1, 1, beside_peer),
            make(spot, 0, 3, across_peer),
        ]
        for copy in first:
            copy.start()
        return first

    def relay_plane(make, first):
        first[0].wait_recv()
        ahead = make(beside, 0, 4, across_peer)
        ahead.start()
        first[1].wait_recv()
        aside = make(across, 1, 5, beside_peer)
        aside.start()
        return [ahead, aside]

    def close_plane(first, second):
        first[2].wait_recv()
        first[3].wait_recv()
        for copy in first:
            copy.wait_send()
        for copy in second:
            copy.wait()

    make_a = plane_copies(weight_view(weights_a), a_send, a_recv)
    make_b = plane_copies(weight_view(weights_b), b_send, b_recv)
    make_o = plane_copies(out_view, o_send, o_recv)
    a_first = open_plane(make_a)
    gate_copies = []
    for slot, target in enumerate((beside_peer, across_peer, corner_peer)):
        view = gate_rows.at[spot]
        copy = remote(view, view, g_send.at[slot], g_recv.at[slot], target)
        copy.start()
        gate_copies.append(copy)
    for copy in first_loads[4:9]:
        copy.wait()
    widened = tokens[...].astype(f32)
    scale = lax.rsqrt(jnp.mean(widened * widened, axis=-1, keepdims=True) + 1e-06)
    normed[...] = (widened * scale * mix_gain[...]).astype(bf)
    x_copies, z_copies = [], []
    for step in range(1, lines):
        other, target = line_peer(step)
        copy = remote(
            normed.at[:, place(other, block)],
            spread.at[line],
            x_send.at[step],
            x_recv.at[step],
            target,
        )
        copy.start()
        x_copies.append(copy)
    for step in range(1, lines):
        view = w_planes.at[spot, my_rows, place(line, columns)]
        copy = remote(view, view, z_send.at[step], z_recv.at[step], line_peer(step)[1])
        copy.start()
        z_copies.append(copy)
    spread[line] = normed[:, place(line, block)]
    for copy in first_loads[9:]:
        copy.wait()
    late_loads = fetch_all(
        (
            (matrix_hbm, matrix),
            (norm_hbm, state_norm),
            (max_hbm, state_max),
            (ibias_hbm, ibias),
            (fbias_hbm, fbias),
            (head_gain_hbm, head_gain),
            (ffn_gain_hbm, ffn_gain),
            (w_gate_hbm, w_gate),
            (w_up_hbm, w_up),
            (w_down_hbm, w_down),
        ),
        local_sem,
    )

    slot_row = lax.broadcasted_iota(jnp.int32, (area, rows), 0).astype(f32)
    expert = lax.broadcasted_iota(jnp.int32, (count, rows), 0).astype(f32)
    before = jnp.where(
        lax.broadcasted_iota(jnp.int32, (rows, rows), 0)
        < lax.broadcasted_iota(jnp.int32, (rows, rows), 1),
        1.0,
        0.0,
    )
    taken = jnp.zeros((count, 1), f32)
    sent = [jnp.zeros((area, rows), f32) for _ in range(3)]
    mixes = [jnp.zeros((area, rows), f32) for _ in range(3)]
    for k in range(top):
        named = routes[k : k + 1, :].astype(f32)
        match = jnp.where(expert == named, 1.0, 0.0)
        earlier = jnp.dot(match, before, preferred_element_type=f32) + taken
        taken = taken + jnp.sum(match, axis=1, keepdims=True)
        position = jnp.sum(match * earlier, axis=0, keepdims=True)
        low = jnp.where(position < SUB, named * SUB + position, -1000.0)
        high = jnp.where(position < SUB, -1000.0, named * SUB + position - SUB)
        for index, target in enumerate((low, high, high + SUB // 2)):
            hit = slot_row == target
            sent[index] += jnp.where(hit, 1.0, 0.0)
            mixes[index] += jnp.where(hit, route_weights[k : k + 1, :], 0.0)
    for index in range(3):
        chosen_out[index] = sent[index].astype(bf)
        coarse = mixes[index].astype(bf).astype(f32)
        joined = jnp.concatenate(
            [coarse, mixes[index] - coarse, jnp.zeros((area, area - 2 * rows), f32)], axis=1
        )
        chosen_in[index] = joined.T[: 2 * rows].astype(bf)

    def pack_rows(values, target):
        middle = values.shape[1] // 2
        target[:, :, : 2 * middle] = gather_rows(chosen_out[0], values).reshape(
            count, SUB, 2 * middle
        )
        extra = jnp.dot(chosen_out[1], values[:, :middle], preferred_element_type=f32)
        extra += jnp.dot(chosen_out[2], values[:, middle:], preferred_element_type=f32)
        target[:, :, 2 * middle :] = extra.astype(bf).reshape(count, SUB, middle)

    a_second = relay_plane(make_a, a_first)
    b_first = open_plane(make_b)
    pack_rows(tokens[:, my_half], token_out)
    late_loads[0].wait()

    def pack_matrix(start, stop):
        @pl.loop(start, stop)
        def _(index):
            item = 2 * index
            joined = jnp.concatenate(
                [matrix[item].reshape(wide, size), matrix[item + 1].reshape(wide, size)], axis=1
            )
            flipped = joined.T
            upper = flipped.astype(bf)
            packed[index, : 2 * size] = upper
            packed[index, 2 * size :] = (flipped - upper.astype(f32)).astype(bf)

    pack_matrix(0, rows // 4)
    for copy in gate_copies:
        copy.wait()
    for owner in range(PLANE):
        part = gate_rows[owner]
        gate_t[: 2 * heads, owner * depth : (owner + 1) * depth] = part
        gate_t[LANES // 2 : LANES // 2 + 2 * heads, owner * depth : (owner + 1) * depth] = part
    for copy in x_copies:
        copy.wait()
    close_plane(a_first, a_second)
    arranged = spread[...].reshape(lines * rows, block)
    product = jnp.dot(arranged, weights_a[...], preferred_element_type=f32)
    gates = dot_t(arranged, gate_t[...])
    coarse = gates.astype(bf).astype(f32)
    first = lax.broadcasted_iota(jnp.int32, gates.shape, 1) < LANES // 2
    picked = jnp.where(first, coarse, gates - coarse).astype(bf)
    outgoing_a[:, :, :pair] = product.astype(bf).reshape(lines, rows, pair)
    outgoing_a[:, :, pair:] = picked.reshape(lines, rows, LANES)
    partial_a[:, :, :pair] = product.reshape(lines, rows, pair)
    partial_a[:, :, pair:] = jnp.where(first, gates, 0.0).reshape(lines, rows, LANES)

    def send_partials(outgoing, arrived, send, recv):
        copies = []
        for step in range(1, lines):
            other, target = line_peer(step)
            copy = remote(
                outgoing.at[other], arrived.at[step], send.at[step], recv.at[step], target
            )
            copy.start()
            copies.append(copy)
        return copies

    pa_copies = send_partials(outgoing_a, arrived_a, pa_send, pa_recv)
    b_second = relay_plane(make_b, b_first)
    pack_matrix(rows // 4, rows // 2)
    for copy in late_loads[1:7]:
        copy.wait()

    chosen_head = ones_where(
        lax.broadcasted_iota(jnp.int32, (LANES, pair), 0) % (LANES // 2)
        == lax.broadcasted_iota(jnp.int32, (LANES, pair), 1) // size
    )
    same_head = ones_where(
        lax.broadcasted_iota(jnp.int32, (wide, wide), 0) // size
        == lax.broadcasted_iota(jnp.int32, (wide, wide), 1) // size
    )
    same_place = ones_where(
        lax.broadcasted_iota(jnp.int32, (wide, wide), 0) % size
        == lax.broadcasted_iota(jnp.int32, (wide, wide), 1) % size
    )
    turned[...] = jnp.zeros_like(turned)
    turned[:heads, :rows] = state_max[...]
    old_max_lane = turned[...].T[:rows]
    turned[...] = jnp.zeros_like(turned)
    turned[0:1, :heads] = ibias[...]
    turned[1:2, :heads] = fbias[...]
    ibias_lane, fbias_lane = turned[0:1, :], turned[1:2, :]
    biases = jnp.concatenate(
        [ibias_lane + pltpu.roll(fbias_lane, heads, 1), jnp.zeros((7, LANES), f32)], axis=0
    )
    old_max_wide, bias_wide = (
        exact_dot([old_max_lane], chosen_head)[0][:, :wide],
        exact_dot([biases], chosen_head)[0][:1],
    )
    old_norm = jnp.concatenate([state_norm[:, head, :] for head in range(heads)], axis=1)

    for copy in z_copies:
        copy.wait()
    close_plane(b_first, b_second)
    product = jnp.dot(arranged, weights_b[...], preferred_element_type=f32)
    outgoing_b[...] = product.astype(bf).reshape(lines, rows, pair)
    partial_b[...] = product.reshape(lines, rows, pair)
    pb_copies = send_partials(outgoing_b, arrived_b, pb_send, pb_recv)
    o_first = open_plane(make_o)

    def scatter(source, near, send, recv):
        copies = []
        for step in range(1, count):
            other = lax.rem(ep + step, count)
            copy = remote(
                source.at[other], near.at[ep], send.at[step], recv.at[step], (other, tp)
            )
            copy.start()
            copies.append(copy)
        near[ep] = source[ep]
        return copies

    token_copies = scatter(token_out, token_near, k_send, k_recv)

    total = partial_a[line]
    for step in range(1, lines):
        pa_copies[step - 1].wait()
        total = total + arrived_a[step].astype(f32)
    gates_lane = total[:, pair:]
    gates_wide = exact_dot([gates_lane], chosen_head)[0]

    def gate_math(input_pre, forget_pre, old_max):
        log_forget = jnp.minimum(forget_pre, 0.0) - jnp.log(1.0 + jnp.exp(-jnp.abs(forget_pre)))
        new_max = jnp.maximum(log_forget + old_max, input_pre)
        return new_max, jnp.exp(log_forget + old_max - new_max), jnp.exp(input_pre - new_max)

    new_max, keep_old, keep_new = gate_math(
        gates_wide[:, :wide] + bias_wide[:, :wide],
        gates_wide[:, wide:] + bias_wide[:, wide:],
        old_max_wide,
    )
    query = total[:, :wide].astype(bf).astype(f32)
    key = total[:, wide:pair].astype(bf).astype(f32) * size ** (-0.5)
    pack = 2 * heads
    row = lax.broadcasted_iota(jnp.int32, (rows, pack, wide), 1)
    head = lax.broadcasted_iota(jnp.int32, (rows, pack, wide), 2) // size
    only = row == head
    spread_query = jnp.where(only, jnp.broadcast_to(query[:, None, :], only.shape), 0.0)
    tiled = jnp.dot(
        spread_query.reshape(rows * pack, wide).astype(bf),
        same_place,
        preferred_element_type=f32,
    )
    asked_shape = (rows * pack, wide)
    parity = (lax.broadcasted_iota(jnp.int32, asked_shape, 0) // pack) % 2
    lane_parity = (lax.broadcasted_iota(jnp.int32, asked_shape, 1) // size) % 2
    asked = jnp.where(parity == lane_parity, tiled, 0.0).astype(bf)
    for index in range(rows // 2):
        span = slice(2 * pack * index, 2 * pack * (index + 1))
        reads[span, :] = jnp.dot(asked[span], packed[index], preferred_element_type=f32)
    read_old = jnp.sum(jnp.where(only, reads[...].reshape(rows, pack, wide), 0.0), axis=1)
    query_key, query_norm = exact_dot([query * key, query * old_norm], same_head)
    divisor = jnp.maximum(
        jnp.abs(keep_old * query_norm + keep_new * query_key), jnp.exp(-new_max)
    )
    o_second = relay_plane(make_o, o_first)
    late = partial_b[line]
    for step in range(1, lines):
        pb_copies[step - 1].wait()
        late = late + arrived_b[step].astype(f32)
    value = late[:, :wide].astype(bf).astype(f32)
    outgate = late[:, wide:].astype(bf).astype(f32)
    read = (keep_old * read_old + keep_new * query_key * value) / divisor
    centered = read - exact_dot([read], same_head)[0] * (1.0 / size)
    variance = exact_dot([centered * centered], same_head)[0] * (1.0 / size)
    cell = (
        centered * lax.rsqrt(variance + 1e-06) * head_gain[...] * jax.nn.sigmoid(outgate)
    ).astype(bf)
    cell_mine[...] = cell
    swap = remote(cell_mine, cell_theirs, t_send.at[0], t_recv.at[0], partner)
    swap.start()
    pack_rows(cell, cell_out)
    cell_copies = scatter(cell_out, cell_near, c_send, c_recv)

    for copy in token_copies:
        copy.wait()
    token_swap = remote(token_near, token_far, t_send.at[1], t_recv.at[1], partner)
    token_swap.start()
    close_plane(o_first, o_second)
    out_slab = w_planes.at[:, my_rows]
    out_swap = remote(out_slab, out_slab, t_send.at[2], t_recv.at[2], partner)
    out_swap.start()

    lane_gates = gates_lane + pltpu.roll(gates_lane, LANES // 2, 1)
    lane_max, lane_old, lane_new = gate_math(
        lane_gates + ibias_lane,
        pltpu.roll(lane_gates, LANES - heads, 1) + fbias_lane,
        old_max_lane,
    )
    turned[:rows, :] = lane_max
    new_max_ref[...] = turned[...].T[:heads, :rows]
    row_lane = lax.broadcasted_iota(jnp.int32, (rows, pack, LANES), 1)
    lane = lax.broadcasted_iota(jnp.int32, (rows, pack, LANES), 2)
    chosen = ((row_lane == lane) | (row_lane == lane + heads)) & (lane < heads)

    def per_head(values):
        wider = jnp.broadcast_to(values[:, None, :], (rows, pack, LANES))
        return jnp.sum(jnp.where(chosen, wider, 0.0), axis=-1, keepdims=True)

    old_scale, new_scale = per_head(lane_old), per_head(lane_new)
    decay_ref[...] = jnp.broadcast_to(old_scale, decay_ref.shape)
    same = only | (row == head + heads)
    spread_key = jnp.where(same, jnp.broadcast_to(key[:, None, :], same.shape), 0.0)
    key_rows = jnp.dot(
        spread_key.reshape(rows * pack, wide).astype(bf),
        same_place[:, :size],
        preferred_element_type=f32,
    ).reshape(rows, pack, size)
    keys_ref[...] = key_rows
    new_norm_ref[...] = (
        old_scale[:, :heads] * state_norm[...] + (new_scale * key_rows)[:, :heads]
    )
    scaled = jnp.where(same, jnp.broadcast_to(value[:, None, :], same.shape) * new_scale, 0.0)
    coarse = scaled.astype(bf).astype(f32)
    left_ref[...] = jnp.where(row < heads, coarse, scaled - coarse)

    swap.wait()
    token_swap.wait()
    out_swap.wait()
    home_columns = pl.ds(pl.multiple_of(tp * part_wide, part_wide), part_wide)
    for owner in range(PLANE):
        added = jnp.dot(
            cell_mine[...], w_planes[owner, my_rows, home_columns], preferred_element_type=f32
        ) + jnp.dot(
            cell_theirs[...], w_planes[owner, other_rows, home_columns], preferred_element_type=f32
        )
        for index in range(lines // 2):
            start = (index * PLANE + owner) * columns
            resid[:, start : start + columns] = added[:, index * columns : (index + 1) * columns]
    resid[...] = (tokens[:, my_half].astype(f32) + resid[...]).astype(bf).astype(f32)

    extra_rows = area // 2
    lift_row = lax.broadcasted_iota(jnp.int32, (extra_rows, area), 0)
    lift_column = lax.broadcasted_iota(jnp.int32, (extra_rows, area), 1)
    lift_place = (lift_row // (SUB // 2)) * SUB + lift_row % (SUB // 2)
    lift_low = ones_where(lift_column == lift_place)
    lift_high = ones_where(lift_column == lift_place + SUB // 2)

    def unpack_rows(source):
        middle = source.shape[2] // 3
        flat = source[:, :, : 2 * middle].reshape(area, 2 * middle)
        extra = source[:, :, 2 * middle :].reshape(area, middle)
        joined = jnp.concatenate(
            [gather_rows(lift_low, extra), gather_rows(lift_high, extra)], axis=1
        )
        return jnp.concatenate([flat, joined], axis=0)

    token_rows[:, my_half] = unpack_rows(token_near)
    token_rows[:, other_half] = unpack_rows(token_far)

    forwards = []
    for step in range(count):
        source = lax.rem(ep + count - step, count)
        if step > 0:
            cell_copies[step - 1].wait()
        copy = remote(
            cell_near.at[source],
            cell_far.at[source],
            f_send.at[step],
            f_recv.at[step],
            partner,
        )
        copy.start()
        forwards.append(copy)
    near_rows = unpack_rows(cell_near)
    for copy in forwards:
        copy.wait()
    far_rows = unpack_rows(cell_far)
    squares = jnp.zeros((near_rows.shape[0], columns), f32)
    for owner in range(PLANE):
        added = jnp.dot(
            near_rows, w_planes[owner, my_rows], preferred_element_type=f32
        ) + jnp.dot(far_rows, w_planes[owner, other_rows], preferred_element_type=f32)
        for index in range(lines):
            start = (index * PLANE + owner) * columns
            place_columns = slice(start, start + columns)
            summed = (
                token_rows[:, place_columns].astype(f32)
                + added[:, index * columns : (index + 1) * columns]
            ).astype(bf)
            row_values[:, place_columns] = summed
            widened = summed.astype(f32)
            squares += widened * widened
    scale = lax.rsqrt(jnp.sum(squares, axis=-1, keepdims=True) * (1.0 / width) + 1e-06)
    row_values[...] = (row_values[...].astype(f32) * scale * ffn_gain[...]).astype(bf)
    for copy in late_loads[7:]:
        copy.wait()
    gate_pre = dot_t(row_values[...], w_gate[...])
    up_pre = dot_t(row_values[...], w_up[...])
    hidden = (gate_pre * jax.nn.sigmoid(gate_pre) * up_pre).astype(bf)
    down_send[...] = jnp.dot(
        hidden, w_down[:, other_half], preferred_element_type=f32
    ).astype(bf)
    swap = remote(down_send, down_recv, t_send.at[3], t_recv.at[3], partner)
    swap.start()
    kept = jnp.dot(hidden, w_down[:, my_half], preferred_element_type=f32).astype(bf)
    swap.wait()
    done = (kept.astype(f32) + down_recv[...].astype(f32)).astype(bf)
    finished[:, :, :half] = done[:area].reshape(count, SUB, half)
    turn = (((0,), (0,)), ((), ()))
    folded = lax.dot_general(
        lift_low, done[area:, : half // 2], turn, preferred_element_type=f32
    ) + lax.dot_general(lift_high, done[area:, half // 2 :], turn, preferred_element_type=f32)
    finished[:, :, half:] = folded.astype(bf).reshape(count, SUB, half // 2)
    return_copies = scatter(finished, returned, r_send, r_recv)
    for copy in return_copies:
        copy.wait()
    back = returned[:, :, :half].reshape(area, half)
    back_extra = returned[:, :, half:].reshape(area, half // 2)

    def combine(index, values):
        both = jnp.dot(chosen_in[index], values, preferred_element_type=f32)
        return both[:rows] + both[rows:]

    weighted = combine(0, back) + jnp.concatenate(
        [combine(1, back_extra), combine(2, back_extra)], axis=1
    )
    last_send[...] = (resid[...] + weighted).astype(bf)
    swap = remote(last_send, last_recv, t_send.at[4], t_recv.at[4], partner)
    swap.start()
    mixed_ref[:, my_half] = last_send[...]
    swap.wait()
    mixed_ref[:, other_half] = last_recv[...]


def update_kernel(
    mixed_ref,
    left_ref,
    keys_ref,
    decay_ref,
    norm_ref,
    max_ref,
    matrix_hbm,
    mixed_out,
    new_matrix_ref,
    new_norm_out,
    new_max_out,
    matrix,
    in_sems,
    out_sems,
):
    rows, heads, size, _ = matrix.shape
    wide = heads * size
    chunk = 8
    chunks = rows // chunk
    loads = []
    for index in range(chunks):
        part = pl.ds(index * chunk, chunk)
        copy = pltpu.make_async_copy(matrix_hbm.at[part], matrix.at[part], in_sems.at[index])
        copy.start()
        loads.append(copy)
    mixed_out[...] = mixed_ref[...]
    new_norm_out[...] = norm_ref[...]
    new_max_out[...] = max_ref[...]
    stores = []
    for index in range(chunks):
        loads[index].wait()

        @pl.loop(0, chunk // 4)
        def _(group):
            for inner in range(4):
                item = index * chunk + group * 4 + inner
                outer = lax.dot_general(
                    left_ref[item].astype(jnp.bfloat16),
                    keys_ref[item].astype(jnp.bfloat16),
                    (((0,), (0,)), ((), ())),
                    preferred_element_type=jnp.float32,
                ).reshape(heads, size, size)
                scale = decay_ref[item][:heads][:, None, :]
                matrix[item] = scale * matrix[item] + outer

        part = pl.ds(index * chunk, chunk)
        copy = pltpu.make_async_copy(matrix.at[part], new_matrix_ref.at[part], out_sems.at[index])
        copy.start()
        stores.append(copy)
    for copy in stores:
        copy.wait()


def layer_call(
    tokens,
    mix_gain,
    weight_list,
    igate_bias,
    fgate_bias,
    head_gain,
    w_out,
    state_matrix,
    state_norm,
    state_max,
    ffn_gain,
    expert_weights,
    routes,
    route_weights,
):
    rows, width = tokens.shape
    w_query, w_key, w_value, w_outgate, w_igate, w_fgate = weight_list
    depth, wide = w_query.shape
    count = lax.axis_size("ep")
    lines = count // PLANE
    heads = w_igate.shape[1]
    size = state_matrix.shape[3]
    half, block, pair, area = width // 2, depth * PLANE, 2 * wide, count * SUB
    slots = area + area // 2
    gate_t = jnp.swapaxes(expert_weights[0][0], 0, 1)
    up_t = jnp.swapaxes(expert_weights[1][0], 0, 1)
    down = expert_weights[2][0]
    vmem = pl.BlockSpec(memory_space=pltpu.VMEM)
    far = pl.BlockSpec(memory_space=pltpu.HBM)
    anywhere = pl.BlockSpec(memory_space=pl.ANY)
    dma = pltpu.SemaphoreType.DMA
    bf, f32 = jnp.bfloat16, jnp.float32
    shape = jax.ShapeDtypeStruct
    tile = (count, SUB, half + half // 2)
    thin = (count, SUB, wide + wide // 2)
    made = (
        shape((rows, width), bf),
        shape((rows, 2 * heads, wide), f32),
        shape((rows, 2 * heads, size), f32),
        shape((rows, 2 * heads, size), f32),
        shape(state_norm.shape, f32),
        shape((heads, rows), f32),
    )
    operands = (
        tokens,
        mix_gain[None, :],
        w_query,
        w_key,
        w_value,
        w_outgate,
        jnp.swapaxes(w_igate, 0, 1),
        jnp.swapaxes(w_fgate, 0, 1),
        igate_bias[None, :],
        fgate_bias[None, :],
        head_gain[None, :],
        w_out,
        state_matrix,
        state_norm,
        jnp.swapaxes(state_max, 0, 1),
        ffn_gain[None, :],
        gate_t,
        up_t,
        down,
        jnp.swapaxes(routes, 0, 1),
        jnp.swapaxes(route_weights, 0, 1),
    )
    results = pl.pallas_call(
        functools.partial(layer_kernel, count),
        out_shape=made,
        in_specs=[far] * 21,
        out_specs=(vmem,) * 6,
        scratch_shapes=[
            pltpu.VMEM((rows, width), bf),
            pltpu.VMEM((1, width), f32),
            pltpu.VMEM((heads, depth), bf),
            pltpu.VMEM((heads, depth), bf),
            pltpu.VMEM((1, heads), f32),
            pltpu.VMEM((1, heads), f32),
            pltpu.VMEM((1, wide), f32),
            pltpu.VMEM(state_matrix.shape, f32),
            pltpu.VMEM(state_norm.shape, f32),
            pltpu.VMEM((heads, rows), f32),
            pltpu.VMEM((1, width), f32),
            pltpu.VMEM(gate_t.shape, bf),
            pltpu.VMEM(up_t.shape, bf),
            pltpu.VMEM(down.shape, bf),
            pltpu.VMEM((routes.shape[1], rows), jnp.int32),
            pltpu.VMEM((routes.shape[1], rows), f32),
            pltpu.VMEM((LANES, LANES), f32),
            pltpu.VMEM((PLANE, 2 * heads, depth), bf),
            pltpu.VMEM((LANES, block), bf),
            pltpu.VMEM((block, pair), bf),
            pltpu.VMEM((block, pair), bf),
            pltpu.VMEM((PLANE, pair, lines * w_out.shape[1]), bf),
            pltpu.VMEM((rows, width), bf),
            pltpu.VMEM((lines, rows, block), bf),
            pltpu.VMEM((lines, rows, pair + LANES), f32),
            pltpu.VMEM((lines, rows, pair), f32),
            pltpu.VMEM((lines, rows, pair + LANES), bf),
            pltpu.VMEM((lines, rows, pair), bf),
            pltpu.VMEM((lines, rows, pair + LANES), bf),
            pltpu.VMEM((lines, rows, pair), bf),
            pltpu.VMEM((rows // 2, wide, wide), bf),
            pltpu.VMEM((3, area, rows), bf),
            pltpu.VMEM((3, 2 * rows, area), bf),
            pltpu.VMEM(tile, bf),
            pltpu.VMEM(tile, bf),
            pltpu.VMEM(tile, bf),
            pltpu.VMEM((rows, wide), bf),
            pltpu.VMEM((rows, wide), bf),
            pltpu.VMEM(thin, bf),
            pltpu.VMEM(thin, bf),
            pltpu.VMEM(thin, bf),
            pltpu.VMEM((slots, width), bf),
            pltpu.VMEM((rows * 2 * heads, wide), f32),
            pltpu.VMEM((rows, half), f32),
            pltpu.VMEM((slots, width), bf),
            pltpu.VMEM((slots, half), bf),
            pltpu.VMEM((slots, half), bf),
            pltpu.VMEM(tile, bf),
            pltpu.VMEM(tile, bf),
            pltpu.VMEM((rows, half), bf),
            pltpu.VMEM((rows, half), bf),
            dma((11,)),
            dma((6,)),
            dma((6,)),
            dma((6,)),
            dma((6,)),
            dma((3,)),
            dma((3,)),
            dma((lines,)),
            dma((lines,)),
            dma((lines,)),
            dma((lines,)),
            dma((lines,)),
            dma((lines,)),
            dma((lines,)),
            dma((lines,)),
            dma((6,)),
            dma((6,)),
            dma((5,)),
            dma((5,)),
            dma((count,)),
            dma((count,)),
            dma((count,)),
            dma((count,)),
            dma((count,)),
            dma((count,)),
            dma((count,)),
            dma((count,)),
        ],
        compiler_params=pltpu.CompilerParams(
            collective_id=0, has_side_effects=True, vmem_limit_bytes=LAYER_BYTES
        ),
    )(*[pltpu.with_memory_space_constraint(operand, pltpu.HBM) for operand in operands])
    mixed, new_matrix, new_norm, new_max = pl.pallas_call(
        update_kernel,
        out_shape=(made[0], shape(state_matrix.shape, f32), made[4], made[5]),
        in_specs=[vmem] * 6 + [anywhere],
        out_specs=(vmem, anywhere, vmem, vmem),
        scratch_shapes=[
            pltpu.VMEM(state_matrix.shape, f32),
            dma((rows // 8,)),
            dma((rows // 8,)),
        ],
        compiler_params=pltpu.CompilerParams(vmem_limit_bytes=UPDATE_BYTES),
    )(*results, state_matrix)
    return mixed, new_matrix, new_norm, jnp.swapaxes(new_max, 0, 1)


def rms_scale(values_in, gain_vec):
    widened = values_in.astype(jnp.float32)
    return (
        widened * lax.rsqrt(jnp.mean(widened * widened, axis=-1, keepdims=True) + 1e-06) * gain_vec
    )


def memory_cell(
    query,
    key_row,
    value_row,
    outgate,
    input_pre,
    forget_pre,
    head_gain,
    state_matrix,
    state_norm,
    state_max,
):
    seq_rows, head_count = input_pre.shape
    head_size = query.shape[1] // head_count
    query_heads = query.astype(jnp.float32).reshape(seq_rows, head_count, head_size)
    key_heads = key_row.astype(jnp.float32).reshape(
        seq_rows, head_count, head_size
    ) * head_size ** (-0.5)
    value_heads = value_row.astype(jnp.float32).reshape(seq_rows, head_count, head_size)
    log_forget = jax.nn.log_sigmoid(forget_pre)
    new_max = jnp.maximum(log_forget + state_max, input_pre)
    keep_old = jnp.exp(log_forget + state_max - new_max)
    keep_new = jnp.exp(input_pre - new_max)
    new_matrix = (
        keep_old[:, :, None, None] * state_matrix
        + keep_new[:, :, None, None] * value_heads[:, :, :, None] * key_heads[:, :, None, :]
    )
    new_norm = keep_old[:, :, None] * state_norm + keep_new[:, :, None] * key_heads
    numerator = jnp.einsum(
        "bhvd,bhd->bhv", new_matrix, query_heads, precision=lax.Precision.HIGHEST
    )
    denominator = jnp.sum(new_norm * query_heads, axis=-1)
    cell_read = numerator / jnp.maximum(jnp.abs(denominator), jnp.exp(-new_max))[:, :, None]
    centered = cell_read - jnp.mean(cell_read, axis=-1, keepdims=True)
    variance = jnp.mean(centered * centered, axis=-1, keepdims=True)
    scaled_cell = (centered * lax.rsqrt(variance + 1e-06)).reshape(seq_rows, head_count * head_size)
    cell_out = (scaled_cell * head_gain * jax.nn.sigmoid(outgate.astype(jnp.float32))).astype(
        jnp.bfloat16
    )
    return (cell_out, new_matrix, new_norm, new_max)


def kernels_fit(tokens, w_query, w_igate, w_out, w_expert_gate, routes):
    ep_count = lax.axis_size("ep")
    rows, width = tokens.shape
    capacity = max(2, 2 * rows * routes.shape[1] // (w_expert_gate.shape[0] * ep_count))
    return (
        lax.axis_size("tp") == 2
        and ep_count % (2 * PLANE) == 0
        and w_query.shape[0] == LANES
        and w_query.shape[1] % LANES == 0
        and w_out.shape[1] % LANES == 0
        and width % (2 * LANES) == 0
        and rows % 16 == 0
        and w_igate.shape[1] == 4
        and rows <= LANES
        and w_expert_gate.shape[0] == 1
        and capacity == SUB + SUB // 2
        and ep_count * SUB == LANES
        and w_query.shape[1] == 2 * LANES
    )


def body(
    tokens,
    mix_gain,
    w_query,
    w_key,
    w_value,
    w_outgate,
    w_igate,
    w_fgate,
    igate_bias,
    fgate_bias,
    head_gain,
    w_out,
    state_matrix,
    state_norm,
    state_max,
    ffn_gain,
    w_expert_gate,
    w_expert_up,
    w_expert_down,
    routes,
    route_weights,
):
    seq_rows, width = tokens.shape
    weight_list = (w_query, w_key, w_value, w_outgate, w_igate, w_fgate)
    if kernels_fit(tokens, w_query, w_igate, w_out, w_expert_gate, routes):
        mixed, new_matrix, new_norm, new_max = layer_call(
            tokens,
            mix_gain,
            weight_list,
            igate_bias,
            fgate_bias,
            head_gain,
            w_out,
            state_matrix,
            state_norm,
            state_max,
            ffn_gain,
            (w_expert_gate, w_expert_up, w_expert_down),
            routes,
            route_weights,
        )
        return (mixed, new_matrix, new_norm, new_max)
    normed = rms_scale(tokens, mix_gain).astype(jnp.bfloat16)
    spread = lax.all_to_all(normed, "ep", split_axis=1, concat_axis=0, tiled=True)
    joined = jnp.concatenate(weight_list, axis=1)
    summed = lax.psum_scatter(
        jnp.dot(spread, joined, preferred_element_type=jnp.float32),
        "ep",
        scatter_dimension=0,
        tiled=True,
    )
    bounds = [0]
    for weight in weight_list:
        bounds.append(bounds[-1] + weight.shape[1])
    projected = tuple(
        (summed[:, bounds[index] : bounds[index + 1]] for index in range(len(weight_list)))
    )
    query = projected[0].astype(jnp.bfloat16)
    key_row = projected[1].astype(jnp.bfloat16)
    value_row = projected[2].astype(jnp.bfloat16)
    outgate = projected[3].astype(jnp.bfloat16)
    input_pre = projected[4] + igate_bias
    forget_pre = projected[5] + fgate_bias
    cell_out, new_matrix, new_norm, new_max = memory_cell(
        query,
        key_row,
        value_row,
        outgate,
        input_pre,
        forget_pre,
        head_gain,
        state_matrix,
        state_norm,
        state_max,
    )
    partial_out = jnp.dot(
        cell_out,
        lax.all_gather(w_out, "ep", axis=1, tiled=True),
        preferred_element_type=jnp.float32,
    )
    attended = lax.psum(partial_out.astype(jnp.bfloat16), "tp").astype(jnp.float32)
    resid = (tokens.astype(jnp.float32) + attended).astype(jnp.bfloat16)
    normed_two = rms_scale(resid, ffn_gain).astype(jnp.bfloat16)
    ep_count = lax.axis_size("ep")
    local_experts = w_expert_gate.shape[0]
    expert_total = local_experts * ep_count
    top_count = routes.shape[1]
    capacity = max(2, 2 * seq_rows * top_count // expert_total)
    flat_routes = routes.reshape(-1)
    onehot = (flat_routes[:, None] == jnp.arange(expert_total, dtype=jnp.int32)[None, :]).astype(
        jnp.int32
    )
    earlier = jnp.cumsum(onehot, axis=0, dtype=jnp.int32) - onehot
    slots = jnp.sum(onehot * earlier, axis=1, dtype=jnp.int32)
    targets = flat_routes * capacity + slots
    dispatch = (
        targets[:, None] == jnp.arange(expert_total * capacity, dtype=jnp.int32)[None, :]
    ).astype(jnp.bfloat16)
    route_rows = jnp.repeat(normed_two, top_count, axis=0)
    outgoing = jnp.einsum(
        "rs,rd->sd", dispatch, route_rows, preferred_element_type=jnp.float32
    ).astype(jnp.bfloat16)
    outgoing = outgoing.reshape(expert_total, capacity, width)
    received = lax.all_to_all(outgoing, "ep", split_axis=0, concat_axis=0, tiled=True)
    slot_count = received.shape[1]
    regrouped = received.reshape(ep_count, local_experts, slot_count, width)
    gate_pre = jnp.einsum(
        "nxcd,xdf->nxcf", regrouped, w_expert_gate, preferred_element_type=jnp.float32
    )
    up_pre = jnp.einsum(
        "nxcd,xdf->nxcf", regrouped, w_expert_up, preferred_element_type=jnp.float32
    )
    hidden = (jax.nn.silu(gate_pre) * up_pre).astype(jnp.bfloat16)
    partial_down = jnp.einsum(
        "nxcf,xfd->nxcd", hidden, w_expert_down, preferred_element_type=jnp.float32
    )
    expert_sum = lax.psum(partial_down.astype(jnp.bfloat16), "tp")
    finished = expert_sum.reshape(ep_count * local_experts, slot_count, width)
    returned = lax.all_to_all(finished, "ep", split_axis=0, concat_axis=0, tiled=True)
    picked = jnp.dot(
        dispatch,
        returned.reshape(expert_total * capacity, width),
        preferred_element_type=jnp.float32,
    )
    weighted = jnp.sum(
        picked.reshape(seq_rows, top_count, width) * route_weights[:, :, None], axis=1
    )
    mixed = (resid.astype(jnp.float32) + weighted).astype(jnp.bfloat16)
    return (mixed, new_matrix, new_norm, new_max)


def solution(mesh):
    placed = (
        P("ep", None),
        P(),
        P("ep", "tp"),
        P("ep", "tp"),
        P("ep", "tp"),
        P("ep", "tp"),
        P("ep", "tp"),
        P("ep", "tp"),
        P("tp"),
        P("tp"),
        P("tp"),
        P("tp", "ep"),
        P("ep", "tp", None, None),
        P("ep", "tp", None),
        P("ep", "tp"),
        P(),
        P("ep", None, "tp"),
        P("ep", None, "tp"),
        P("ep", "tp", None),
        P("ep", None),
        P("ep", None),
    )
    return jax.shard_map(
        body,
        mesh=mesh,
        in_specs=placed,
        out_specs=(P("ep", None), P("ep", "tp", None, None), P("ep", "tp", None), P("ep", "tp")),
        check_vma=False,
    )
```

```python
import functools

import jax
import jax.numpy as jnp
from jax import lax
from jax.experimental import pallas as pl
from jax.experimental.pallas import tpu as pltpu
from jax.sharding import PartitionSpec as P

MESH = pl.DeviceIdType.MESH
PLANE = 4
LANES = 128
SUB = 8
LAYER_BYTES = 40 * 1024 * 1024
STORE_BYTES = 8 * 1024 * 1024


def remote(src, dst, send_sem, recv_sem, target):
    return pltpu.make_async_remote_copy(
        src_ref=src,
        dst_ref=dst,
        send_sem=send_sem,
        recv_sem=recv_sem,
        device_id=target,
        device_id_type=MESH,
    )


def dot_t(left, right):
    return lax.dot_general(
        left, right, (((1,), (1,)), ((), ())), preferred_element_type=jnp.float32
    )


def fetch_all(pairs, sems):
    copies = []
    for index, (source, kept) in enumerate(pairs):
        copy = pltpu.make_async_copy(source, kept, sems.at[index])
        copy.start()
        copies.append(copy)
    return copies


def place(index, size):
    return pl.ds(pl.multiple_of(index * size, size), size)


def split_three(values):
    high = values.astype(jnp.bfloat16)
    rest = values - high.astype(jnp.float32)
    middle = rest.astype(jnp.bfloat16)
    return [high, middle, (rest - middle.astype(jnp.float32)).astype(jnp.bfloat16)]


def exact_dot(values, chosen):
    rows = values[0].shape[0]
    parts = [part for value in values for part in split_three(value)]
    product = jnp.dot(
        jnp.concatenate(parts, axis=0), chosen, preferred_element_type=jnp.float32
    )
    results = []
    for index in range(len(values)):
        start = 3 * index * rows
        pieces = [product[start + rows * part : start + rows * (part + 1)] for part in range(3)]
        results.append(pieces[0] + pieces[1] + pieces[2])
    return results


def ones_where(condition):
    return jnp.where(condition, 1.0, 0.0).astype(jnp.bfloat16)


def gather_rows(chosen, values):
    return jnp.dot(chosen, values, preferred_element_type=jnp.float32).astype(jnp.bfloat16)


def layer_kernel(
    count,
    tokens_hbm,
    mix_gain_hbm,
    wq_hbm,
    wk_hbm,
    wv_hbm,
    wg_hbm,
    igate_hbm,
    fgate_hbm,
    ibias_hbm,
    fbias_hbm,
    head_gain_hbm,
    w_out_hbm,
    matrix_hbm,
    norm_hbm,
    max_hbm,
    ffn_gain_hbm,
    w_gate_hbm,
    w_up_hbm,
    w_down_hbm,
    routes_hbm,
    route_weights_hbm,
    mixed_ref,
    new_matrix_ref,
    new_norm_ref,
    new_max_ref,
    tokens,
    mix_gain,
    igate,
    fgate,
    ibias,
    fbias,
    head_gain,
    matrix,
    state_norm,
    state_max,
    ffn_gain,
    w_gate,
    w_up,
    w_down,
    routes,
    route_weights,
    turned,
    gate_rows,
    gate_t,
    weights_a,
    weights_b,
    w_planes,
    normed,
    spread,
    partial_a,
    partial_b,
    outgoing_a,
    outgoing_b,
    arrived_a,
    arrived_b,
    packed,
    chosen_out,
    chosen_in,
    token_out,
    token_near,
    token_far,
    cell_mine,
    cell_theirs,
    cell_out,
    cell_near,
    cell_far,
    token_rows,
    reads,
    left,
    keys,
    decay,
    resid,
    row_values,
    down_send,
    down_recv,
    finished,
    returned,
    last_send,
    last_recv,
    local_sem,
    a_send,
    a_recv,
    b_send,
    b_recv,
    g_send,
    g_recv,
    x_send,
    x_recv,
    y_send,
    y_recv,
    z_send,
    z_recv,
    pa_send,
    pa_recv,
    pb_send,
    pb_recv,
    o_send,
    o_recv,
    t_send,
    t_recv,
    k_send,
    k_recv,
    kf_send,
    kf_recv,
    c_send,
    c_recv,
    f_send,
    f_recv,
    w_send,
    w_recv,
    r_send,
    r_recv,
    ready,
):
    bf, f32 = jnp.bfloat16, jnp.float32
    ep, tp = lax.axis_index("ep"), lax.axis_index("tp")
    lines = count // PLANE
    line, spot = ep // PLANE, ep % PLANE
    rows, width = tokens.shape
    half = width // 2
    depth = wq_hbm.shape[0]
    block = depth * PLANE
    heads = igate.shape[0]
    size = matrix.shape[3]
    wide = heads * size
    pair = 2 * wide
    area = count * SUB
    top = route_weights.shape[0]
    columns = w_out_hbm.shape[1]
    slab = lines * columns
    part_wide = slab // 2
    partner = (ep, 1 - tp)
    beside = spot + 1 - 2 * (spot % 2)
    across = lax.rem(spot + 2, PLANE)
    beside_peer = (line * PLANE + beside, tp)
    across_peer = (line * PLANE + across, tp)
    corner_peer = (line * PLANE + PLANE - 1 - spot, tp)
    my_half, other_half = place(tp, half), place(1 - tp, half)
    my_rows, other_rows = place(tp, wide), place(1 - tp, wide)
    own_rows = place(spot, depth)

    def line_peer(step):
        other = lax.rem(line + step, lines)
        return other, (other * PLANE + spot, tp)

    first_loads = fetch_all(
        (
            (wq_hbm, weights_a.at[own_rows, :wide]),
            (wk_hbm, weights_a.at[own_rows, wide:]),
            (igate_hbm, igate),
            (fgate_hbm, fgate),
            (wv_hbm, weights_b.at[own_rows, :wide]),
            (wg_hbm, weights_b.at[own_rows, wide:]),
            (tokens_hbm, tokens),
            (mix_gain_hbm, mix_gain),
            (w_out_hbm, w_planes.at[spot, my_rows, place(line, columns)]),
            (routes_hbm, routes),
            (route_weights_hbm, route_weights),
        ),
        local_sem,
    )
    barrier = pltpu.get_barrier_semaphore()
    greeted = [beside_peer, across_peer, corner_peer, partner]
    greeted += [line_peer(step)[1] for step in range(1, lines)]
    for target in greeted:
        pl.semaphore_signal(barrier, inc=1, device_id=target, device_id_type=MESH)
    turned[...] = jnp.zeros_like(turned)
    gate_t[...] = jnp.zeros_like(gate_t)
    for copy in first_loads[:4]:
        copy.wait()
    turned[:heads, :] = igate[...].astype(f32)
    turned[heads : 2 * heads, :] = fgate[...].astype(f32)
    gate_rows[spot] = turned[: 2 * heads, :].astype(bf)
    pl.semaphore_wait(barrier, len(greeted))
    for step in range(1, lines):
        pl.semaphore_signal(ready, inc=1, device_id=line_peer(step)[1], device_id_type=MESH)

    def plane_copies(buffer_view, send, recv):
        def make(owner, part, slot, target):
            view = buffer_view(owner, part)
            return remote(view, view, send.at[slot], recv.at[slot], target)

        return make

    def weight_view(buffer):
        def view(owner, part):
            tall = depth // 2
            return buffer.at[pl.ds(pl.multiple_of(owner * depth + part * tall, tall), tall)]

        return view

    def out_view(owner, part):
        return w_planes.at[owner, my_rows, part * part_wide : (part + 1) * part_wide]

    def open_plane(make):
        first = [
            make(spot, 0, 0, beside_peer),
            make(spot, 1, 2, across_peer),
            make(spot, 1, 1, beside_peer),
            make(spot, 0, 3, across_peer),
        ]
        for copy in first:
            copy.start()
        return first

    def relay_plane(make, first):
        first[0].wait_recv()
        ahead = make(beside, 0, 4, across_peer)
        ahead.start()
        first[1].wait_recv()
        aside = make(across, 1, 5, beside_peer)
        aside.start()
        return [ahead, aside]

    def close_plane(first, second):
        first[2].wait_recv()
        first[3].wait_recv()
        for copy in first:
            copy.wait_send()
        for copy in second:
            copy.wait()

    make_a = plane_copies(weight_view(weights_a), a_send, a_recv)
    make_b = plane_copies(weight_view(weights_b), b_send, b_recv)
    make_o = plane_copies(out_view, o_send, o_recv)
    a_first = open_plane(make_a)
    gate_copies = []
    for slot, target in enumerate((beside_peer, across_peer, corner_peer)):
        view = gate_rows.at[spot]
        copy = remote(view, view, g_send.at[slot], g_recv.at[slot], target)
        copy.start()
        gate_copies.append(copy)
    for copy in first_loads[4:9]:
        copy.wait()
    widened = tokens[...].astype(f32)
    scale = lax.rsqrt(jnp.mean(widened * widened, axis=-1, keepdims=True) + 1e-06)
    normed[...] = (widened * scale * mix_gain[...]).astype(bf)
    x_copies, z_copies = [], []
    narrow = block // 2
    my_part = place(tp, narrow)
    for step in range(1, lines):
        other, target = line_peer(step)
        copy = remote(
            normed.at[:, place(other * 2 + tp, narrow)],
            spread.at[line, :, my_part],
            x_send.at[step],
            x_recv.at[step],
            target,
        )
        copy.start()
        x_copies.append(copy)
    for step in range(1, lines):
        view = w_planes.at[spot, my_rows, place(line, columns)]
        copy = remote(view, view, z_send.at[step], z_recv.at[step], line_peer(step)[1])
        copy.start()
        z_copies.append(copy)
    spread[line] = normed[:, place(line, block)]
    for copy in first_loads[9:]:
        copy.wait()
    late_loads = fetch_all(
        (
            (matrix_hbm, matrix),
            (norm_hbm, state_norm),
            (max_hbm, state_max),
            (ibias_hbm, ibias),
            (fbias_hbm, fbias),
            (head_gain_hbm, head_gain),
            (ffn_gain_hbm, ffn_gain),
            (w_gate_hbm, w_gate),
            (w_up_hbm, w_up),
            (w_down_hbm, w_down),
        ),
        local_sem,
    )

    slot_row = lax.broadcasted_iota(jnp.int32, (area, rows), 0).astype(f32)
    expert = lax.broadcasted_iota(jnp.int32, (count, rows), 0).astype(f32)
    before = jnp.where(
        lax.broadcasted_iota(jnp.int32, (rows, rows), 0)
        < lax.broadcasted_iota(jnp.int32, (rows, rows), 1),
        1.0,
        0.0,
    )
    taken = jnp.zeros((count, 1), f32)
    sent = [jnp.zeros((area, rows), f32) for _ in range(3)]
    mixes = [jnp.zeros((area, rows), f32) for _ in range(3)]
    for k in range(top):
        named = routes[k : k + 1, :].astype(f32)
        match = jnp.where(expert == named, 1.0, 0.0)
        earlier = jnp.dot(match, before, preferred_element_type=f32) + taken
        taken = taken + jnp.sum(match, axis=1, keepdims=True)
        position = jnp.sum(match * earlier, axis=0, keepdims=True)
        low = jnp.where(position < SUB, named * SUB + position, -1000.0)
        high = jnp.where(position < SUB, -1000.0, named * SUB + position - SUB)
        for index, target in enumerate((low, high, high + SUB // 2)):
            hit = slot_row == target
            sent[index] += jnp.where(hit, 1.0, 0.0)
            mixes[index] += jnp.where(hit, route_weights[k : k + 1, :], 0.0)
    for index in range(3):
        chosen_out[index] = sent[index].astype(bf)
        coarse = mixes[index].astype(bf).astype(f32)
        joined = jnp.concatenate(
            [coarse, mixes[index] - coarse, jnp.zeros((area, area - 2 * rows), f32)], axis=1
        )
        chosen_in[index] = joined.T[: 2 * rows].astype(bf)

    def pack_rows(values, target):
        middle = values.shape[1] // 2
        target[:, :, : 2 * middle] = gather_rows(chosen_out[0], values).reshape(
            count, SUB, 2 * middle
        )
        extra = jnp.dot(chosen_out[1], values[:, :middle], preferred_element_type=f32)
        extra += jnp.dot(chosen_out[2], values[:, middle:], preferred_element_type=f32)
        target[:, :, 2 * middle :] = extra.astype(bf).reshape(count, SUB, middle)

    a_second = relay_plane(make_a, a_first)
    b_first = open_plane(make_b)
    pack_rows(tokens[:, my_half], token_out)
    late_loads[0].wait()

    def pack_matrix(start, stop):
        @pl.loop(start, stop)
        def _(index):
            item = 2 * index
            joined = jnp.concatenate(
                [matrix[item].reshape(wide, size), matrix[item + 1].reshape(wide, size)], axis=1
            )
            flipped = joined.T
            upper = flipped.astype(bf)
            packed[index, : 2 * size] = upper
            packed[index, 2 * size :] = (flipped - upper.astype(f32)).astype(bf)

    y_copies = []
    for step in range(1, lines):
        x_copies[step - 1].wait()
        view = spread.at[lax.rem(line + lines - step, lines), :, my_part]
        copy = remote(view, view, y_send.at[step], y_recv.at[step], partner)
        copy.start()
        y_copies.append(copy)
    pack_matrix(0, rows // 4)
    for copy in gate_copies:
        copy.wait()
    for owner in range(PLANE):
        part = gate_rows[owner]
        gate_t[: 2 * heads, owner * depth : (owner + 1) * depth] = part
        gate_t[LANES // 2 : LANES // 2 + 2 * heads, owner * depth : (owner + 1) * depth] = part
    for copy in y_copies:
        copy.wait()
    close_plane(a_first, a_second)
    arranged = spread[...].reshape(lines * rows, block)
    product = jnp.dot(arranged, weights_a[...], preferred_element_type=f32)
    gates = dot_t(arranged, gate_t[...])
    coarse = gates.astype(bf).astype(f32)
    first = lax.broadcasted_iota(jnp.int32, gates.shape, 1) < LANES // 2
    picked = jnp.where(first, coarse, gates - coarse).astype(bf)
    outgoing_a[:, :, :pair] = product.astype(bf).reshape(lines, rows, pair)
    outgoing_a[:, :, pair:] = picked.reshape(lines, rows, LANES)
    partial_a[:, :, :pair] = product.reshape(lines, rows, pair)
    partial_a[:, :, pair:] = jnp.where(first, gates, 0.0).reshape(lines, rows, LANES)

    def send_partials(outgoing, arrived, send, recv):
        copies = []
        for step in range(1, lines):
            other, target = line_peer(step)
            copy = remote(
                outgoing.at[other], arrived.at[step], send.at[step], recv.at[step], target
            )
            copy.start()
            copies.append(copy)
        return copies

    pa_copies = send_partials(outgoing_a, arrived_a, pa_send, pa_recv)
    b_second = relay_plane(make_b, b_first)
    for copy in z_copies:
        copy.wait()
    o_first = open_plane(make_o)
    slabs = []

    def pass_slab(view):
        slot = len(slabs)
        copy = remote(view, view, w_send.at[slot], w_recv.at[slot], partner)
        copy.start()
        slabs.append(copy)

    pass_slab(w_planes.at[spot, my_rows])
    pack_matrix(rows // 4, rows // 2)
    for copy in late_loads[1:7]:
        copy.wait()

    chosen_head = ones_where(
        lax.broadcasted_iota(jnp.int32, (LANES, pair), 0) % (LANES // 2)
        == lax.broadcasted_iota(jnp.int32, (LANES, pair), 1) // size
    )
    same_head = ones_where(
        lax.broadcasted_iota(jnp.int32, (wide, wide), 0) // size
        == lax.broadcasted_iota(jnp.int32, (wide, wide), 1) // size
    )
    same_place = ones_where(
        lax.broadcasted_iota(jnp.int32, (wide, wide), 0) % size
        == lax.broadcasted_iota(jnp.int32, (wide, wide), 1) % size
    )
    turned[...] = jnp.zeros_like(turned)
    turned[:heads, :rows] = state_max[...]
    old_max_lane = turned[...].T[:rows]
    turned[...] = jnp.zeros_like(turned)
    turned[0:1, :heads] = ibias[...]
    turned[1:2, :heads] = fbias[...]
    ibias_lane, fbias_lane = turned[0:1, :], turned[1:2, :]
    biases = jnp.concatenate(
        [ibias_lane + pltpu.roll(fbias_lane, heads, 1), jnp.zeros((7, LANES), f32)], axis=0
    )
    old_max_wide, bias_wide = (
        exact_dot([old_max_lane], chosen_head)[0][:, :wide],
        exact_dot([biases], chosen_head)[0][:1],
    )
    old_norm = jnp.concatenate([state_norm[:, head, :] for head in range(heads)], axis=1)

    close_plane(b_first, b_second)
    product = jnp.dot(arranged, weights_b[...], preferred_element_type=f32)
    outgoing_b[...] = product.astype(bf).reshape(lines, rows, pair)
    partial_b[...] = product.reshape(lines, rows, pair)
    pb_copies = send_partials(outgoing_b, arrived_b, pb_send, pb_recv)

    def scatter(source, near, send, recv):
        groups = {}
        for hop in [lines // 2] + [n for n in range(1, lines) if n != lines // 2] + [0]:
            groups[hop] = []
            for turn in range(PLANE):
                if hop == 0 and turn == 0:
                    continue
                other = lax.rem(line + hop, lines) * PLANE + lax.rem(spot + turn, PLANE)
                slot = hop * PLANE + turn
                copy = remote(
                    source.at[other], near.at[ep], send.at[slot], recv.at[slot], (other, tp)
                )
                copy.start()
                groups[hop].append(copy)
        near[ep] = source[ep]
        return groups

    def forward(groups, near, far, send, recv):
        copies = []
        for hop in range(lines):
            for copy in groups[hop]:
                copy.wait()
            span = place(lax.rem(line + lines - hop, lines), PLANE)
            copy = remote(near.at[span], far.at[span], send.at[hop], recv.at[hop], partner)
            copy.start()
            copies.append(copy)
        return copies

    pl.semaphore_wait(ready, lines - 1)
    token_copies = scatter(token_out, token_near, k_send, k_recv)

    total = partial_a[line]
    for step in range(1, lines):
        pa_copies[step - 1].wait()
        total = total + arrived_a[step].astype(f32)
    gates_lane = total[:, pair:]
    gates_wide = exact_dot([gates_lane], chosen_head)[0]

    def gate_math(input_pre, forget_pre, old_max):
        log_forget = jnp.minimum(forget_pre, 0.0) - jnp.log(1.0 + jnp.exp(-jnp.abs(forget_pre)))
        new_max = jnp.maximum(log_forget + old_max, input_pre)
        return new_max, jnp.exp(log_forget + old_max - new_max), jnp.exp(input_pre - new_max)

    new_max, keep_old, keep_new = gate_math(
        gates_wide[:, :wide] + bias_wide[:, :wide],
        gates_wide[:, wide:] + bias_wide[:, wide:],
        old_max_wide,
    )
    query = total[:, :wide].astype(bf).astype(f32)
    key = total[:, wide:pair].astype(bf).astype(f32) * size ** (-0.5)
    pack = 2 * heads
    row = lax.broadcasted_iota(jnp.int32, (rows, pack, wide), 1)
    head = lax.broadcasted_iota(jnp.int32, (rows, pack, wide), 2) // size
    only = row == head
    spread_query = jnp.where(only, jnp.broadcast_to(query[:, None, :], only.shape), 0.0)
    tiled = jnp.dot(
        spread_query.reshape(rows * pack, wide).astype(bf),
        same_place,
        preferred_element_type=f32,
    )
    asked_shape = (rows * pack, wide)
    parity = (lax.broadcasted_iota(jnp.int32, asked_shape, 0) // pack) % 2
    lane_parity = (lax.broadcasted_iota(jnp.int32, asked_shape, 1) // size) % 2
    asked = jnp.where(parity == lane_parity, tiled, 0.0).astype(bf)
    for index in range(rows // 2):
        span = slice(2 * pack * index, 2 * pack * (index + 1))
        reads[span, :] = jnp.dot(asked[span], packed[index], preferred_element_type=f32)
    read_old = jnp.sum(jnp.where(only, reads[...].reshape(rows, pack, wide), 0.0), axis=1)
    query_key, query_norm = exact_dot([query * key, query * old_norm], same_head)
    divisor = jnp.maximum(
        jnp.abs(keep_old * query_norm + keep_new * query_key), jnp.exp(-new_max)
    )
    o_second = relay_plane(make_o, o_first)
    pass_slab(out_view(beside, 0))
    pass_slab(out_view(across, 1))
    late = partial_b[line]
    for step in range(1, lines):
        pb_copies[step - 1].wait()
        late = late + arrived_b[step].astype(f32)
    value = late[:, :wide].astype(bf).astype(f32)
    outgate = late[:, wide:].astype(bf).astype(f32)
    read = (keep_old * read_old + keep_new * query_key * value) / divisor
    centered = read - exact_dot([read], same_head)[0] * (1.0 / size)
    variance = exact_dot([centered * centered], same_head)[0] * (1.0 / size)
    cell = (
        centered * lax.rsqrt(variance + 1e-06) * head_gain[...] * jax.nn.sigmoid(outgate)
    ).astype(bf)
    cell_mine[...] = cell
    swap = remote(cell_mine, cell_theirs, t_send.at[0], t_recv.at[0], partner)
    swap.start()
    pack_rows(cell, cell_out)
    cell_copies = scatter(cell_out, cell_near, c_send, c_recv)

    o_first[2].wait_recv()
    pass_slab(out_view(beside, 1))
    o_first[3].wait_recv()
    pass_slab(out_view(across, 0))

    lane_gates = gates_lane + pltpu.roll(gates_lane, LANES // 2, 1)
    lane_max, lane_old, lane_new = gate_math(
        lane_gates + ibias_lane,
        pltpu.roll(lane_gates, LANES - heads, 1) + fbias_lane,
        old_max_lane,
    )
    turned[:rows, :] = lane_max
    new_max_ref[...] = turned[...].T[:heads, :rows]
    row_lane = lax.broadcasted_iota(jnp.int32, (rows, pack, LANES), 1)
    lane = lax.broadcasted_iota(jnp.int32, (rows, pack, LANES), 2)
    chosen = ((row_lane == lane) | (row_lane == lane + heads)) & (lane < heads)

    def per_head(values):
        wider = jnp.broadcast_to(values[:, None, :], (rows, pack, LANES))
        return jnp.sum(jnp.where(chosen, wider, 0.0), axis=-1, keepdims=True)

    old_scale, new_scale = per_head(lane_old), per_head(lane_new)
    decay[...] = jnp.broadcast_to(old_scale, decay.shape)
    same = only | (row == head + heads)
    spread_key = jnp.where(same, jnp.broadcast_to(key[:, None, :], same.shape), 0.0)
    key_rows = jnp.dot(
        spread_key.reshape(rows * pack, wide).astype(bf),
        same_place[:, :size],
        preferred_element_type=f32,
    ).reshape(rows, pack, size)
    keys[...] = key_rows
    new_norm_ref[...] = (
        old_scale[:, :heads] * state_norm[...] + (new_scale * key_rows)[:, :heads]
    )
    scaled = jnp.where(same, jnp.broadcast_to(value[:, None, :], same.shape) * new_scale, 0.0)
    coarse = scaled.astype(bf).astype(f32)
    left[...] = jnp.where(row < heads, coarse, scaled - coarse)

    corner = PLANE - 1 - spot
    token_forwards = forward(token_copies, token_near, token_far, kf_send, kf_recv)
    for part in range(2):
        o_second[part].wait_recv()
        pass_slab(out_view(corner, part))

    extra_rows = area // 2
    lift_row = lax.broadcasted_iota(jnp.int32, (extra_rows, area), 0)
    lift_column = lax.broadcasted_iota(jnp.int32, (extra_rows, area), 1)
    lift_place = (lift_row // (SUB // 2)) * SUB + lift_row % (SUB // 2)
    lift_low = ones_where(lift_column == lift_place)
    lift_high = ones_where(lift_column == lift_place + SUB // 2)

    def unpack_rows(source):
        middle = source.shape[2] // 3
        flat = source[:, :, : 2 * middle].reshape(area, 2 * middle)
        extra = source[:, :, 2 * middle :].reshape(area, middle)
        joined = jnp.concatenate(
            [gather_rows(lift_low, extra), gather_rows(lift_high, extra)], axis=1
        )
        return jnp.concatenate([flat, joined], axis=0)

    token_rows[:, my_half] = unpack_rows(token_near)
    for copy in token_forwards:
        copy.wait()
    token_rows[:, other_half] = unpack_rows(token_far)

    forwards = forward(cell_copies, cell_near, cell_far, f_send, f_recv)
    near_rows = unpack_rows(cell_near)
    for copy in o_first + o_second:
        copy.wait_send()
    near_parts = [
        jnp.dot(near_rows, w_planes[owner, my_rows], preferred_element_type=f32)
        for owner in range(PLANE)
    ]
    for copy in slabs:
        copy.wait()
    for copy in forwards:
        copy.wait()
    far_rows = unpack_rows(cell_far)
    squares = jnp.zeros((near_rows.shape[0], columns), f32)
    for owner in range(PLANE):
        added = near_parts[owner] + jnp.dot(
            far_rows, w_planes[owner, other_rows], preferred_element_type=f32
        )
        for index in range(lines):
            start = (index * PLANE + owner) * columns
            place_columns = slice(start, start + columns)
            summed = (
                token_rows[:, place_columns].astype(f32)
                + added[:, index * columns : (index + 1) * columns]
            ).astype(bf)
            row_values[:, place_columns] = summed
            widened = summed.astype(f32)
            squares += widened * widened
    scale = lax.rsqrt(jnp.sum(squares, axis=-1, keepdims=True) * (1.0 / width) + 1e-06)
    row_values[...] = (row_values[...].astype(f32) * scale * ffn_gain[...]).astype(bf)
    for copy in late_loads[7:]:
        copy.wait()
    gate_pre = dot_t(row_values[...], w_gate[...])
    up_pre = dot_t(row_values[...], w_up[...])
    hidden = (gate_pre * jax.nn.sigmoid(gate_pre) * up_pre).astype(bf)
    quarter = half // 2
    swaps, kept = [], []
    for part in range(2):
        theirs = w_down[:, place((1 - tp) * 2 + part, quarter)]
        down_send[part] = jnp.dot(hidden, theirs, preferred_element_type=f32).astype(bf)
        copy = remote(
            down_send.at[part],
            down_recv.at[part],
            t_send.at[2 + part],
            t_recv.at[2 + part],
            partner,
        )
        copy.start()
        swaps.append(copy)
        mine = w_down[:, place(tp * 2 + part, quarter)]
        kept.append(jnp.dot(hidden, mine, preferred_element_type=f32).astype(bf))
    over = (((0,), (0,)), ((), ()))
    middle = quarter // 2
    return_groups = []
    for part in range(2):
        swaps[part].wait()
        done = (kept[part].astype(f32) + down_recv[part].astype(f32)).astype(bf)
        finished[part, :, :, :quarter] = done[:area].reshape(count, SUB, quarter)
        folded = lax.dot_general(
            lift_low, done[area:, :middle], over, preferred_element_type=f32
        ) + lax.dot_general(lift_high, done[area:, middle:], over, preferred_element_type=f32)
        finished[part, :, :, quarter:] = folded.astype(bf).reshape(count, SUB, middle)
        return_groups.append(
            scatter(finished.at[part], returned.at[part], r_send.at[part], r_recv.at[part])
        )

    swap.wait()
    home_columns = pl.ds(pl.multiple_of(tp * part_wide, part_wide), part_wide)
    for owner in range(PLANE):
        added = jnp.dot(
            cell_mine[...], w_planes[owner, my_rows, home_columns], preferred_element_type=f32
        ) + jnp.dot(
            cell_theirs[...], w_planes[owner, other_rows, home_columns], preferred_element_type=f32
        )
        for index in range(lines // 2):
            start = (index * PLANE + owner) * columns
            resid[:, start : start + columns] = added[:, index * columns : (index + 1) * columns]
    resid[...] = (tokens[:, my_half].astype(f32) + resid[...]).astype(bf).astype(f32)

    @pl.loop(0, rows // 4)
    def _(group):
        for inner in range(4):
            item = group * 4 + inner
            outer = lax.dot_general(
                left[item].astype(bf), keys[item].astype(bf), over, preferred_element_type=f32
            ).reshape(heads, size, size)
            new_matrix_ref[item] = decay[item][:heads][:, None, :] * matrix[item] + outer

    def combine(index, values):
        both = jnp.dot(chosen_in[index], values, preferred_element_type=f32)
        return both[:rows] + both[rows:]

    swaps = []
    for part in range(2):
        for group in return_groups[part].values():
            for copy in group:
                copy.wait()
        back = returned[part, :, :, :quarter].reshape(area, quarter)
        extra = returned[part, :, :, quarter:].reshape(area, middle)
        weighted = combine(0, back) + jnp.concatenate(
            [combine(1, extra), combine(2, extra)], axis=1
        )
        span = slice(part * quarter, (part + 1) * quarter)
        last_send[part] = (resid[:, span] + weighted).astype(bf)
        copy = remote(
            last_send.at[part],
            last_recv.at[part],
            t_send.at[4 + part],
            t_recv.at[4 + part],
            partner,
        )
        copy.start()
        swaps.append(copy)
        mixed_ref[:, place(tp * 2 + part, quarter)] = last_send[part]
    for part in range(2):
        swaps[part].wait()
        mixed_ref[:, place((1 - tp) * 2 + part, quarter)] = last_recv[part]


def store_kernel(
    mixed_ref,
    matrix_ref,
    norm_ref,
    max_ref,
    mixed_out,
    matrix_out,
    norm_out,
    max_out,
    sems,
):
    chunks = 4
    tall = matrix_ref.shape[0] // chunks
    pairs = []
    for index in range(chunks):
        part = pl.ds(index * tall, tall)
        pairs.append((matrix_ref.at[part], matrix_out.at[part]))
    pairs += [(mixed_ref, mixed_out), (norm_ref, norm_out), (max_ref, max_out)]
    for copy in fetch_all(pairs, sems):
        copy.wait()


def layer_call(
    tokens,
    mix_gain,
    weight_list,
    igate_bias,
    fgate_bias,
    head_gain,
    w_out,
    state_matrix,
    state_norm,
    state_max,
    ffn_gain,
    expert_weights,
    routes,
    route_weights,
):
    rows, width = tokens.shape
    w_query, w_key, w_value, w_outgate, w_igate, w_fgate = weight_list
    depth, wide = w_query.shape
    count = lax.axis_size("ep")
    lines = count // PLANE
    heads = w_igate.shape[1]
    size = state_matrix.shape[3]
    half, block, pair, area = width // 2, depth * PLANE, 2 * wide, count * SUB
    slots = area + area // 2
    gate_t = jnp.swapaxes(expert_weights[0][0], 0, 1)
    up_t = jnp.swapaxes(expert_weights[1][0], 0, 1)
    down = expert_weights[2][0]
    vmem = pl.BlockSpec(memory_space=pltpu.VMEM)
    far = pl.BlockSpec(memory_space=pltpu.HBM)
    anywhere = pl.BlockSpec(memory_space=pl.ANY)
    dma = pltpu.SemaphoreType.DMA
    bf, f32 = jnp.bfloat16, jnp.float32
    shape = jax.ShapeDtypeStruct
    tile = (count, SUB, half + half // 2)
    thin = (count, SUB, wide + wide // 2)
    parts = (2, count, SUB, half // 2 + half // 4)
    made = (
        shape((rows, width), bf),
        shape(state_matrix.shape, f32),
        shape(state_norm.shape, f32),
        shape((heads, rows), f32),
    )
    operands = (
        tokens,
        mix_gain[None, :],
        w_query,
        w_key,
        w_value,
        w_outgate,
        jnp.swapaxes(w_igate, 0, 1),
        jnp.swapaxes(w_fgate, 0, 1),
        igate_bias[None, :],
        fgate_bias[None, :],
        head_gain[None, :],
        w_out,
        state_matrix,
        state_norm,
        jnp.swapaxes(state_max, 0, 1),
        ffn_gain[None, :],
        gate_t,
        up_t,
        down,
        jnp.swapaxes(routes, 0, 1),
        jnp.swapaxes(route_weights, 0, 1),
    )
    results = pl.pallas_call(
        functools.partial(layer_kernel, count),
        out_shape=made,
        in_specs=[far] * 21,
        out_specs=(vmem,) * 4,
        scratch_shapes=[
            pltpu.VMEM((rows, width), bf),
            pltpu.VMEM((1, width), f32),
            pltpu.VMEM((heads, depth), bf),
            pltpu.VMEM((heads, depth), bf),
            pltpu.VMEM((1, heads), f32),
            pltpu.VMEM((1, heads), f32),
            pltpu.VMEM((1, wide), f32),
            pltpu.VMEM(state_matrix.shape, f32),
            pltpu.VMEM(state_norm.shape, f32),
            pltpu.VMEM((heads, rows), f32),
            pltpu.VMEM((1, width), f32),
            pltpu.VMEM(gate_t.shape, bf),
            pltpu.VMEM(up_t.shape, bf),
            pltpu.VMEM(down.shape, bf),
            pltpu.VMEM((routes.shape[1], rows), jnp.int32),
            pltpu.VMEM((routes.shape[1], rows), f32),
            pltpu.VMEM((LANES, LANES), f32),
            pltpu.VMEM((PLANE, 2 * heads, depth), bf),
            pltpu.VMEM((LANES, block), bf),
            pltpu.VMEM((block, pair), bf),
            pltpu.VMEM((block, pair), bf),
            pltpu.VMEM((PLANE, pair, lines * w_out.shape[1]), bf),
            pltpu.VMEM((rows, width), bf),
            pltpu.VMEM((lines, rows, block), bf),
            pltpu.VMEM((lines, rows, pair + LANES), f32),
            pltpu.VMEM((lines, rows, pair), f32),
            pltpu.VMEM((lines, rows, pair + LANES), bf),
            pltpu.VMEM((lines, rows, pair), bf),
            pltpu.VMEM((lines, rows, pair + LANES), bf),
            pltpu.VMEM((lines, rows, pair), bf),
            pltpu.VMEM((rows // 2, wide, wide), bf),
            pltpu.VMEM((3, area, rows), bf),
            pltpu.VMEM((3, 2 * rows, area), bf),
            pltpu.VMEM(tile, bf),
            pltpu.VMEM(tile, bf),
            pltpu.VMEM(tile, bf),
            pltpu.VMEM((rows, wide), bf),
            pltpu.VMEM((rows, wide), bf),
            pltpu.VMEM(thin, bf),
            pltpu.VMEM(thin, bf),
            pltpu.VMEM(thin, bf),
            pltpu.VMEM((slots, width), bf),
            pltpu.VMEM((rows * 2 * heads, wide), f32),
            pltpu.VMEM((rows, 2 * heads, wide), f32),
            pltpu.VMEM((rows, 2 * heads, size), f32),
            pltpu.VMEM((rows, 2 * heads, size), f32),
            pltpu.VMEM((rows, half), f32),
            pltpu.VMEM((slots, width), bf),
            pltpu.VMEM((2, slots, half // 2), bf),
            pltpu.VMEM((2, slots, half // 2), bf),
            pltpu.VMEM(parts, bf),
            pltpu.VMEM(parts, bf),
            pltpu.VMEM((2, rows, half // 2), bf),
            pltpu.VMEM((2, rows, half // 2), bf),
            dma((11,)),
            dma((6,)),
            dma((6,)),
            dma((6,)),
            dma((6,)),
            dma((3,)),
            dma((3,)),
            dma((lines,)),
            dma((lines,)),
            dma((lines,)),
            dma((lines,)),
            dma((lines,)),
            dma((lines,)),
            dma((lines,)),
            dma((lines,)),
            dma((lines,)),
            dma((lines,)),
            dma((6,)),
            dma((6,)),
            dma((6,)),
            dma((6,)),
            dma((count,)),
            dma((count,)),
            dma((lines,)),
            dma((lines,)),
            dma((count,)),
            dma((count,)),
            dma((lines,)),
            dma((lines,)),
            dma((7,)),
            dma((7,)),
            dma((2, count)),
            dma((2, count)),
            pltpu.SemaphoreType.REGULAR,
        ],
        compiler_params=pltpu.CompilerParams(
            collective_id=0, has_side_effects=True, vmem_limit_bytes=LAYER_BYTES
        ),
    )(*[pltpu.with_memory_space_constraint(operand, pltpu.HBM) for operand in operands])
    mixed, new_matrix, new_norm, new_max = pl.pallas_call(
        store_kernel,
        out_shape=made,
        in_specs=[vmem] * 4,
        out_specs=(anywhere,) * 4,
        scratch_shapes=[dma((7,))],
        compiler_params=pltpu.CompilerParams(vmem_limit_bytes=STORE_BYTES),
    )(*results)
    return mixed, new_matrix, new_norm, jnp.swapaxes(new_max, 0, 1)


def rms_scale(values_in, gain_vec):
    widened = values_in.astype(jnp.float32)
    return (
        widened * lax.rsqrt(jnp.mean(widened * widened, axis=-1, keepdims=True) + 1e-06) * gain_vec
    )


def memory_cell(
    query,
    key_row,
    value_row,
    outgate,
    input_pre,
    forget_pre,
    head_gain,
    state_matrix,
    state_norm,
    state_max,
):
    seq_rows, head_count = input_pre.shape
    head_size = query.shape[1] // head_count
    query_heads = query.astype(jnp.float32).reshape(seq_rows, head_count, head_size)
    key_heads = key_row.astype(jnp.float32).reshape(
        seq_rows, head_count, head_size
    ) * head_size ** (-0.5)
    value_heads = value_row.astype(jnp.float32).reshape(seq_rows, head_count, head_size)
    log_forget = jax.nn.log_sigmoid(forget_pre)
    new_max = jnp.maximum(log_forget + state_max, input_pre)
    keep_old = jnp.exp(log_forget + state_max - new_max)
    keep_new = jnp.exp(input_pre - new_max)
    new_matrix = (
        keep_old[:, :, None, None] * state_matrix
        + keep_new[:, :, None, None] * value_heads[:, :, :, None] * key_heads[:, :, None, :]
    )
    new_norm = keep_old[:, :, None] * state_norm + keep_new[:, :, None] * key_heads
    numerator = jnp.einsum(
        "bhvd,bhd->bhv", new_matrix, query_heads, precision=lax.Precision.HIGHEST
    )
    denominator = jnp.sum(new_norm * query_heads, axis=-1)
    cell_read = numerator / jnp.maximum(jnp.abs(denominator), jnp.exp(-new_max))[:, :, None]
    centered = cell_read - jnp.mean(cell_read, axis=-1, keepdims=True)
    variance = jnp.mean(centered * centered, axis=-1, keepdims=True)
    scaled_cell = (centered * lax.rsqrt(variance + 1e-06)).reshape(seq_rows, head_count * head_size)
    cell_out = (scaled_cell * head_gain * jax.nn.sigmoid(outgate.astype(jnp.float32))).astype(
        jnp.bfloat16
    )
    return (cell_out, new_matrix, new_norm, new_max)


def kernels_fit(tokens, w_query, w_igate, w_out, w_expert_gate, routes):
    ep_count = lax.axis_size("ep")
    rows, width = tokens.shape
    capacity = max(2, 2 * rows * routes.shape[1] // (w_expert_gate.shape[0] * ep_count))
    return (
        lax.axis_size("tp") == 2
        and ep_count % (2 * PLANE) == 0
        and w_query.shape[0] == LANES
        and w_query.shape[1] % LANES == 0
        and w_out.shape[1] % LANES == 0
        and width % (2 * LANES) == 0
        and rows % 16 == 0
        and w_igate.shape[1] == 4
        and rows <= LANES
        and w_expert_gate.shape[0] == 1
        and capacity == SUB + SUB // 2
        and ep_count * SUB == LANES
        and w_query.shape[1] == 2 * LANES
    )


def body(
    tokens,
    mix_gain,
    w_query,
    w_key,
    w_value,
    w_outgate,
    w_igate,
    w_fgate,
    igate_bias,
    fgate_bias,
    head_gain,
    w_out,
    state_matrix,
    state_norm,
    state_max,
    ffn_gain,
    w_expert_gate,
    w_expert_up,
    w_expert_down,
    routes,
    route_weights,
):
    seq_rows, width = tokens.shape
    weight_list = (w_query, w_key, w_value, w_outgate, w_igate, w_fgate)
    if kernels_fit(tokens, w_query, w_igate, w_out, w_expert_gate, routes):
        mixed, new_matrix, new_norm, new_max = layer_call(
            tokens,
            mix_gain,
            weight_list,
            igate_bias,
            fgate_bias,
            head_gain,
            w_out,
            state_matrix,
            state_norm,
            state_max,
            ffn_gain,
            (w_expert_gate, w_expert_up, w_expert_down),
            routes,
            route_weights,
        )
        return (mixed, new_matrix, new_norm, new_max)
    normed = rms_scale(tokens, mix_gain).astype(jnp.bfloat16)
    spread = lax.all_to_all(normed, "ep", split_axis=1, concat_axis=0, tiled=True)
    joined = jnp.concatenate(weight_list, axis=1)
    summed = lax.psum_scatter(
        jnp.dot(spread, joined, preferred_element_type=jnp.float32),
        "ep",
        scatter_dimension=0,
        tiled=True,
    )
    bounds = [0]
    for weight in weight_list:
        bounds.append(bounds[-1] + weight.shape[1])
    projected = tuple(
        (summed[:, bounds[index] : bounds[index + 1]] for index in range(len(weight_list)))
    )
    query = projected[0].astype(jnp.bfloat16)
    key_row = projected[1].astype(jnp.bfloat16)
    value_row = projected[2].astype(jnp.bfloat16)
    outgate = projected[3].astype(jnp.bfloat16)
    input_pre = projected[4] + igate_bias
    forget_pre = projected[5] + fgate_bias
    cell_out, new_matrix, new_norm, new_max = memory_cell(
        query,
        key_row,
        value_row,
        outgate,
        input_pre,
        forget_pre,
        head_gain,
        state_matrix,
        state_norm,
        state_max,
    )
    partial_out = jnp.dot(
        cell_out,
        lax.all_gather(w_out, "ep", axis=1, tiled=True),
        preferred_element_type=jnp.float32,
    )
    attended = lax.psum(partial_out.astype(jnp.bfloat16), "tp").astype(jnp.float32)
    resid = (tokens.astype(jnp.float32) + attended).astype(jnp.bfloat16)
    normed_two = rms_scale(resid, ffn_gain).astype(jnp.bfloat16)
    ep_count = lax.axis_size("ep")
    local_experts = w_expert_gate.shape[0]
    expert_total = local_experts * ep_count
    top_count = routes.shape[1]
    capacity = max(2, 2 * seq_rows * top_count // expert_total)
    flat_routes = routes.reshape(-1)
    onehot = (flat_routes[:, None] == jnp.arange(expert_total, dtype=jnp.int32)[None, :]).astype(
        jnp.int32
    )
    earlier = jnp.cumsum(onehot, axis=0, dtype=jnp.int32) - onehot
    slots = jnp.sum(onehot * earlier, axis=1, dtype=jnp.int32)
    targets = flat_routes * capacity + slots
    dispatch = (
        targets[:, None] == jnp.arange(expert_total * capacity, dtype=jnp.int32)[None, :]
    ).astype(jnp.bfloat16)
    route_rows = jnp.repeat(normed_two, top_count, axis=0)
    outgoing = jnp.einsum(
        "rs,rd->sd", dispatch, route_rows, preferred_element_type=jnp.float32
    ).astype(jnp.bfloat16)
    outgoing = outgoing.reshape(expert_total, capacity, width)
    received = lax.all_to_all(outgoing, "ep", split_axis=0, concat_axis=0, tiled=True)
    slot_count = received.shape[1]
    regrouped = received.reshape(ep_count, local_experts, slot_count, width)
    gate_pre = jnp.einsum(
        "nxcd,xdf->nxcf", regrouped, w_expert_gate, preferred_element_type=jnp.float32
    )
    up_pre = jnp.einsum(
        "nxcd,xdf->nxcf", regrouped, w_expert_up, preferred_element_type=jnp.float32
    )
    hidden = (jax.nn.silu(gate_pre) * up_pre).astype(jnp.bfloat16)
    partial_down = jnp.einsum(
        "nxcf,xfd->nxcd", hidden, w_expert_down, preferred_element_type=jnp.float32
    )
    expert_sum = lax.psum(partial_down.astype(jnp.bfloat16), "tp")
    finished = expert_sum.reshape(ep_count * local_experts, slot_count, width)
    returned = lax.all_to_all(finished, "ep", split_axis=0, concat_axis=0, tiled=True)
    picked = jnp.dot(
        dispatch,
        returned.reshape(expert_total * capacity, width),
        preferred_element_type=jnp.float32,
    )
    weighted = jnp.sum(
        picked.reshape(seq_rows, top_count, width) * route_weights[:, :, None], axis=1
    )
    mixed = (resid.astype(jnp.float32) + weighted).astype(jnp.bfloat16)
    return (mixed, new_matrix, new_norm, new_max)


def solution(mesh):
    placed = (
        P("ep", None),
        P(),
        P("ep", "tp"),
        P("ep", "tp"),
        P("ep", "tp"),
        P("ep", "tp"),
        P("ep", "tp"),
        P("ep", "tp"),
        P("tp"),
        P("tp"),
        P("tp"),
        P("tp", "ep"),
        P("ep", "tp", None, None),
        P("ep", "tp", None),
        P("ep", "tp"),
        P(),
        P("ep", None, "tp"),
        P("ep", None, "tp"),
        P("ep", "tp", None),
        P("ep", None),
        P("ep", None),
    )
    return jax.shard_map(
        body,
        mesh=mesh,
        in_specs=placed,
        out_specs=(P("ep", None), P("ep", "tp", None, None), P("ep", "tp", None), P("ep", "tp")),
        check_vma=False,
    )
```

```python
import functools

import jax
import jax.numpy as jnp
from jax import lax
from jax.experimental import pallas as pl
from jax.experimental.pallas import tpu as pltpu
from jax.sharding import PartitionSpec as P

MESH = pl.DeviceIdType.MESH
PLANE = 4
LANES = 128
SUB = 8
LAYER_BYTES = 40 * 1024 * 1024
STORE_BYTES = 8 * 1024 * 1024


def remote(src, dst, send_sem, recv_sem, target):
    return pltpu.make_async_remote_copy(
        src_ref=src,
        dst_ref=dst,
        send_sem=send_sem,
        recv_sem=recv_sem,
        device_id=target,
        device_id_type=MESH,
    )


def dot_t(left, right):
    return lax.dot_general(
        left, right, (((1,), (1,)), ((), ())), preferred_element_type=jnp.float32
    )


def fetch_all(pairs, sems):
    copies = []
    for index, (source, kept) in enumerate(pairs):
        copy = pltpu.make_async_copy(source, kept, sems.at[index])
        copy.start()
        copies.append(copy)
    return copies


def place(index, size):
    return pl.ds(pl.multiple_of(index * size, size), size)


def split_three(values):
    high = values.astype(jnp.bfloat16)
    rest = values - high.astype(jnp.float32)
    middle = rest.astype(jnp.bfloat16)
    return [high, middle, (rest - middle.astype(jnp.float32)).astype(jnp.bfloat16)]


def exact_dot(values, chosen):
    rows = values[0].shape[0]
    parts = [part for value in values for part in split_three(value)]
    product = jnp.dot(
        jnp.concatenate(parts, axis=0), chosen, preferred_element_type=jnp.float32
    )
    results = []
    for index in range(len(values)):
        start = 3 * index * rows
        pieces = [product[start + rows * part : start + rows * (part + 1)] for part in range(3)]
        results.append(pieces[0] + pieces[1] + pieces[2])
    return results


def ones_where(condition):
    return jnp.where(condition, 1.0, 0.0).astype(jnp.bfloat16)


def gather_rows(chosen, values):
    return jnp.dot(chosen, values, preferred_element_type=jnp.float32).astype(jnp.bfloat16)


def layer_kernel(
    count,
    tokens_hbm,
    mix_gain_hbm,
    wq_hbm,
    wk_hbm,
    wv_hbm,
    wg_hbm,
    igate_hbm,
    fgate_hbm,
    ibias_hbm,
    fbias_hbm,
    head_gain_hbm,
    w_out_hbm,
    matrix_hbm,
    norm_hbm,
    max_hbm,
    ffn_gain_hbm,
    w_gate_hbm,
    w_up_hbm,
    w_down_hbm,
    routes_hbm,
    route_weights_hbm,
    mixed_ref,
    new_matrix_ref,
    new_norm_ref,
    new_max_ref,
    tokens,
    mix_gain,
    igate,
    fgate,
    ibias,
    fbias,
    head_gain,
    matrix,
    state_norm,
    state_max,
    ffn_gain,
    w_gate,
    w_up,
    w_down,
    routes,
    route_weights,
    turned,
    gate_rows,
    gate_t,
    weights_a,
    weights_b,
    w_planes,
    normed,
    spread,
    partial_a,
    partial_b,
    outgoing_a,
    outgoing_b,
    arrived_a,
    arrived_b,
    packed,
    chosen_out,
    chosen_in,
    token_out,
    token_near,
    token_far,
    cell_mine,
    cell_theirs,
    cell_out,
    cell_near,
    cell_far,
    token_rows,
    reads,
    left,
    keys,
    decay,
    added,
    resid,
    row_values,
    down_send,
    down_recv,
    finished,
    returned,
    last_send,
    last_recv,
    local_sem,
    a_send,
    a_recv,
    b_send,
    b_recv,
    g_send,
    g_recv,
    x_send,
    x_recv,
    y_send,
    y_recv,
    z_send,
    z_recv,
    pa_send,
    pa_recv,
    pb_send,
    pb_recv,
    o_send,
    o_recv,
    t_send,
    t_recv,
    k_send,
    k_recv,
    kf_send,
    kf_recv,
    c_send,
    c_recv,
    f_send,
    f_recv,
    w_send,
    w_recv,
    r_send,
    r_recv,
    ready,
):
    bf, f32 = jnp.bfloat16, jnp.float32
    ep, tp = lax.axis_index("ep"), lax.axis_index("tp")
    lines = count // PLANE
    line, spot = ep // PLANE, ep % PLANE
    rows, width = tokens.shape
    half = width // 2
    depth = wq_hbm.shape[0]
    block = depth * PLANE
    heads = igate.shape[0]
    size = matrix.shape[3]
    wide = heads * size
    pair = 2 * wide
    area = count * SUB
    top = route_weights.shape[0]
    columns = w_out_hbm.shape[1]
    slab = lines * columns
    part_wide = slab // 2
    partner = (ep, 1 - tp)
    beside = spot + 1 - 2 * (spot % 2)
    across = lax.rem(spot + 2, PLANE)
    beside_peer = (line * PLANE + beside, tp)
    across_peer = (line * PLANE + across, tp)
    corner_peer = (line * PLANE + PLANE - 1 - spot, tp)
    my_half, other_half = place(tp, half), place(1 - tp, half)
    my_rows, other_rows = place(tp, wide), place(1 - tp, wide)
    own_rows = place(spot, depth)

    def line_peer(step):
        other = lax.rem(line + step, lines)
        return other, (other * PLANE + spot, tp)

    first_loads = fetch_all(
        (
            (wq_hbm, weights_a.at[own_rows, :wide]),
            (wk_hbm, weights_a.at[own_rows, wide:]),
            (igate_hbm, igate),
            (fgate_hbm, fgate),
            (wv_hbm, weights_b.at[own_rows, :wide]),
            (wg_hbm, weights_b.at[own_rows, wide:]),
            (tokens_hbm, tokens),
            (mix_gain_hbm, mix_gain),
            (w_out_hbm, w_planes.at[spot, my_rows, place(line, columns)]),
            (routes_hbm, routes),
            (route_weights_hbm, route_weights),
        ),
        local_sem,
    )
    barrier = pltpu.get_barrier_semaphore()
    greeted = [beside_peer, across_peer, corner_peer, partner]
    greeted += [line_peer(step)[1] for step in range(1, lines)]
    for target in greeted:
        pl.semaphore_signal(barrier, inc=1, device_id=target, device_id_type=MESH)
    turned[...] = jnp.zeros_like(turned)
    gate_t[...] = jnp.zeros_like(gate_t)
    for copy in first_loads[:4]:
        copy.wait()
    turned[:heads, :] = igate[...].astype(f32)
    turned[heads : 2 * heads, :] = fgate[...].astype(f32)
    gate_rows[spot] = turned[: 2 * heads, :].astype(bf)
    pl.semaphore_wait(barrier, len(greeted))
    for step in range(1, lines):
        pl.semaphore_signal(ready, inc=1, device_id=line_peer(step)[1], device_id_type=MESH)

    def plane_copies(buffer_view, send, recv):
        def make(owner, part, slot, target):
            view = buffer_view(owner, part)
            return remote(view, view, send.at[slot], recv.at[slot], target)

        return make

    def weight_view(buffer):
        def view(owner, part):
            tall = depth // 2
            return buffer.at[pl.ds(pl.multiple_of(owner * depth + part * tall, tall), tall)]

        return view

    def out_view(owner, part):
        return w_planes.at[owner, my_rows, place(part, part_wide)]

    def open_plane(make):
        first = [
            make(spot, 0, 0, beside_peer),
            make(spot, 1, 2, across_peer),
            make(spot, 1, 1, beside_peer),
            make(spot, 0, 3, across_peer),
        ]
        for copy in first:
            copy.start()
        return first

    def relay_plane(make, first):
        first[0].wait_recv()
        ahead = make(beside, 0, 4, across_peer)
        ahead.start()
        first[1].wait_recv()
        aside = make(across, 1, 5, beside_peer)
        aside.start()
        return [ahead, aside]

    def close_plane(first, second):
        first[2].wait_recv()
        first[3].wait_recv()
        for copy in first:
            copy.wait_send()
        for copy in second:
            copy.wait()

    make_a = plane_copies(weight_view(weights_a), a_send, a_recv)
    make_b = plane_copies(weight_view(weights_b), b_send, b_recv)
    make_o = plane_copies(out_view, o_send, o_recv)
    a_first = open_plane(make_a)
    gate_copies = []
    for slot, target in enumerate((beside_peer, across_peer, corner_peer)):
        view = gate_rows.at[spot]
        copy = remote(view, view, g_send.at[slot], g_recv.at[slot], target)
        copy.start()
        gate_copies.append(copy)
    for copy in first_loads[4:9]:
        copy.wait()
    widened = tokens[...].astype(f32)
    scale = lax.rsqrt(jnp.mean(widened * widened, axis=-1, keepdims=True) + 1e-06)
    normed[...] = (widened * scale * mix_gain[...]).astype(bf)
    x_copies = []
    narrow = block // 2
    my_part = place(tp, narrow)
    for step in range(1, lines):
        other, target = line_peer(step)
        copy = remote(
            normed.at[:, place(other * 2 + tp, narrow)],
            spread.at[line, :, my_part],
            x_send.at[step],
            x_recv.at[step],
            target,
        )
        copy.start()
        x_copies.append(copy)
    near_line = line + 1 - 2 * (line % 2)
    mirror_line = lines - 1 - line
    near_peer = (near_line * PLANE + spot, tp)
    mirror_peer = (mirror_line * PLANE + spot, tp)

    def line_copy(owner, slot, target):
        view = w_planes.at[spot, my_rows, place(owner, columns)]
        return remote(view, view, z_send.at[slot], z_recv.at[slot], target)

    z_copies = [line_copy(line, 0, near_peer), line_copy(line, 1, mirror_peer)]
    for copy in z_copies:
        copy.start()
    spread[line] = normed[:, place(line, block)]
    for copy in first_loads[9:]:
        copy.wait()
    late_loads = fetch_all(
        (
            (matrix_hbm, matrix),
            (norm_hbm, state_norm),
            (max_hbm, state_max),
            (ibias_hbm, ibias),
            (fbias_hbm, fbias),
            (head_gain_hbm, head_gain),
            (ffn_gain_hbm, ffn_gain),
            (w_gate_hbm, w_gate),
            (w_up_hbm, w_up),
            (w_down_hbm, w_down),
        ),
        local_sem,
    )

    slot_row = lax.broadcasted_iota(jnp.int32, (area, rows), 0).astype(f32)
    expert = lax.broadcasted_iota(jnp.int32, (count, rows), 0).astype(f32)
    before = jnp.where(
        lax.broadcasted_iota(jnp.int32, (rows, rows), 0)
        < lax.broadcasted_iota(jnp.int32, (rows, rows), 1),
        1.0,
        0.0,
    )
    taken = jnp.zeros((count, 1), f32)
    sent = [jnp.zeros((area, rows), f32) for _ in range(3)]
    mixes = [jnp.zeros((area, rows), f32) for _ in range(3)]
    for k in range(top):
        named = routes[k : k + 1, :].astype(f32)
        match = jnp.where(expert == named, 1.0, 0.0)
        earlier = jnp.dot(match, before, preferred_element_type=f32) + taken
        taken = taken + jnp.sum(match, axis=1, keepdims=True)
        position = jnp.sum(match * earlier, axis=0, keepdims=True)
        low = jnp.where(position < SUB, named * SUB + position, -1000.0)
        high = jnp.where(position < SUB, -1000.0, named * SUB + position - SUB)
        for index, target in enumerate((low, high, high + SUB // 2)):
            hit = slot_row == target
            sent[index] += jnp.where(hit, 1.0, 0.0)
            mixes[index] += jnp.where(hit, route_weights[k : k + 1, :], 0.0)
    for index in range(3):
        chosen_out[index] = sent[index].astype(bf)
        coarse = mixes[index].astype(bf).astype(f32)
        joined = jnp.concatenate(
            [coarse, mixes[index] - coarse, jnp.zeros((area, area - 2 * rows), f32)], axis=1
        )
        chosen_in[index] = joined.T[: 2 * rows].astype(bf)

    line_of = (lax.rem(line + lines // 2, lines), mirror_line, near_line, line)
    own_group = len(line_of) - 1

    def scatter(groups, turns, source, near, send, recv):
        copies = {}
        for group in groups:
            copies[group] = []
            for turn in turns:
                if group == own_group and turn == 0:
                    near[ep] = source[ep]
                    continue
                other = line_of[group] * PLANE + lax.rem(spot + turn, PLANE)
                slot = group * PLANE + turn
                copy = remote(
                    source.at[other], near.at[ep], send.at[slot], recv.at[slot], (other, tp)
                )
                copy.start()
                copies[group].append(copy)
        return copies

    def forward(copies, near, far, send, recv):
        passed = []
        for group, arriving in copies.items():
            for copy in arriving:
                copy.wait()
            span = place(line_of[group], PLANE)
            copy = remote(near.at[span], far.at[span], send.at[group], recv.at[group], partner)
            copy.start()
            passed.append(copy)
        return passed

    def pack_rows(values, target):
        middle = values.shape[1] // 2
        target[:, :, : 2 * middle] = gather_rows(chosen_out[0], values).reshape(
            count, SUB, 2 * middle
        )
        extra = jnp.dot(chosen_out[1], values[:, :middle], preferred_element_type=f32)
        extra += jnp.dot(chosen_out[2], values[:, middle:], preferred_element_type=f32)
        target[:, :, 2 * middle :] = extra.astype(bf).reshape(count, SUB, middle)

    a_second = relay_plane(make_a, a_first)
    b_first = open_plane(make_b)
    pack_rows(tokens[:, my_half], token_out)
    straight_tokens = scatter(range(own_group), (0,), token_out, token_near, k_send, k_recv)
    late_loads[0].wait()

    def pack_matrix(start, stop):
        @pl.loop(start, stop)
        def _(index):
            item = 2 * index
            joined = jnp.concatenate(
                [matrix[item].reshape(wide, size), matrix[item + 1].reshape(wide, size)], axis=1
            )
            flipped = joined.T
            upper = flipped.astype(bf)
            packed[index, : 2 * size] = upper
            packed[index, 2 * size :] = (flipped - upper.astype(f32)).astype(bf)

    y_copies = []
    for step in range(1, lines):
        x_copies[step - 1].wait()
        view = spread.at[lax.rem(line + lines - step, lines), :, my_part]
        copy = remote(view, view, y_send.at[step], y_recv.at[step], partner)
        copy.start()
        y_copies.append(copy)
    pack_matrix(0, rows // 4)
    for copy in gate_copies:
        copy.wait()
    for owner in range(PLANE):
        part = gate_rows[owner]
        gate_t[: 2 * heads, owner * depth : (owner + 1) * depth] = part
        gate_t[LANES // 2 : LANES // 2 + 2 * heads, owner * depth : (owner + 1) * depth] = part
    for copy in y_copies:
        copy.wait()
    close_plane(a_first, a_second)
    arranged = spread[...].reshape(lines * rows, block)
    product = jnp.dot(arranged, weights_a[...], preferred_element_type=f32)
    gates = dot_t(arranged, gate_t[...])
    coarse = gates.astype(bf).astype(f32)
    first = lax.broadcasted_iota(jnp.int32, gates.shape, 1) < LANES // 2
    picked = jnp.where(first, coarse, gates - coarse).astype(bf)
    outgoing_a[:, :, :pair] = product.astype(bf).reshape(lines, rows, pair)
    outgoing_a[:, :, pair:] = picked.reshape(lines, rows, LANES)
    partial_a[:, :, :pair] = product.reshape(lines, rows, pair)
    partial_a[:, :, pair:] = jnp.where(first, gates, 0.0).reshape(lines, rows, LANES)

    def send_partials(outgoing, arrived, send, recv):
        copies = []
        for step in range(1, lines):
            other, target = line_peer(step)
            copy = remote(
                outgoing.at[other], arrived.at[step], send.at[step], recv.at[step], target
            )
            copy.start()
            copies.append(copy)
        return copies

    z_copies[1].wait_recv()
    z_copies.append(line_copy(mirror_line, 2, near_peer))
    z_copies[2].start()
    pa_copies = send_partials(outgoing_a, arrived_a, pa_send, pa_recv)
    b_second = relay_plane(make_b, b_first)
    z_copies[0].wait_recv()
    held = line // (lines // 2)
    o_first = [make_o(spot, held, 0, beside_peer), make_o(spot, held, 3, across_peer)]
    for copy in o_first:
        copy.start()
    slabs = []

    def pass_slab(view):
        slot = len(slabs)
        copy = remote(view, view, w_send.at[slot], w_recv.at[slot], partner)
        copy.start()
        slabs.append(copy)

    pack_matrix(rows // 4, rows // 2)
    for copy in late_loads[1:7]:
        copy.wait()

    chosen_head = ones_where(
        lax.broadcasted_iota(jnp.int32, (LANES, pair), 0) % (LANES // 2)
        == lax.broadcasted_iota(jnp.int32, (LANES, pair), 1) // size
    )
    same_head = ones_where(
        lax.broadcasted_iota(jnp.int32, (wide, wide), 0) // size
        == lax.broadcasted_iota(jnp.int32, (wide, wide), 1) // size
    )
    same_place = ones_where(
        lax.broadcasted_iota(jnp.int32, (wide, wide), 0) % size
        == lax.broadcasted_iota(jnp.int32, (wide, wide), 1) % size
    )
    turned[...] = jnp.zeros_like(turned)
    turned[:heads, :rows] = state_max[...]
    old_max_lane = turned[...].T[:rows]
    turned[...] = jnp.zeros_like(turned)
    turned[0:1, :heads] = ibias[...]
    turned[1:2, :heads] = fbias[...]
    ibias_lane, fbias_lane = turned[0:1, :], turned[1:2, :]
    biases = jnp.concatenate(
        [ibias_lane + pltpu.roll(fbias_lane, heads, 1), jnp.zeros((7, LANES), f32)], axis=0
    )
    old_max_wide, bias_wide = (
        exact_dot([old_max_lane], chosen_head)[0][:, :wide],
        exact_dot([biases], chosen_head)[0][:1],
    )
    old_norm = jnp.concatenate([state_norm[:, head, :] for head in range(heads)], axis=1)

    close_plane(b_first, b_second)
    product = jnp.dot(arranged, weights_b[...], preferred_element_type=f32)
    outgoing_b[...] = product.astype(bf).reshape(lines, rows, pair)
    partial_b[...] = product.reshape(lines, rows, pair)
    pb_copies = send_partials(outgoing_b, arrived_b, pb_send, pb_recv)

    z_copies[2].wait_recv()
    for copy in z_copies:
        copy.wait_send()

    pl.semaphore_wait(ready, lines - 1)
    slanted = tuple(range(1, PLANE))
    early_tokens = scatter((0,), slanted, token_out, token_near, k_send, k_recv)
    o_first += [make_o(spot, 1 - held, 1, beside_peer), make_o(spot, 1 - held, 2, across_peer)]
    for copy in o_first[2:]:
        copy.start()
    pass_slab(w_planes.at[spot, my_rows])

    total = partial_a[line]
    for step in range(1, lines):
        pa_copies[step - 1].wait()
        total = total + arrived_a[step].astype(f32)
    gates_lane = total[:, pair:]
    gates_wide = exact_dot([gates_lane], chosen_head)[0]

    def gate_math(input_pre, forget_pre, old_max):
        log_forget = jnp.minimum(forget_pre, 0.0) - jnp.log(1.0 + jnp.exp(-jnp.abs(forget_pre)))
        new_max = jnp.maximum(log_forget + old_max, input_pre)
        return new_max, jnp.exp(log_forget + old_max - new_max), jnp.exp(input_pre - new_max)

    new_max, keep_old, keep_new = gate_math(
        gates_wide[:, :wide] + bias_wide[:, :wide],
        gates_wide[:, wide:] + bias_wide[:, wide:],
        old_max_wide,
    )
    query = total[:, :wide].astype(bf).astype(f32)
    key = total[:, wide:pair].astype(bf).astype(f32) * size ** (-0.5)
    pack = 2 * heads
    row = lax.broadcasted_iota(jnp.int32, (rows, pack, wide), 1)
    head = lax.broadcasted_iota(jnp.int32, (rows, pack, wide), 2) // size
    only = row == head
    spread_query = jnp.where(only, jnp.broadcast_to(query[:, None, :], only.shape), 0.0)
    tiled = jnp.dot(
        spread_query.reshape(rows * pack, wide).astype(bf),
        same_place,
        preferred_element_type=f32,
    )
    asked_shape = (rows * pack, wide)
    parity = (lax.broadcasted_iota(jnp.int32, asked_shape, 0) // pack) % 2
    lane_parity = (lax.broadcasted_iota(jnp.int32, asked_shape, 1) // size) % 2
    asked = jnp.where(parity == lane_parity, tiled, 0.0).astype(bf)
    for index in range(rows // 2):
        span = slice(2 * pack * index, 2 * pack * (index + 1))
        reads[span, :] = jnp.dot(asked[span], packed[index], preferred_element_type=f32)
    read_old = jnp.sum(jnp.where(only, reads[...].reshape(rows, pack, wide), 0.0), axis=1)
    query_key, query_norm = exact_dot([query * key, query * old_norm], same_head)
    divisor = jnp.maximum(
        jnp.abs(keep_old * query_norm + keep_new * query_key), jnp.exp(-new_max)
    )
    late = partial_b[line]
    for step in range(1, lines):
        pb_copies[step - 1].wait()
        late = late + arrived_b[step].astype(f32)
    value = late[:, :wide].astype(bf).astype(f32)
    outgate = late[:, wide:].astype(bf).astype(f32)
    read = (keep_old * read_old + keep_new * query_key * value) / divisor
    centered = read - exact_dot([read], same_head)[0] * (1.0 / size)
    variance = exact_dot([centered * centered], same_head)[0] * (1.0 / size)
    cell = (
        centered * lax.rsqrt(variance + 1e-06) * head_gain[...] * jax.nn.sigmoid(outgate)
    ).astype(bf)
    cell_mine[...] = cell
    swap = remote(cell_mine, cell_theirs, t_send.at[0], t_recv.at[0], partner)
    swap.start()
    pack_rows(cell, cell_out)
    everyone = range(len(line_of)), range(PLANE)
    cell_copies = scatter(*everyone, cell_out, cell_near, c_send, c_recv)
    late_tokens = scatter((1, 2), slanted, token_out, token_near, k_send, k_recv)
    late_tokens.update(
        scatter((own_group,), range(PLANE), token_out, token_near, k_send, k_recv)
    )
    for group in straight_tokens:
        (early_tokens if group in early_tokens else late_tokens)[group] += straight_tokens[group]

    o_first[0].wait_recv()
    o_second = [make_o(beside, held, 4, across_peer)]
    o_second[0].start()
    pass_slab(out_view(beside, held))
    o_first[1].wait_recv()
    pass_slab(out_view(across, held))
    o_first[3].wait_recv()
    o_second.append(make_o(across, 1 - held, 5, beside_peer))
    o_second[1].start()
    pass_slab(out_view(across, 1 - held))
    o_first[2].wait_recv()
    pass_slab(out_view(beside, 1 - held))

    lane_gates = gates_lane + pltpu.roll(gates_lane, LANES // 2, 1)
    lane_max, lane_old, lane_new = gate_math(
        lane_gates + ibias_lane,
        pltpu.roll(lane_gates, LANES - heads, 1) + fbias_lane,
        old_max_lane,
    )
    turned[:rows, :] = lane_max
    new_max_ref[...] = turned[...].T[:heads, :rows]
    row_lane = lax.broadcasted_iota(jnp.int32, (rows, pack, LANES), 1)
    lane = lax.broadcasted_iota(jnp.int32, (rows, pack, LANES), 2)
    chosen = ((row_lane == lane) | (row_lane == lane + heads)) & (lane < heads)

    def per_head(values):
        wider = jnp.broadcast_to(values[:, None, :], (rows, pack, LANES))
        return jnp.sum(jnp.where(chosen, wider, 0.0), axis=-1, keepdims=True)

    old_scale, new_scale = per_head(lane_old), per_head(lane_new)
    decay[...] = jnp.broadcast_to(old_scale, decay.shape)
    same = only | (row == head + heads)
    spread_key = jnp.where(same, jnp.broadcast_to(key[:, None, :], same.shape), 0.0)
    key_rows = jnp.dot(
        spread_key.reshape(rows * pack, wide).astype(bf),
        same_place[:, :size],
        preferred_element_type=f32,
    ).reshape(rows, pack, size)
    keys[...] = key_rows
    new_norm_ref[...] = (
        old_scale[:, :heads] * state_norm[...] + (new_scale * key_rows)[:, :heads]
    )
    scaled = jnp.where(same, jnp.broadcast_to(value[:, None, :], same.shape) * new_scale, 0.0)
    coarse = scaled.astype(bf).astype(f32)
    left[...] = jnp.where(row < heads, coarse, scaled - coarse)

    extra_rows, block_rows = area // 4, area // 2
    part_rows = block_rows + extra_rows
    sides = (1 - held, held)
    lift_row = lax.broadcasted_iota(jnp.int32, (extra_rows, block_rows), 0)
    lift_column = lax.broadcasted_iota(jnp.int32, (extra_rows, block_rows), 1)
    lift_place = (lift_row // (SUB // 2)) * SUB + lift_row % (SUB // 2)
    lift_low = ones_where(lift_column == lift_place)
    lift_high = ones_where(lift_column == lift_place + SUB // 2)

    def unpack_rows(source):
        middle = source.shape[2] // 3
        pieces = []
        for side in sides:
            span = place(side, count // 2)
            extra = source[span, :, 2 * middle :].reshape(block_rows, middle)
            pieces.append(source[span, :, : 2 * middle].reshape(block_rows, 2 * middle))
            pieces.append(
                jnp.concatenate(
                    [gather_rows(lift_low, extra), gather_rows(lift_high, extra)], axis=1
                )
            )
        return jnp.concatenate(pieces, axis=0)

    token_forwards = forward(early_tokens, token_near, token_far, kf_send, kf_recv)
    corner = PLANE - 1 - spot
    for part in range(2):
        o_second[part].wait_recv()
        pass_slab(out_view(corner, held if part == 0 else 1 - held))
    forwards = forward(cell_copies, cell_near, cell_far, f_send, f_recv)
    near_rows = unpack_rows(cell_near)
    for copy in o_first + o_second:
        copy.wait_send()
    for owner in range(PLANE):
        added[owner] = jnp.dot(near_rows, w_planes[owner, my_rows], preferred_element_type=f32)
    token_forwards += forward(late_tokens, token_near, token_far, kf_send, kf_recv)
    for copy in slabs:
        copy.wait()
    for copy in forwards:
        copy.wait()
    far_rows = unpack_rows(cell_far)
    for owner in range(PLANE):
        added[owner] += jnp.dot(far_rows, w_planes[owner, other_rows], preferred_element_type=f32)
    token_rows[:, my_half] = unpack_rows(token_near)
    for copy in token_forwards:
        copy.wait()
    token_rows[:, other_half] = unpack_rows(token_far)
    for copy in late_loads[7:]:
        copy.wait()
    quarter = half // 2
    middle = quarter // 2
    over = (((0,), (0,)), ((), ()))

    def raw_rows(index):
        span = slice(index * part_rows, (index + 1) * part_rows)
        squares = jnp.zeros((part_rows, columns), f32)
        for owner in range(PLANE):
            for step in range(lines):
                start = (step * PLANE + owner) * columns
                across_columns = slice(start, start + columns)
                summed = (
                    token_rows[span, across_columns].astype(f32)
                    + added[owner, span, step * columns : (step + 1) * columns]
                )
                widened = summed.astype(bf).astype(f32)
                row_values[span, across_columns] = (
                    widened * ffn_gain[:, across_columns]
                ).astype(bf)
                squares += widened * widened
        return squares

    def run_expert(index, squares):
        span = slice(index * part_rows, (index + 1) * part_rows)
        values = row_values[span, :]
        gate_pre = dot_t(values, w_gate[...])
        up_pre = dot_t(values, w_up[...])
        scale = lax.rsqrt(jnp.sum(squares, axis=-1, keepdims=True) * (1.0 / width) + 1e-06)
        gate_pre, up_pre = gate_pre * scale, up_pre * scale
        hidden = (gate_pre * jax.nn.sigmoid(gate_pre) * up_pre).astype(bf)
        swaps, kept = [], []
        for part in range(2):
            theirs = w_down[:, place((1 - tp) * 2 + part, quarter)]
            down_send[index, part] = jnp.dot(hidden, theirs, preferred_element_type=f32).astype(bf)
            slot = 2 + 2 * index + part
            copy = remote(
                down_send.at[index, part],
                down_recv.at[index, part],
                t_send.at[slot],
                t_recv.at[slot],
                partner,
            )
            copy.start()
            swaps.append(copy)
            mine = w_down[:, place(tp * 2 + part, quarter)]
            kept.append(jnp.dot(hidden, mine, preferred_element_type=f32).astype(bf))
        return swaps, kept

    def send_back(index, swaps, kept):
        span = place(sides[index], count // 2)
        groups = ((0, 1), (2, 3))[index]
        for part in range(2):
            swaps[part].wait()
            done = (kept[part].astype(f32) + down_recv[index, part].astype(f32)).astype(bf)
            finished[part, span, :, :quarter] = done[:block_rows].reshape(
                count // 2, SUB, quarter
            )
            folded = lax.dot_general(
                lift_low, done[block_rows:, :middle], over, preferred_element_type=f32
            ) + lax.dot_general(
                lift_high, done[block_rows:, middle:], over, preferred_element_type=f32
            )
            finished[part, span, :, quarter:] = folded.astype(bf).reshape(
                count // 2, SUB, middle
            )
            return_copies[part].update(
                scatter(
                    groups,
                    range(PLANE),
                    finished.at[part],
                    returned.at[part],
                    r_send.at[part],
                    r_recv.at[part],
                )
            )

    return_copies = [{}, {}]
    pending = run_expert(0, raw_rows(0))
    squares = raw_rows(1)
    send_back(0, *pending)
    send_back(1, *run_expert(1, squares))

    swap.wait()
    home_columns = pl.ds(pl.multiple_of(tp * part_wide, part_wide), part_wide)
    for owner in range(PLANE):
        shared = jnp.dot(
            cell_mine[...], w_planes[owner, my_rows, home_columns], preferred_element_type=f32
        ) + jnp.dot(
            cell_theirs[...], w_planes[owner, other_rows, home_columns], preferred_element_type=f32
        )
        for index in range(lines // 2):
            start = (index * PLANE + owner) * columns
            resid[:, start : start + columns] = shared[:, index * columns : (index + 1) * columns]
    resid[...] = (tokens[:, my_half].astype(f32) + resid[...]).astype(bf).astype(f32)

    @pl.loop(0, rows // 4)
    def _(group):
        for inner in range(4):
            item = group * 4 + inner
            outer = lax.dot_general(
                left[item].astype(bf), keys[item].astype(bf), over, preferred_element_type=f32
            ).reshape(heads, size, size)
            new_matrix_ref[item] = decay[item][:heads][:, None, :] * matrix[item] + outer

    def combine(index, values):
        both = jnp.dot(chosen_in[index], values, preferred_element_type=f32)
        return both[:rows] + both[rows:]

    swaps = []
    for part in range(2):
        for group in return_copies[part].values():
            for copy in group:
                copy.wait()
        back = returned[part, :, :, :quarter].reshape(area, quarter)
        extra = returned[part, :, :, quarter:].reshape(area, middle)
        weighted = combine(0, back) + jnp.concatenate(
            [combine(1, extra), combine(2, extra)], axis=1
        )
        span = slice(part * quarter, (part + 1) * quarter)
        last_send[part] = (resid[:, span] + weighted).astype(bf)
        copy = remote(
            last_send.at[part],
            last_recv.at[part],
            t_send.at[6 + part],
            t_recv.at[6 + part],
            partner,
        )
        copy.start()
        swaps.append(copy)
        mixed_ref[:, place(tp * 2 + part, quarter)] = last_send[part]
    for part in range(2):
        swaps[part].wait()
        mixed_ref[:, place((1 - tp) * 2 + part, quarter)] = last_recv[part]


def store_kernel(
    mixed_ref,
    matrix_ref,
    norm_ref,
    max_ref,
    mixed_out,
    matrix_out,
    norm_out,
    max_out,
    sems,
):
    chunks = 4
    tall = matrix_ref.shape[0] // chunks
    pairs = []
    for index in range(chunks):
        part = pl.ds(index * tall, tall)
        pairs.append((matrix_ref.at[part], matrix_out.at[part]))
    pairs += [(mixed_ref, mixed_out), (norm_ref, norm_out), (max_ref, max_out)]
    for copy in fetch_all(pairs, sems):
        copy.wait()


def layer_call(
    tokens,
    mix_gain,
    weight_list,
    igate_bias,
    fgate_bias,
    head_gain,
    w_out,
    state_matrix,
    state_norm,
    state_max,
    ffn_gain,
    expert_weights,
    routes,
    route_weights,
):
    rows, width = tokens.shape
    w_query, w_key, w_value, w_outgate, w_igate, w_fgate = weight_list
    depth, wide = w_query.shape
    count = lax.axis_size("ep")
    lines = count // PLANE
    heads = w_igate.shape[1]
    size = state_matrix.shape[3]
    half, block, pair, area = width // 2, depth * PLANE, 2 * wide, count * SUB
    slots = area + area // 2
    gate_t = jnp.swapaxes(expert_weights[0][0], 0, 1)
    up_t = jnp.swapaxes(expert_weights[1][0], 0, 1)
    down = expert_weights[2][0]
    vmem = pl.BlockSpec(memory_space=pltpu.VMEM)
    far = pl.BlockSpec(memory_space=pltpu.HBM)
    anywhere = pl.BlockSpec(memory_space=pl.ANY)
    dma = pltpu.SemaphoreType.DMA
    bf, f32 = jnp.bfloat16, jnp.float32
    shape = jax.ShapeDtypeStruct
    tile = (count, SUB, half + half // 2)
    thin = (count, SUB, wide + wide // 2)
    parts = (2, count, SUB, half // 2 + half // 4)
    made = (
        shape((rows, width), bf),
        shape(state_matrix.shape, f32),
        shape(state_norm.shape, f32),
        shape((heads, rows), f32),
    )
    operands = (
        tokens,
        mix_gain[None, :],
        w_query,
        w_key,
        w_value,
        w_outgate,
        jnp.swapaxes(w_igate, 0, 1),
        jnp.swapaxes(w_fgate, 0, 1),
        igate_bias[None, :],
        fgate_bias[None, :],
        head_gain[None, :],
        w_out,
        state_matrix,
        state_norm,
        jnp.swapaxes(state_max, 0, 1),
        ffn_gain[None, :],
        gate_t,
        up_t,
        down,
        jnp.swapaxes(routes, 0, 1),
        jnp.swapaxes(route_weights, 0, 1),
    )
    results = pl.pallas_call(
        functools.partial(layer_kernel, count),
        out_shape=made,
        in_specs=[far] * 21,
        out_specs=(vmem,) * 4,
        scratch_shapes=[
            pltpu.VMEM((rows, width), bf),
            pltpu.VMEM((1, width), f32),
            pltpu.VMEM((heads, depth), bf),
            pltpu.VMEM((heads, depth), bf),
            pltpu.VMEM((1, heads), f32),
            pltpu.VMEM((1, heads), f32),
            pltpu.VMEM((1, wide), f32),
            pltpu.VMEM(state_matrix.shape, f32),
            pltpu.VMEM(state_norm.shape, f32),
            pltpu.VMEM((heads, rows), f32),
            pltpu.VMEM((1, width), f32),
            pltpu.VMEM(gate_t.shape, bf),
            pltpu.VMEM(up_t.shape, bf),
            pltpu.VMEM(down.shape, bf),
            pltpu.VMEM((routes.shape[1], rows), jnp.int32),
            pltpu.VMEM((routes.shape[1], rows), f32),
            pltpu.VMEM((LANES, LANES), f32),
            pltpu.VMEM((PLANE, 2 * heads, depth), bf),
            pltpu.VMEM((LANES, block), bf),
            pltpu.VMEM((block, pair), bf),
            pltpu.VMEM((block, pair), bf),
            pltpu.VMEM((PLANE, pair, lines * w_out.shape[1]), bf),
            pltpu.VMEM((rows, width), bf),
            pltpu.VMEM((lines, rows, block), bf),
            pltpu.VMEM((lines, rows, pair + LANES), f32),
            pltpu.VMEM((lines, rows, pair), f32),
            pltpu.VMEM((lines, rows, pair + LANES), bf),
            pltpu.VMEM((lines, rows, pair), bf),
            pltpu.VMEM((lines, rows, pair + LANES), bf),
            pltpu.VMEM((lines, rows, pair), bf),
            pltpu.VMEM((rows // 2, wide, wide), bf),
            pltpu.VMEM((3, area, rows), bf),
            pltpu.VMEM((3, 2 * rows, area), bf),
            pltpu.VMEM(tile, bf),
            pltpu.VMEM(tile, bf),
            pltpu.VMEM(tile, bf),
            pltpu.VMEM((rows, wide), bf),
            pltpu.VMEM((rows, wide), bf),
            pltpu.VMEM(thin, bf),
            pltpu.VMEM(thin, bf),
            pltpu.VMEM(thin, bf),
            pltpu.VMEM((slots, width), bf),
            pltpu.VMEM((rows * 2 * heads, wide), f32),
            pltpu.VMEM((rows, 2 * heads, wide), f32),
            pltpu.VMEM((rows, 2 * heads, size), f32),
            pltpu.VMEM((rows, 2 * heads, size), f32),
            pltpu.VMEM((PLANE, slots, width // PLANE), f32),
            pltpu.VMEM((rows, half), f32),
            pltpu.VMEM((slots, width), bf),
            pltpu.VMEM((2, 2, slots // 2, half // 2), bf),
            pltpu.VMEM((2, 2, slots // 2, half // 2), bf),
            pltpu.VMEM(parts, bf),
            pltpu.VMEM(parts, bf),
            pltpu.VMEM((2, rows, half // 2), bf),
            pltpu.VMEM((2, rows, half // 2), bf),
            dma((11,)),
            dma((6,)),
            dma((6,)),
            dma((6,)),
            dma((6,)),
            dma((3,)),
            dma((3,)),
            dma((lines,)),
            dma((lines,)),
            dma((lines,)),
            dma((lines,)),
            dma((lines,)),
            dma((lines,)),
            dma((lines,)),
            dma((lines,)),
            dma((lines,)),
            dma((lines,)),
            dma((6,)),
            dma((6,)),
            dma((8,)),
            dma((8,)),
            dma((count,)),
            dma((count,)),
            dma((lines,)),
            dma((lines,)),
            dma((count,)),
            dma((count,)),
            dma((lines,)),
            dma((lines,)),
            dma((7,)),
            dma((7,)),
            dma((2, count)),
            dma((2, count)),
            pltpu.SemaphoreType.REGULAR,
        ],
        compiler_params=pltpu.CompilerParams(
            collective_id=0, has_side_effects=True, vmem_limit_bytes=LAYER_BYTES
        ),
    )(*[pltpu.with_memory_space_constraint(operand, pltpu.HBM) for operand in operands])
    mixed, new_matrix, new_norm, new_max = pl.pallas_call(
        store_kernel,
        out_shape=made,
        in_specs=[vmem] * 4,
        out_specs=(anywhere,) * 4,
        scratch_shapes=[dma((7,))],
        compiler_params=pltpu.CompilerParams(vmem_limit_bytes=STORE_BYTES),
    )(*results)
    return mixed, new_matrix, new_norm, jnp.swapaxes(new_max, 0, 1)


def rms_scale(values_in, gain_vec):
    widened = values_in.astype(jnp.float32)
    return (
        widened * lax.rsqrt(jnp.mean(widened * widened, axis=-1, keepdims=True) + 1e-06) * gain_vec
    )


def memory_cell(
    query,
    key_row,
    value_row,
    outgate,
    input_pre,
    forget_pre,
    head_gain,
    state_matrix,
    state_norm,
    state_max,
):
    seq_rows, head_count = input_pre.shape
    head_size = query.shape[1] // head_count
    query_heads = query.astype(jnp.float32).reshape(seq_rows, head_count, head_size)
    key_heads = key_row.astype(jnp.float32).reshape(
        seq_rows, head_count, head_size
    ) * head_size ** (-0.5)
    value_heads = value_row.astype(jnp.float32).reshape(seq_rows, head_count, head_size)
    log_forget = jax.nn.log_sigmoid(forget_pre)
    new_max = jnp.maximum(log_forget + state_max, input_pre)
    keep_old = jnp.exp(log_forget + state_max - new_max)
    keep_new = jnp.exp(input_pre - new_max)
    new_matrix = (
        keep_old[:, :, None, None] * state_matrix
        + keep_new[:, :, None, None] * value_heads[:, :, :, None] * key_heads[:, :, None, :]
    )
    new_norm = keep_old[:, :, None] * state_norm + keep_new[:, :, None] * key_heads
    numerator = jnp.einsum(
        "bhvd,bhd->bhv", new_matrix, query_heads, precision=lax.Precision.HIGHEST
    )
    denominator = jnp.sum(new_norm * query_heads, axis=-1)
    cell_read = numerator / jnp.maximum(jnp.abs(denominator), jnp.exp(-new_max))[:, :, None]
    centered = cell_read - jnp.mean(cell_read, axis=-1, keepdims=True)
    variance = jnp.mean(centered * centered, axis=-1, keepdims=True)
    scaled_cell = (centered * lax.rsqrt(variance + 1e-06)).reshape(seq_rows, head_count * head_size)
    cell_out = (scaled_cell * head_gain * jax.nn.sigmoid(outgate.astype(jnp.float32))).astype(
        jnp.bfloat16
    )
    return (cell_out, new_matrix, new_norm, new_max)


def kernels_fit(tokens, w_query, w_igate, w_out, w_expert_gate, routes):
    ep_count = lax.axis_size("ep")
    rows, width = tokens.shape
    capacity = max(2, 2 * rows * routes.shape[1] // (w_expert_gate.shape[0] * ep_count))
    return (
        lax.axis_size("tp") == 2
        and ep_count % (2 * PLANE) == 0
        and w_query.shape[0] == LANES
        and w_query.shape[1] % LANES == 0
        and w_out.shape[1] % LANES == 0
        and width % (2 * LANES) == 0
        and rows % 16 == 0
        and w_igate.shape[1] == 4
        and rows <= LANES
        and w_expert_gate.shape[0] == 1
        and capacity == SUB + SUB // 2
        and ep_count * SUB == LANES
        and ep_count // PLANE == 4
        and w_query.shape[1] == 2 * LANES
    )


def body(
    tokens,
    mix_gain,
    w_query,
    w_key,
    w_value,
    w_outgate,
    w_igate,
    w_fgate,
    igate_bias,
    fgate_bias,
    head_gain,
    w_out,
    state_matrix,
    state_norm,
    state_max,
    ffn_gain,
    w_expert_gate,
    w_expert_up,
    w_expert_down,
    routes,
    route_weights,
):
    seq_rows, width = tokens.shape
    weight_list = (w_query, w_key, w_value, w_outgate, w_igate, w_fgate)
    if kernels_fit(tokens, w_query, w_igate, w_out, w_expert_gate, routes):
        mixed, new_matrix, new_norm, new_max = layer_call(
            tokens,
            mix_gain,
            weight_list,
            igate_bias,
            fgate_bias,
            head_gain,
            w_out,
            state_matrix,
            state_norm,
            state_max,
            ffn_gain,
            (w_expert_gate, w_expert_up, w_expert_down),
            routes,
            route_weights,
        )
        return (mixed, new_matrix, new_norm, new_max)
    normed = rms_scale(tokens, mix_gain).astype(jnp.bfloat16)
    spread = lax.all_to_all(normed, "ep", split_axis=1, concat_axis=0, tiled=True)
    joined = jnp.concatenate(weight_list, axis=1)
    summed = lax.psum_scatter(
        jnp.dot(spread, joined, preferred_element_type=jnp.float32),
        "ep",
        scatter_dimension=0,
        tiled=True,
    )
    bounds = [0]
    for weight in weight_list:
        bounds.append(bounds[-1] + weight.shape[1])
    projected = tuple(
        (summed[:, bounds[index] : bounds[index + 1]] for index in range(len(weight_list)))
    )
    query = projected[0].astype(jnp.bfloat16)
    key_row = projected[1].astype(jnp.bfloat16)
    value_row = projected[2].astype(jnp.bfloat16)
    outgate = projected[3].astype(jnp.bfloat16)
    input_pre = projected[4] + igate_bias
    forget_pre = projected[5] + fgate_bias
    cell_out, new_matrix, new_norm, new_max = memory_cell(
        query,
        key_row,
        value_row,
        outgate,
        input_pre,
        forget_pre,
        head_gain,
        state_matrix,
        state_norm,
        state_max,
    )
    partial_out = jnp.dot(
        cell_out,
        lax.all_gather(w_out, "ep", axis=1, tiled=True),
        preferred_element_type=jnp.float32,
    )
    attended = lax.psum(partial_out.astype(jnp.bfloat16), "tp").astype(jnp.float32)
    resid = (tokens.astype(jnp.float32) + attended).astype(jnp.bfloat16)
    normed_two = rms_scale(resid, ffn_gain).astype(jnp.bfloat16)
    ep_count = lax.axis_size("ep")
    local_experts = w_expert_gate.shape[0]
    expert_total = local_experts * ep_count
    top_count = routes.shape[1]
    capacity = max(2, 2 * seq_rows * top_count // expert_total)
    flat_routes = routes.reshape(-1)
    onehot = (flat_routes[:, None] == jnp.arange(expert_total, dtype=jnp.int32)[None, :]).astype(
        jnp.int32
    )
    earlier = jnp.cumsum(onehot, axis=0, dtype=jnp.int32) - onehot
    slots = jnp.sum(onehot * earlier, axis=1, dtype=jnp.int32)
    targets = flat_routes * capacity + slots
    dispatch = (
        targets[:, None] == jnp.arange(expert_total * capacity, dtype=jnp.int32)[None, :]
    ).astype(jnp.bfloat16)
    route_rows = jnp.repeat(normed_two, top_count, axis=0)
    outgoing = jnp.einsum(
        "rs,rd->sd", dispatch, route_rows, preferred_element_type=jnp.float32
    ).astype(jnp.bfloat16)
    outgoing = outgoing.reshape(expert_total, capacity, width)
    received = lax.all_to_all(outgoing, "ep", split_axis=0, concat_axis=0, tiled=True)
    slot_count = received.shape[1]
    regrouped = received.reshape(ep_count, local_experts, slot_count, width)
    gate_pre = jnp.einsum(
        "nxcd,xdf->nxcf", regrouped, w_expert_gate, preferred_element_type=jnp.float32
    )
    up_pre = jnp.einsum(
        "nxcd,xdf->nxcf", regrouped, w_expert_up, preferred_element_type=jnp.float32
    )
    hidden = (jax.nn.silu(gate_pre) * up_pre).astype(jnp.bfloat16)
    partial_down = jnp.einsum(
        "nxcf,xfd->nxcd", hidden, w_expert_down, preferred_element_type=jnp.float32
    )
    expert_sum = lax.psum(partial_down.astype(jnp.bfloat16), "tp")
    finished = expert_sum.reshape(ep_count * local_experts, slot_count, width)
    returned = lax.all_to_all(finished, "ep", split_axis=0, concat_axis=0, tiled=True)
    picked = jnp.dot(
        dispatch,
        returned.reshape(expert_total * capacity, width),
        preferred_element_type=jnp.float32,
    )
    weighted = jnp.sum(
        picked.reshape(seq_rows, top_count, width) * route_weights[:, :, None], axis=1
    )
    mixed = (resid.astype(jnp.float32) + weighted).astype(jnp.bfloat16)
    return (mixed, new_matrix, new_norm, new_max)


def solution(mesh):
    placed = (
        P("ep", None),
        P(),
        P("ep", "tp"),
        P("ep", "tp"),
        P("ep", "tp"),
        P("ep", "tp"),
        P("ep", "tp"),
        P("ep", "tp"),
        P("tp"),
        P("tp"),
        P("tp"),
        P("tp", "ep"),
        P("ep", "tp", None, None),
        P("ep", "tp", None),
        P("ep", "tp"),
        P(),
        P("ep", None, "tp"),
        P("ep", None, "tp"),
        P("ep", "tp", None),
        P("ep", None),
        P("ep", None),
    )
    return jax.shard_map(
        body,
        mesh=mesh,
        in_specs=placed,
        out_specs=(P("ep", None), P("ep", "tp", None, None), P("ep", "tp", None), P("ep", "tp")),
        check_vma=False,
    )
```

```python
import functools

import jax
import jax.numpy as jnp
from jax import lax
from jax.experimental import pallas as pl
from jax.experimental.pallas import tpu as pltpu
from jax.sharding import PartitionSpec as P

MESH = pl.DeviceIdType.MESH
PLANE = 4
LANES = 128
SUB = 8
LAYER_BYTES = 40 * 1024 * 1024
STORE_BYTES = 8 * 1024 * 1024


def remote(src, dst, send_sem, recv_sem, target):
    return pltpu.make_async_remote_copy(
        src_ref=src,
        dst_ref=dst,
        send_sem=send_sem,
        recv_sem=recv_sem,
        device_id=target,
        device_id_type=MESH,
    )


def dot_t(left, right):
    return lax.dot_general(
        left, right, (((1,), (1,)), ((), ())), preferred_element_type=jnp.float32
    )


def fetch_all(pairs, sems):
    copies = []
    for index, (source, kept) in enumerate(pairs):
        copy = pltpu.make_async_copy(source, kept, sems.at[index])
        copy.start()
        copies.append(copy)
    return copies


def place(index, size):
    return pl.ds(pl.multiple_of(index * size, size), size)


def split_three(values):
    high = values.astype(jnp.bfloat16)
    rest = values - high.astype(jnp.float32)
    middle = rest.astype(jnp.bfloat16)
    return [high, middle, (rest - middle.astype(jnp.float32)).astype(jnp.bfloat16)]


def exact_dot(values, chosen):
    rows = values[0].shape[0]
    parts = [part for value in values for part in split_three(value)]
    product = jnp.dot(
        jnp.concatenate(parts, axis=0), chosen, preferred_element_type=jnp.float32
    )
    results = []
    for index in range(len(values)):
        start = 3 * index * rows
        pieces = [product[start + rows * part : start + rows * (part + 1)] for part in range(3)]
        results.append(pieces[0] + pieces[1] + pieces[2])
    return results


def ones_where(condition):
    return jnp.where(condition, 1.0, 0.0).astype(jnp.bfloat16)


def gather_rows(chosen, values):
    return jnp.dot(chosen, values, preferred_element_type=jnp.float32).astype(jnp.bfloat16)


def layer_kernel(
    count,
    tokens_hbm,
    mix_gain_hbm,
    wq_hbm,
    wk_hbm,
    wv_hbm,
    wg_hbm,
    igate_hbm,
    fgate_hbm,
    ibias_hbm,
    fbias_hbm,
    head_gain_hbm,
    w_out_hbm,
    matrix_hbm,
    norm_hbm,
    max_hbm,
    ffn_gain_hbm,
    w_gate_hbm,
    w_up_hbm,
    w_down_hbm,
    routes_hbm,
    route_weights_hbm,
    mixed_ref,
    new_matrix_ref,
    new_norm_ref,
    new_max_ref,
    tokens,
    mix_gain,
    igate,
    fgate,
    ibias,
    fbias,
    head_gain,
    matrix,
    state_norm,
    state_max,
    ffn_gain,
    w_gate,
    w_up,
    w_down,
    routes,
    route_weights,
    turned,
    gate_rows,
    gate_t,
    weights_a,
    weights_b,
    w_planes,
    normed,
    spread,
    partial_a,
    partial_b,
    outgoing_a,
    outgoing_b,
    arrived_a,
    arrived_b,
    packed,
    chosen_out,
    chosen_in,
    token_out,
    token_near,
    token_far,
    cell_mine,
    cell_theirs,
    cell_out,
    cell_near,
    cell_far,
    token_rows,
    reads,
    left,
    keys,
    decay,
    added,
    resid,
    row_values,
    down_send,
    down_recv,
    finished,
    returned,
    last_send,
    norm_made,
    max_made,
    local_sem,
    store_sem,
    a_send,
    a_recv,
    b_send,
    b_recv,
    g_send,
    g_recv,
    x_send,
    x_recv,
    y_send,
    y_recv,
    z_send,
    z_recv,
    pa_send,
    pa_recv,
    pb_send,
    pb_recv,
    o_send,
    o_recv,
    t_send,
    t_recv,
    kf_send,
    kf_recv,
    f_send,
    f_recv,
    w_send,
    w_recv,
    r_send,
    r_recv,
    ready,
):
    bf, f32 = jnp.bfloat16, jnp.float32
    ep, tp = lax.axis_index("ep"), lax.axis_index("tp")
    lines = count // PLANE
    line, spot = ep // PLANE, ep % PLANE
    rows, width = tokens.shape
    half = width // 2
    depth = wq_hbm.shape[0]
    block = depth * PLANE
    heads = igate.shape[0]
    size = matrix.shape[3]
    wide = heads * size
    pair = 2 * wide
    area = count * SUB
    top = route_weights.shape[0]
    columns = w_out_hbm.shape[1]
    slab = lines * columns
    part_wide = slab // 2
    partner = (ep, 1 - tp)
    beside = spot + 1 - 2 * (spot % 2)
    across = lax.rem(spot + 2, PLANE)
    beside_peer = (line * PLANE + beside, tp)
    across_peer = (line * PLANE + across, tp)
    corner_peer = (line * PLANE + PLANE - 1 - spot, tp)
    my_half, other_half = place(tp, half), place(1 - tp, half)
    my_rows, other_rows = place(tp, wide), place(1 - tp, wide)
    own_rows = place(spot, depth)

    def line_peer(step):
        other = lax.rem(line + step, lines)
        return other, (other * PLANE + spot, tp)

    first_loads = fetch_all(
        (
            (wq_hbm, weights_a.at[own_rows, :wide]),
            (wk_hbm, weights_a.at[own_rows, wide:]),
            (igate_hbm, igate),
            (fgate_hbm, fgate),
            (wv_hbm, weights_b.at[own_rows, :wide]),
            (wg_hbm, weights_b.at[own_rows, wide:]),
            (tokens_hbm, tokens),
            (mix_gain_hbm, mix_gain),
            (w_out_hbm, w_planes.at[spot, my_rows, place(line, columns)]),
            (routes_hbm, routes),
            (route_weights_hbm, route_weights),
        ),
        local_sem,
    )
    barrier = pltpu.get_barrier_semaphore()
    greeted = [beside_peer, across_peer, corner_peer, partner]
    greeted += [line_peer(step)[1] for step in range(1, lines)]
    for target in greeted:
        pl.semaphore_signal(barrier, inc=1, device_id=target, device_id_type=MESH)
    turned[...] = jnp.zeros_like(turned)
    gate_t[...] = jnp.zeros_like(gate_t)
    for copy in first_loads[:4]:
        copy.wait()
    turned[:heads, :] = igate[...].astype(f32)
    turned[heads : 2 * heads, :] = fgate[...].astype(f32)
    gate_rows[spot] = turned[: 2 * heads, :].astype(bf)
    pl.semaphore_wait(barrier, len(greeted))
    for step in range(1, lines):
        pl.semaphore_signal(ready, inc=1, device_id=line_peer(step)[1], device_id_type=MESH)

    def all_of(view, send, recv):
        return remote(view, view, send.at[0], recv, partner)

    def plane_copies(buffer_view, send, recv, kept=2):
        def make(owner, part, slot, target):
            view = buffer_view(owner, part)
            return remote(view, view, send.at[0], recv.at[min(slot, kept)], target)

        return make

    def weight_view(buffer):
        def view(owner, part):
            tall = depth // 2
            return buffer.at[pl.ds(pl.multiple_of(owner * depth + part * tall, tall), tall)]

        return view

    def out_view(owner, part):
        return w_planes.at[owner, my_rows, place(part, part_wide)]

    def open_plane(make):
        first = [
            make(spot, 0, 0, beside_peer),
            make(spot, 1, 1, across_peer),
            make(spot, 1, 2, beside_peer),
            make(spot, 0, 3, across_peer),
        ]
        for copy in first:
            copy.start()
        return first

    def relay_plane(make, first):
        first[0].wait_recv()
        ahead = make(beside, 0, 4, across_peer)
        ahead.start()
        first[1].wait_recv()
        aside = make(across, 1, 5, beside_peer)
        aside.start()

    def close_plane(buffer, send, recv):
        all_of(buffer.at[pl.ds(0, 2 * depth)], send, recv.at[2]).wait_recv()
        all_of(buffer.at[pl.ds(0, 3 * depth)], send, recv.at[2]).wait_send()

    make_a = plane_copies(weight_view(weights_a), a_send, a_recv)
    make_b = plane_copies(weight_view(weights_b), b_send, b_recv)
    make_o = plane_copies(out_view, o_send, o_recv, 5)
    a_first = open_plane(make_a)
    for target in (beside_peer, across_peer, corner_peer):
        view = gate_rows.at[spot]
        remote(view, view, g_send.at[0], g_recv.at[0], target).start()
    for copy in first_loads[4:9]:
        copy.wait()
    widened = tokens[...].astype(f32)
    scale = lax.rsqrt(jnp.mean(widened * widened, axis=-1, keepdims=True) + 1e-06)
    normed[...] = (widened * scale * mix_gain[...]).astype(bf)
    x_copies = []
    narrow = block // 2
    my_part = place(tp, narrow)
    for step in range(1, lines):
        other, target = line_peer(step)
        copy = remote(
            normed.at[:, place(other * 2 + tp, narrow)],
            spread.at[line, :, my_part],
            x_send.at[0],
            x_recv.at[step - 1],
            target,
        )
        copy.start()
        x_copies.append(copy)
    near_line = line + 1 - 2 * (line % 2)
    mirror_line = lines - 1 - line
    near_peer = (near_line * PLANE + spot, tp)
    mirror_peer = (mirror_line * PLANE + spot, tp)

    def line_copy(owner, slot, target):
        view = w_planes.at[spot, my_rows, place(owner, columns)]
        return remote(view, view, z_send.at[0], z_recv.at[slot], target)

    z_copies = [line_copy(line, 0, near_peer), line_copy(line, 1, mirror_peer)]
    for copy in z_copies:
        copy.start()
    spread[line] = normed[:, place(line, block)]
    for copy in first_loads[9:]:
        copy.wait()
    late_loads = fetch_all(
        (
            (matrix_hbm, matrix),
            (norm_hbm, state_norm),
            (max_hbm, state_max),
            (ibias_hbm, ibias),
            (fbias_hbm, fbias),
            (head_gain_hbm, head_gain),
            (ffn_gain_hbm, ffn_gain),
            (w_gate_hbm, w_gate),
            (w_up_hbm, w_up),
            (w_down_hbm, w_down),
        ),
        local_sem,
    )

    slot_row = lax.broadcasted_iota(jnp.int32, (area, rows), 0).astype(f32)
    expert = lax.broadcasted_iota(jnp.int32, (count, rows), 0).astype(f32)
    before = jnp.where(
        lax.broadcasted_iota(jnp.int32, (rows, rows), 0)
        < lax.broadcasted_iota(jnp.int32, (rows, rows), 1),
        1.0,
        0.0,
    )
    taken = jnp.zeros((count, 1), f32)
    sent = [jnp.zeros((area, rows), f32) for _ in range(3)]
    mixes = [jnp.zeros((area, rows), f32) for _ in range(3)]
    for k in range(top):
        named = routes[k : k + 1, :].astype(f32)
        match = jnp.where(expert == named, 1.0, 0.0)
        earlier = jnp.dot(match, before, preferred_element_type=f32) + taken
        taken = taken + jnp.sum(match, axis=1, keepdims=True)
        position = jnp.sum(match * earlier, axis=0, keepdims=True)
        low = jnp.where(position < SUB, named * SUB + position, -1000.0)
        high = jnp.where(position < SUB, -1000.0, named * SUB + position - SUB)
        for index, target in enumerate((low, high, high + SUB // 2)):
            hit = slot_row == target
            sent[index] += jnp.where(hit, 1.0, 0.0)
            mixes[index] += jnp.where(hit, route_weights[k : k + 1, :], 0.0)
    for index in range(3):
        chosen_out[index] = sent[index].astype(bf)
        coarse = mixes[index].astype(bf).astype(f32)
        joined = jnp.concatenate(
            [coarse, mixes[index] - coarse, jnp.zeros((area, area - 2 * rows), f32)], axis=1
        )
        chosen_in[index] = joined.T[: 2 * rows].astype(bf)

    line_of = (lax.rem(line + lines // 2, lines), mirror_line, near_line, line)
    own_group = len(line_of) - 1
    spot_of = (spot, beside, across, PLANE - 1 - spot)

    def scatter(groups, turns, source, near, family):
        for group in groups:
            for turn in turns:
                if group == own_group and turn == 0:
                    near[ep] = source[ep]
                    continue
                other = line_of[group] * PLANE + spot_of[turn]
                remote(
                    source.at[other],
                    near.at[ep],
                    r_send.at[family],
                    r_recv.at[family, group],
                    (other, tp),
                ).start()

    def wait_group(group, near, family):
        span = pl.ds(0, PLANE - 1) if group == own_group else place(line_of[group], PLANE)
        view = near.at[span]
        remote(view, view, r_send.at[family], r_recv.at[family, group], partner).wait_recv()

    def wait_sent(source, family):
        view = source.at[pl.ds(0, count - 1)]
        remote(view, view, r_send.at[family], r_recv.at[family, 0], partner).wait_send()

    def forward(groups, near, far, family, send, recv):
        for group in groups:
            wait_group(group, near, family)
            span = place(line_of[group], PLANE)
            remote(near.at[span], far.at[span], send.at[0], recv.at[0], partner).start()

    def pack_rows(values, target):
        middle = values.shape[1] // 2
        target[:, :, : 2 * middle] = gather_rows(chosen_out[0], values).reshape(
            count, SUB, 2 * middle
        )
        extra = jnp.dot(chosen_out[1], values[:, :middle], preferred_element_type=f32)
        extra += jnp.dot(chosen_out[2], values[:, middle:], preferred_element_type=f32)
        target[:, :, 2 * middle :] = extra.astype(bf).reshape(count, SUB, middle)

    relay_plane(make_a, a_first)
    b_first = open_plane(make_b)
    pack_rows(tokens[:, my_half], token_out)
    scatter(range(own_group), (0,), token_out, token_near, 0)
    late_loads[0].wait()

    def pack_matrix(start, stop):
        @pl.loop(start, stop)
        def _(index):
            item = 2 * index
            joined = jnp.concatenate(
                [matrix[item].reshape(wide, size), matrix[item + 1].reshape(wide, size)], axis=1
            )
            flipped = joined.T
            upper = flipped.astype(bf)
            packed[index, : 2 * size] = upper
            packed[index, 2 * size :] = (flipped - upper.astype(f32)).astype(bf)

    for step in range(1, lines):
        x_copies[step - 1].wait_recv()
        view = spread.at[lax.rem(line + lines - step, lines), :, my_part]
        remote(view, view, y_send.at[0], y_recv.at[0], partner).start()
    pack_matrix(0, rows // 4)
    all_of(gate_rows.at[pl.ds(0, PLANE - 1)], g_send, g_recv.at[0]).wait()
    for owner in range(PLANE):
        part = gate_rows[owner]
        gate_t[: 2 * heads, owner * depth : (owner + 1) * depth] = part
        gate_t[LANES // 2 : LANES // 2 + 2 * heads, owner * depth : (owner + 1) * depth] = part
    others = pl.ds(1, lines - 1)
    all_of(spread.at[others, :, my_part], x_send, x_recv.at[0]).wait_send()
    all_of(spread.at[others, :, my_part], y_send, y_recv.at[0]).wait()
    close_plane(weights_a, a_send, a_recv)
    arranged = spread[...].reshape(lines * rows, block)
    product = jnp.dot(arranged, weights_a[...], preferred_element_type=f32)
    gates = dot_t(arranged, gate_t[...])
    coarse = gates.astype(bf).astype(f32)
    first = lax.broadcasted_iota(jnp.int32, gates.shape, 1) < LANES // 2
    picked = jnp.where(first, coarse, gates - coarse).astype(bf)
    outgoing_a[:, :, :pair] = product.astype(bf).reshape(lines, rows, pair)
    outgoing_a[:, :, pair:] = picked.reshape(lines, rows, LANES)
    partial_a[:, :, :pair] = product.reshape(lines, rows, pair)
    partial_a[:, :, pair:] = jnp.where(first, gates, 0.0).reshape(lines, rows, LANES)

    def send_partials(outgoing, arrived, send, recv):
        for step in range(1, lines):
            other, target = line_peer(step)
            remote(
                outgoing.at[other], arrived.at[step], send.at[0], recv.at[0], target
            ).start()

    z_copies[1].wait_recv()
    z_copies.append(line_copy(mirror_line, 2, near_peer))
    z_copies[2].start()
    send_partials(outgoing_a, arrived_a, pa_send, pa_recv)
    relay_plane(make_b, b_first)
    z_copies[0].wait_recv()
    held = line // (lines // 2)
    o_first = [make_o(spot, held, 0, beside_peer), make_o(spot, held, 3, across_peer)]
    for copy in o_first:
        copy.start()

    def pass_slab(view):
        remote(view, view, w_send.at[0], w_recv.at[0], partner).start()

    pack_matrix(rows // 4, rows // 2)
    for copy in late_loads[1:7]:
        copy.wait()

    chosen_head = ones_where(
        lax.broadcasted_iota(jnp.int32, (LANES, pair), 0) % (LANES // 2)
        == lax.broadcasted_iota(jnp.int32, (LANES, pair), 1) // size
    )
    same_head = ones_where(
        lax.broadcasted_iota(jnp.int32, (wide, wide), 0) // size
        == lax.broadcasted_iota(jnp.int32, (wide, wide), 1) // size
    )
    same_place = ones_where(
        lax.broadcasted_iota(jnp.int32, (wide, wide), 0) % size
        == lax.broadcasted_iota(jnp.int32, (wide, wide), 1) % size
    )
    turned[...] = jnp.zeros_like(turned)
    turned[:heads, :rows] = state_max[...]
    old_max_lane = turned[...].T[:rows]
    turned[...] = jnp.zeros_like(turned)
    turned[0:1, :heads] = ibias[...]
    turned[1:2, :heads] = fbias[...]
    ibias_lane, fbias_lane = turned[0:1, :], turned[1:2, :]
    biases = jnp.concatenate(
        [ibias_lane + pltpu.roll(fbias_lane, heads, 1), jnp.zeros((7, LANES), f32)], axis=0
    )
    old_max_wide, bias_wide = (
        exact_dot([old_max_lane], chosen_head)[0][:, :wide],
        exact_dot([biases], chosen_head)[0][:1],
    )
    old_norm = jnp.concatenate([state_norm[:, head, :] for head in range(heads)], axis=1)

    close_plane(weights_b, b_send, b_recv)
    product = jnp.dot(arranged, weights_b[...], preferred_element_type=f32)
    outgoing_b[...] = product.astype(bf).reshape(lines, rows, pair)
    partial_b[...] = product.reshape(lines, rows, pair)
    send_partials(outgoing_b, arrived_b, pb_send, pb_recv)

    z_copies[2].wait_recv()
    all_of(w_planes.at[spot, my_rows, pl.ds(0, 3 * columns)], z_send, z_recv.at[0]).wait_send()

    pl.semaphore_wait(ready, lines - 1)
    slanted = tuple(range(PLANE - 1, 0, -1))
    scatter((0, own_group), slanted, token_out, token_near, 0)
    token_near[ep] = token_out[ep]
    o_first += [make_o(spot, 1 - held, 1, beside_peer), make_o(spot, 1 - held, 2, across_peer)]
    for copy in o_first[2:]:
        copy.start()
    pass_slab(w_planes.at[spot, my_rows])

    total = partial_a[line]
    all_of(arrived_a.at[others], pa_send, pa_recv.at[0]).wait()
    for step in range(1, lines):
        total = total + arrived_a[step].astype(f32)
    gates_lane = total[:, pair:]
    gates_wide = exact_dot([gates_lane], chosen_head)[0]

    def gate_math(input_pre, forget_pre, old_max):
        log_forget = jnp.minimum(forget_pre, 0.0) - jnp.log(1.0 + jnp.exp(-jnp.abs(forget_pre)))
        new_max = jnp.maximum(log_forget + old_max, input_pre)
        return new_max, jnp.exp(log_forget + old_max - new_max), jnp.exp(input_pre - new_max)

    new_max, keep_old, keep_new = gate_math(
        gates_wide[:, :wide] + bias_wide[:, :wide],
        gates_wide[:, wide:] + bias_wide[:, wide:],
        old_max_wide,
    )
    query = total[:, :wide].astype(bf).astype(f32)
    key = total[:, wide:pair].astype(bf).astype(f32) * size ** (-0.5)
    pack = 2 * heads
    row = lax.broadcasted_iota(jnp.int32, (rows, pack, wide), 1)
    head = lax.broadcasted_iota(jnp.int32, (rows, pack, wide), 2) // size
    only = row == head
    spread_query = jnp.where(only, jnp.broadcast_to(query[:, None, :], only.shape), 0.0)
    tiled = jnp.dot(
        spread_query.reshape(rows * pack, wide).astype(bf),
        same_place,
        preferred_element_type=f32,
    )
    asked_shape = (rows * pack, wide)
    parity = (lax.broadcasted_iota(jnp.int32, asked_shape, 0) // pack) % 2
    lane_parity = (lax.broadcasted_iota(jnp.int32, asked_shape, 1) // size) % 2
    asked = jnp.where(parity == lane_parity, tiled, 0.0).astype(bf)
    for index in range(rows // 2):
        span = slice(2 * pack * index, 2 * pack * (index + 1))
        reads[span, :] = jnp.dot(asked[span], packed[index], preferred_element_type=f32)
    read_old = jnp.sum(jnp.where(only, reads[...].reshape(rows, pack, wide), 0.0), axis=1)
    query_key, query_norm = exact_dot([query * key, query * old_norm], same_head)
    divisor = jnp.maximum(
        jnp.abs(keep_old * query_norm + keep_new * query_key), jnp.exp(-new_max)
    )
    late = partial_b[line]
    all_of(arrived_b.at[others], pb_send, pb_recv.at[0]).wait()
    for step in range(1, lines):
        late = late + arrived_b[step].astype(f32)
    value = late[:, :wide].astype(bf).astype(f32)
    outgate = late[:, wide:].astype(bf).astype(f32)
    read = (keep_old * read_old + keep_new * query_key * value) / divisor
    centered = read - exact_dot([read], same_head)[0] * (1.0 / size)
    variance = exact_dot([centered * centered], same_head)[0] * (1.0 / size)
    cell = (
        centered * lax.rsqrt(variance + 1e-06) * head_gain[...] * jax.nn.sigmoid(outgate)
    ).astype(bf)
    cell_mine[...] = cell
    swap = remote(cell_mine, cell_theirs, t_send.at[0], t_recv.at[0], partner)
    swap.start()
    pack_rows(cell, cell_out)
    everyone = range(len(line_of))
    scatter(everyone, slanted + (0,), cell_out, cell_near, 1)
    scatter((1, 2), slanted, token_out, token_near, 0)
    o_first[0].wait_recv()
    o_second = [make_o(beside, held, 4, across_peer)]
    o_second[0].start()
    pass_slab(out_view(beside, held))
    o_first[1].wait_recv()
    pass_slab(out_view(across, held))
    o_first[3].wait_recv()
    o_second.append(make_o(across, 1 - held, 5, beside_peer))
    o_second[1].start()
    pass_slab(out_view(across, 1 - held))
    o_first[2].wait_recv()
    pass_slab(out_view(beside, 1 - held))

    lane_gates = gates_lane + pltpu.roll(gates_lane, LANES // 2, 1)
    lane_max, lane_old, lane_new = gate_math(
        lane_gates + ibias_lane,
        pltpu.roll(lane_gates, LANES - heads, 1) + fbias_lane,
        old_max_lane,
    )
    turned[:rows, :] = lane_max
    max_made[...] = turned[...].T[:heads, :rows]
    row_lane = lax.broadcasted_iota(jnp.int32, (rows, pack, LANES), 1)
    lane = lax.broadcasted_iota(jnp.int32, (rows, pack, LANES), 2)
    chosen = ((row_lane == lane) | (row_lane == lane + heads)) & (lane < heads)

    def per_head(values):
        wider = jnp.broadcast_to(values[:, None, :], (rows, pack, LANES))
        return jnp.sum(jnp.where(chosen, wider, 0.0), axis=-1, keepdims=True)

    old_scale, new_scale = per_head(lane_old), per_head(lane_new)
    decay[...] = jnp.broadcast_to(old_scale, decay.shape)
    same = only | (row == head + heads)
    spread_key = jnp.where(same, jnp.broadcast_to(key[:, None, :], same.shape), 0.0)
    key_rows = jnp.dot(
        spread_key.reshape(rows * pack, wide).astype(bf),
        same_place[:, :size],
        preferred_element_type=f32,
    ).reshape(rows, pack, size)
    keys[...] = key_rows
    norm_made[...] = (
        old_scale[:, :heads] * state_norm[...] + (new_scale * key_rows)[:, :heads]
    )
    scaled = jnp.where(same, jnp.broadcast_to(value[:, None, :], same.shape) * new_scale, 0.0)
    coarse = scaled.astype(bf).astype(f32)
    left[...] = jnp.where(row < heads, coarse, scaled - coarse)
    stores = fetch_all(((norm_made, new_norm_ref), (max_made, new_max_ref)), store_sem)

    extra_rows, block_rows = area // 4, area // 2
    part_rows = block_rows + extra_rows
    sides = (1 - held, held)
    lift_row = lax.broadcasted_iota(jnp.int32, (extra_rows, block_rows), 0)
    lift_column = lax.broadcasted_iota(jnp.int32, (extra_rows, block_rows), 1)
    lift_place = (lift_row // (SUB // 2)) * SUB + lift_row % (SUB // 2)
    lift_low = ones_where(lift_column == lift_place)
    lift_high = ones_where(lift_column == lift_place + SUB // 2)

    def unpack_rows(source):
        middle = source.shape[2] // 3
        pieces = []
        for side in sides:
            span = place(side, count // 2)
            extra = source[span, :, 2 * middle :].reshape(block_rows, middle)
            pieces.append(source[span, :, : 2 * middle].reshape(block_rows, 2 * middle))
            pieces.append(
                jnp.concatenate(
                    [gather_rows(lift_low, extra), gather_rows(lift_high, extra)], axis=1
                )
            )
        return jnp.concatenate(pieces, axis=0)

    forward((0, own_group), token_near, token_far, 0, kf_send, kf_recv)
    corner = PLANE - 1 - spot
    for part in range(2):
        o_second[part].wait_recv()
        pass_slab(out_view(corner, held if part == 0 else 1 - held))
    forward(everyone, cell_near, cell_far, 1, f_send, f_recv)
    near_rows = unpack_rows(cell_near)
    all_of(w_planes.at[pl.ds(0, PLANE - 1), my_rows], o_send, o_recv.at[0]).wait_send()
    for owner in range(PLANE):
        added[owner] = jnp.dot(near_rows, w_planes[owner, my_rows], preferred_element_type=f32)
    forward((1, 2), token_near, token_far, 0, kf_send, kf_recv)
    token_rows[:, my_half] = unpack_rows(token_near)
    all_of(w_planes.at[:, my_rows], w_send, w_recv.at[0]).wait()
    all_of(cell_near, f_send, f_recv.at[0]).wait()
    far_rows = unpack_rows(cell_far)
    for owner in range(PLANE):
        added[owner] += jnp.dot(far_rows, w_planes[owner, other_rows], preferred_element_type=f32)
    all_of(token_near, kf_send, kf_recv.at[0]).wait()
    token_rows[:, other_half] = unpack_rows(token_far)
    for copy in late_loads[7:]:
        copy.wait()
    quarter = half // 2
    middle = quarter // 2
    over = (((0,), (0,)), ((), ()))

    def raw_rows(index):
        span = slice(index * part_rows, (index + 1) * part_rows)
        squares = jnp.zeros((part_rows, columns), f32)
        for owner in range(PLANE):
            for step in range(lines):
                start = (step * PLANE + owner) * columns
                across_columns = slice(start, start + columns)
                summed = (
                    token_rows[span, across_columns].astype(f32)
                    + added[owner, span, step * columns : (step + 1) * columns]
                )
                widened = summed.astype(bf).astype(f32)
                row_values[span, across_columns] = (
                    widened * ffn_gain[:, across_columns]
                ).astype(bf)
                squares += widened * widened
        return squares

    def run_expert(index, squares):
        span = slice(index * part_rows, (index + 1) * part_rows)
        values = row_values[span, :]
        gate_pre = dot_t(values, w_gate[...])
        up_pre = dot_t(values, w_up[...])
        scale = lax.rsqrt(jnp.sum(squares, axis=-1, keepdims=True) * (1.0 / width) + 1e-06)
        gate_pre, up_pre = gate_pre * scale, up_pre * scale
        hidden = (gate_pre * jax.nn.sigmoid(gate_pre) * up_pre).astype(bf)
        swaps, kept = [], []
        for part in range(2):
            theirs = w_down[:, place((1 - tp) * 2 + part, quarter)]
            down_send[index, part] = jnp.dot(hidden, theirs, preferred_element_type=f32).astype(bf)
            slot = 1 + 2 * index + part
            copy = remote(
                down_send.at[index, part],
                down_recv.at[index, part],
                t_send.at[slot],
                t_recv.at[slot],
                partner,
            )
            copy.start()
            swaps.append(copy)
            mine = w_down[:, place(tp * 2 + part, quarter)]
            kept.append(jnp.dot(hidden, mine, preferred_element_type=f32).astype(bf))
        return swaps, kept

    def send_back(index, swaps, kept):
        span = place(sides[index], count // 2)
        groups = ((0, 1), (2, 3))[index]
        for part in range(2):
            swaps[part].wait()
            done = (kept[part].astype(f32) + down_recv[index, part].astype(f32)).astype(bf)
            finished[part, span, :, :quarter] = done[:block_rows].reshape(
                count // 2, SUB, quarter
            )
            folded = lax.dot_general(
                lift_low, done[block_rows:, :middle], over, preferred_element_type=f32
            ) + lax.dot_general(
                lift_high, done[block_rows:, middle:], over, preferred_element_type=f32
            )
            finished[part, span, :, quarter:] = folded.astype(bf).reshape(
                count // 2, SUB, middle
            )
            scatter(groups, slanted + (0,), finished.at[part], returned.at[part], 2 + part)

    pending = run_expert(0, raw_rows(0))
    squares = raw_rows(1)
    send_back(0, *pending)
    send_back(1, *run_expert(1, squares))

    swap.wait()
    wait_sent(token_out, 0)
    wait_sent(cell_out, 1)
    home_columns = pl.ds(pl.multiple_of(tp * part_wide, part_wide), part_wide)
    for owner in range(PLANE):
        shared = jnp.dot(
            cell_mine[...], w_planes[owner, my_rows, home_columns], preferred_element_type=f32
        ) + jnp.dot(
            cell_theirs[...], w_planes[owner, other_rows, home_columns], preferred_element_type=f32
        )
        for index in range(lines // 2):
            start = (index * PLANE + owner) * columns
            resid[:, start : start + columns] = shared[:, index * columns : (index + 1) * columns]
    resid[...] = (tokens[:, my_half].astype(f32) + resid[...]).astype(bf).astype(f32)

    @pl.loop(0, rows // 4)
    def _(group):
        for inner in range(4):
            item = group * 4 + inner
            outer = lax.dot_general(
                left[item].astype(bf), keys[item].astype(bf), over, preferred_element_type=f32
            ).reshape(heads, size, size)
            matrix[item] = decay[item][:heads][:, None, :] * matrix[item] + outer

    store = pltpu.make_async_copy(matrix, new_matrix_ref, store_sem.at[2])
    store.start()
    stores.append(store)

    def combine(index, values):
        both = jnp.dot(chosen_in[index], values, preferred_element_type=f32)
        return both[:rows] + both[rows:]

    swaps = []
    for part in range(2):
        for group in everyone:
            wait_group(group, returned.at[part], 2 + part)
        back = returned[part, :, :, :quarter].reshape(area, quarter)
        extra = returned[part, :, :, quarter:].reshape(area, middle)
        weighted = combine(0, back) + jnp.concatenate(
            [combine(1, extra), combine(2, extra)], axis=1
        )
        span = slice(part * quarter, (part + 1) * quarter)
        last_send[part] = (resid[:, span] + weighted).astype(bf)
        target = mixed_ref.at[:, place(tp * 2 + part, quarter)]
        copy = remote(
            last_send.at[part], target, t_send.at[5 + part], t_recv.at[5 + part], partner
        )
        copy.start()
        swaps.append(copy)
        store = pltpu.make_async_copy(last_send.at[part], target, store_sem.at[3 + part])
        store.start()
        stores.append(store)
    for part in range(2):
        wait_sent(finished.at[part], 2 + part)
    for copy in stores + swaps:
        copy.wait()


def store_kernel(
    mixed_ref,
    matrix_ref,
    norm_ref,
    max_ref,
    mixed_out,
    matrix_out,
    norm_out,
    max_out,
    sems,
):
    chunks = 4
    tall = matrix_ref.shape[0] // chunks
    pairs = []
    for index in range(chunks):
        part = pl.ds(index * tall, tall)
        pairs.append((matrix_ref.at[part], matrix_out.at[part]))
    pairs += [(mixed_ref, mixed_out), (norm_ref, norm_out), (max_ref, max_out)]
    for copy in fetch_all(pairs, sems):
        copy.wait()


def layer_call(
    tokens,
    mix_gain,
    weight_list,
    igate_bias,
    fgate_bias,
    head_gain,
    w_out,
    state_matrix,
    state_norm,
    state_max,
    ffn_gain,
    expert_weights,
    routes,
    route_weights,
):
    rows, width = tokens.shape
    w_query, w_key, w_value, w_outgate, w_igate, w_fgate = weight_list
    depth, wide = w_query.shape
    count = lax.axis_size("ep")
    lines = count // PLANE
    heads = w_igate.shape[1]
    size = state_matrix.shape[3]
    half, block, pair, area = width // 2, depth * PLANE, 2 * wide, count * SUB
    slots = area + area // 2
    gate_t = jnp.swapaxes(expert_weights[0][0], 0, 1)
    up_t = jnp.swapaxes(expert_weights[1][0], 0, 1)
    down = expert_weights[2][0]
    vmem = pl.BlockSpec(memory_space=pltpu.VMEM)
    far = pl.BlockSpec(memory_space=pltpu.HBM)
    anywhere = pl.BlockSpec(memory_space=pl.ANY)
    dma = pltpu.SemaphoreType.DMA
    bf, f32 = jnp.bfloat16, jnp.float32
    shape = jax.ShapeDtypeStruct
    tile = (count, SUB, half + half // 2)
    thin = (count, SUB, wide + wide // 2)
    parts = (2, count, SUB, half // 2 + half // 4)
    made = (
        shape((rows, width), bf),
        shape(state_matrix.shape, f32),
        shape(state_norm.shape, f32),
        shape((heads, rows), f32),
    )
    operands = (
        tokens,
        mix_gain[None, :],
        w_query,
        w_key,
        w_value,
        w_outgate,
        jnp.swapaxes(w_igate, 0, 1),
        jnp.swapaxes(w_fgate, 0, 1),
        igate_bias[None, :],
        fgate_bias[None, :],
        head_gain[None, :],
        w_out,
        state_matrix,
        state_norm,
        jnp.swapaxes(state_max, 0, 1),
        ffn_gain[None, :],
        gate_t,
        up_t,
        down,
        jnp.swapaxes(routes, 0, 1),
        jnp.swapaxes(route_weights, 0, 1),
    )
    results = pl.pallas_call(
        functools.partial(layer_kernel, count),
        out_shape=tuple(pltpu.VMEM(each.shape, each.dtype) for each in made),
        in_specs=[far] * 21,
        out_specs=(anywhere,) * 4,
        scratch_shapes=[
            pltpu.VMEM((rows, width), bf),
            pltpu.VMEM((1, width), f32),
            pltpu.VMEM((heads, depth), bf),
            pltpu.VMEM((heads, depth), bf),
            pltpu.VMEM((1, heads), f32),
            pltpu.VMEM((1, heads), f32),
            pltpu.VMEM((1, wide), f32),
            pltpu.VMEM(state_matrix.shape, f32),
            pltpu.VMEM(state_norm.shape, f32),
            pltpu.VMEM((heads, rows), f32),
            pltpu.VMEM((1, width), f32),
            pltpu.VMEM(gate_t.shape, bf),
            pltpu.VMEM(up_t.shape, bf),
            pltpu.VMEM(down.shape, bf),
            pltpu.VMEM((routes.shape[1], rows), jnp.int32),
            pltpu.VMEM((routes.shape[1], rows), f32),
            pltpu.VMEM((LANES, LANES), f32),
            pltpu.VMEM((PLANE, 2 * heads, depth), bf),
            pltpu.VMEM((LANES, block), bf),
            pltpu.VMEM((block, pair), bf),
            pltpu.VMEM((block, pair), bf),
            pltpu.VMEM((PLANE, pair, lines * w_out.shape[1]), bf),
            pltpu.VMEM((rows, width), bf),
            pltpu.VMEM((lines, rows, block), bf),
            pltpu.VMEM((lines, rows, pair + LANES), f32),
            pltpu.VMEM((lines, rows, pair), f32),
            pltpu.VMEM((lines, rows, pair + LANES), bf),
            pltpu.VMEM((lines, rows, pair), bf),
            pltpu.VMEM((lines, rows, pair + LANES), bf),
            pltpu.VMEM((lines, rows, pair), bf),
            pltpu.VMEM((rows // 2, wide, wide), bf),
            pltpu.VMEM((3, area, rows), bf),
            pltpu.VMEM((3, 2 * rows, area), bf),
            pltpu.VMEM(tile, bf),
            pltpu.VMEM(tile, bf),
            pltpu.VMEM(tile, bf),
            pltpu.VMEM((rows, wide), bf),
            pltpu.VMEM((rows, wide), bf),
            pltpu.VMEM(thin, bf),
            pltpu.VMEM(thin, bf),
            pltpu.VMEM(thin, bf),
            pltpu.VMEM((slots, width), bf),
            pltpu.VMEM((rows * 2 * heads, wide), f32),
            pltpu.VMEM((rows, 2 * heads, wide), f32),
            pltpu.VMEM((rows, 2 * heads, size), f32),
            pltpu.VMEM((rows, 2 * heads, size), f32),
            pltpu.VMEM((PLANE, slots, width // PLANE), f32),
            pltpu.VMEM((rows, half), f32),
            pltpu.VMEM((slots, width), bf),
            pltpu.VMEM((2, 2, slots // 2, half // 2), bf),
            pltpu.VMEM((2, 2, slots // 2, half // 2), bf),
            pltpu.VMEM(parts, bf),
            pltpu.VMEM(parts, bf),
            pltpu.VMEM((2, rows, half // 2), bf),
            pltpu.VMEM(state_norm.shape, f32),
            pltpu.VMEM((heads, rows), f32),
            dma((11,)),
            dma((5,)),
            dma((1,)),
            dma((3,)),
            dma((1,)),
            dma((3,)),
            dma((1,)),
            dma((1,)),
            dma((1,)),
            dma((lines - 1,)),
            dma((1,)),
            dma((1,)),
            dma((1,)),
            dma((lines - 1,)),
            dma((1,)),
            dma((1,)),
            dma((1,)),
            dma((1,)),
            dma((1,)),
            dma((6,)),
            dma((7,)),
            dma((7,)),
            dma((1,)),
            dma((1,)),
            dma((1,)),
            dma((1,)),
            dma((1,)),
            dma((1,)),
            dma((4,)),
            dma((4, lines)),
            pltpu.SemaphoreType.REGULAR,
        ],
        compiler_params=pltpu.CompilerParams(
            collective_id=0, has_side_effects=True, vmem_limit_bytes=LAYER_BYTES
        ),
    )(*[pltpu.with_memory_space_constraint(operand, pltpu.HBM) for operand in operands])
    mixed, new_matrix, new_norm, new_max = pl.pallas_call(
        store_kernel,
        out_shape=made,
        in_specs=[anywhere] * 4,
        out_specs=(anywhere,) * 4,
        scratch_shapes=[dma((7,))],
        compiler_params=pltpu.CompilerParams(vmem_limit_bytes=STORE_BYTES),
    )(*results)
    return mixed, new_matrix, new_norm, jnp.swapaxes(new_max, 0, 1)


def rms_scale(values_in, gain_vec):
    widened = values_in.astype(jnp.float32)
    return (
        widened * lax.rsqrt(jnp.mean(widened * widened, axis=-1, keepdims=True) + 1e-06) * gain_vec
    )


def memory_cell(
    query,
    key_row,
    value_row,
    outgate,
    input_pre,
    forget_pre,
    head_gain,
    state_matrix,
    state_norm,
    state_max,
):
    seq_rows, head_count = input_pre.shape
    head_size = query.shape[1] // head_count
    query_heads = query.astype(jnp.float32).reshape(seq_rows, head_count, head_size)
    key_heads = key_row.astype(jnp.float32).reshape(
        seq_rows, head_count, head_size
    ) * head_size ** (-0.5)
    value_heads = value_row.astype(jnp.float32).reshape(seq_rows, head_count, head_size)
    log_forget = jax.nn.log_sigmoid(forget_pre)
    new_max = jnp.maximum(log_forget + state_max, input_pre)
    keep_old = jnp.exp(log_forget + state_max - new_max)
    keep_new = jnp.exp(input_pre - new_max)
    new_matrix = (
        keep_old[:, :, None, None] * state_matrix
        + keep_new[:, :, None, None] * value_heads[:, :, :, None] * key_heads[:, :, None, :]
    )
    new_norm = keep_old[:, :, None] * state_norm + keep_new[:, :, None] * key_heads
    numerator = jnp.einsum(
        "bhvd,bhd->bhv", new_matrix, query_heads, precision=lax.Precision.HIGHEST
    )
    denominator = jnp.sum(new_norm * query_heads, axis=-1)
    cell_read = numerator / jnp.maximum(jnp.abs(denominator), jnp.exp(-new_max))[:, :, None]
    centered = cell_read - jnp.mean(cell_read, axis=-1, keepdims=True)
    variance = jnp.mean(centered * centered, axis=-1, keepdims=True)
    scaled_cell = (centered * lax.rsqrt(variance + 1e-06)).reshape(seq_rows, head_count * head_size)
    cell_out = (scaled_cell * head_gain * jax.nn.sigmoid(outgate.astype(jnp.float32))).astype(
        jnp.bfloat16
    )
    return (cell_out, new_matrix, new_norm, new_max)


def kernels_fit(tokens, w_query, w_igate, w_out, w_expert_gate, routes):
    ep_count = lax.axis_size("ep")
    rows, width = tokens.shape
    capacity = max(2, 2 * rows * routes.shape[1] // (w_expert_gate.shape[0] * ep_count))
    return (
        lax.axis_size("tp") == 2
        and ep_count % (2 * PLANE) == 0
        and w_query.shape[0] == LANES
        and w_query.shape[1] % LANES == 0
        and w_out.shape[1] % LANES == 0
        and width % (2 * LANES) == 0
        and rows % 16 == 0
        and w_igate.shape[1] == 4
        and rows <= LANES
        and w_expert_gate.shape[0] == 1
        and capacity == SUB + SUB // 2
        and ep_count * SUB == LANES
        and ep_count // PLANE == 4
        and w_query.shape[1] == 2 * LANES
    )


def body(
    tokens,
    mix_gain,
    w_query,
    w_key,
    w_value,
    w_outgate,
    w_igate,
    w_fgate,
    igate_bias,
    fgate_bias,
    head_gain,
    w_out,
    state_matrix,
    state_norm,
    state_max,
    ffn_gain,
    w_expert_gate,
    w_expert_up,
    w_expert_down,
    routes,
    route_weights,
):
    seq_rows, width = tokens.shape
    weight_list = (w_query, w_key, w_value, w_outgate, w_igate, w_fgate)
    if kernels_fit(tokens, w_query, w_igate, w_out, w_expert_gate, routes):
        mixed, new_matrix, new_norm, new_max = layer_call(
            tokens,
            mix_gain,
            weight_list,
            igate_bias,
            fgate_bias,
            head_gain,
            w_out,
            state_matrix,
            state_norm,
            state_max,
            ffn_gain,
            (w_expert_gate, w_expert_up, w_expert_down),
            routes,
            route_weights,
        )
        return (mixed, new_matrix, new_norm, new_max)
    normed = rms_scale(tokens, mix_gain).astype(jnp.bfloat16)
    spread = lax.all_to_all(normed, "ep", split_axis=1, concat_axis=0, tiled=True)
    joined = jnp.concatenate(weight_list, axis=1)
    summed = lax.psum_scatter(
        jnp.dot(spread, joined, preferred_element_type=jnp.float32),
        "ep",
        scatter_dimension=0,
        tiled=True,
    )
    bounds = [0]
    for weight in weight_list:
        bounds.append(bounds[-1] + weight.shape[1])
    projected = tuple(
        (summed[:, bounds[index] : bounds[index + 1]] for index in range(len(weight_list)))
    )
    query = projected[0].astype(jnp.bfloat16)
    key_row = projected[1].astype(jnp.bfloat16)
    value_row = projected[2].astype(jnp.bfloat16)
    outgate = projected[3].astype(jnp.bfloat16)
    input_pre = projected[4] + igate_bias
    forget_pre = projected[5] + fgate_bias
    cell_out, new_matrix, new_norm, new_max = memory_cell(
        query,
        key_row,
        value_row,
        outgate,
        input_pre,
        forget_pre,
        head_gain,
        state_matrix,
        state_norm,
        state_max,
    )
    partial_out = jnp.dot(
        cell_out,
        lax.all_gather(w_out, "ep", axis=1, tiled=True),
        preferred_element_type=jnp.float32,
    )
    attended = lax.psum(partial_out.astype(jnp.bfloat16), "tp").astype(jnp.float32)
    resid = (tokens.astype(jnp.float32) + attended).astype(jnp.bfloat16)
    normed_two = rms_scale(resid, ffn_gain).astype(jnp.bfloat16)
    ep_count = lax.axis_size("ep")
    local_experts = w_expert_gate.shape[0]
    expert_total = local_experts * ep_count
    top_count = routes.shape[1]
    capacity = max(2, 2 * seq_rows * top_count // expert_total)
    flat_routes = routes.reshape(-1)
    onehot = (flat_routes[:, None] == jnp.arange(expert_total, dtype=jnp.int32)[None, :]).astype(
        jnp.int32
    )
    earlier = jnp.cumsum(onehot, axis=0, dtype=jnp.int32) - onehot
    slots = jnp.sum(onehot * earlier, axis=1, dtype=jnp.int32)
    targets = flat_routes * capacity + slots
    dispatch = (
        targets[:, None] == jnp.arange(expert_total * capacity, dtype=jnp.int32)[None, :]
    ).astype(jnp.bfloat16)
    route_rows = jnp.repeat(normed_two, top_count, axis=0)
    outgoing = jnp.einsum(
        "rs,rd->sd", dispatch, route_rows, preferred_element_type=jnp.float32
    ).astype(jnp.bfloat16)
    outgoing = outgoing.reshape(expert_total, capacity, width)
    received = lax.all_to_all(outgoing, "ep", split_axis=0, concat_axis=0, tiled=True)
    slot_count = received.shape[1]
    regrouped = received.reshape(ep_count, local_experts, slot_count, width)
    gate_pre = jnp.einsum(
        "nxcd,xdf->nxcf", regrouped, w_expert_gate, preferred_element_type=jnp.float32
    )
    up_pre = jnp.einsum(
        "nxcd,xdf->nxcf", regrouped, w_expert_up, preferred_element_type=jnp.float32
    )
    hidden = (jax.nn.silu(gate_pre) * up_pre).astype(jnp.bfloat16)
    partial_down = jnp.einsum(
        "nxcf,xfd->nxcd", hidden, w_expert_down, preferred_element_type=jnp.float32
    )
    expert_sum = lax.psum(partial_down.astype(jnp.bfloat16), "tp")
    finished = expert_sum.reshape(ep_count * local_experts, slot_count, width)
    returned = lax.all_to_all(finished, "ep", split_axis=0, concat_axis=0, tiled=True)
    picked = jnp.dot(
        dispatch,
        returned.reshape(expert_total * capacity, width),
        preferred_element_type=jnp.float32,
    )
    weighted = jnp.sum(
        picked.reshape(seq_rows, top_count, width) * route_weights[:, :, None], axis=1
    )
    mixed = (resid.astype(jnp.float32) + weighted).astype(jnp.bfloat16)
    return (mixed, new_matrix, new_norm, new_max)


def solution(mesh):
    placed = (
        P("ep", None),
        P(),
        P("ep", "tp"),
        P("ep", "tp"),
        P("ep", "tp"),
        P("ep", "tp"),
        P("ep", "tp"),
        P("ep", "tp"),
        P("tp"),
        P("tp"),
        P("tp"),
        P("tp", "ep"),
        P("ep", "tp", None, None),
        P("ep", "tp", None),
        P("ep", "tp"),
        P(),
        P("ep", None, "tp"),
        P("ep", None, "tp"),
        P("ep", "tp", None),
        P("ep", None),
        P("ep", None),
    )
    return jax.shard_map(
        body,
        mesh=mesh,
        in_specs=placed,
        out_specs=(P("ep", None), P("ep", "tp", None, None), P("ep", "tp", None), P("ep", "tp")),
        check_vma=False,
    )
```
